256 devices in a mesh: ep: 64 (over z, y, core), tp: 4 (over x).
Axes of the slice: x: 4, y: 4, z: 8, core: 2. Of those that a mesh axis runs over, the one named last changes fastest.
Arguments:
- outer_gate: bfloat16 [32768, 2048], P('ep', 'tp'), may hold values from -6 to 6
- inner_gate: bfloat16 [32768, 2048], P('ep', 'tp'), may hold values from -6 to 6
- conv_values: bfloat16 [32768, 2048], P('ep', 'tp'), may hold values from -6 to 6
- conv_taps: bfloat16 [3, 2048], P(None, 'tp'), may hold values from -3 to 3
- out_weight: bfloat16 [2048, 2048], P('tp'), may hold values from -0.125 to 0.125
- moe_input: bfloat16 [32768, 2048], P(('ep', 'tp')), may hold values from -6 to 6
- norm_gain: bfloat16 [2048], replicated, may hold values from 0.099609375 to 1.8984375
- gate_proj: bfloat16 [64, 2048, 1024], P('ep', None, 'tp'), may hold values from -0.125 to 0.125
- up_proj: bfloat16 [64, 2048, 1024], P('ep', None, 'tp'), may hold values from -0.125 to 0.125
- down_proj: bfloat16 [64, 1024, 2048], P('ep', 'tp'), may hold values from -0.1875 to 0.1875
- shared_gate: bfloat16 [2048, 1024], P(None, 'tp'), may hold values from -0.125 to 0.125
- shared_up: bfloat16 [2048, 1024], P(None, 'tp'), may hold values from -0.125 to 0.125
- shared_down: bfloat16 [1024, 2048], P('tp'), may hold values from -0.1875 to 0.1875
- routes: int32 [32768, 2], P('ep'), may hold values from 0 to 63, all different within a row; in each aligned block of 128 rows (0 to 127, 128 to 255, ...) at most 8 rows name the same one
- route_weight: float32 [32768, 2], P('ep'), may hold values from 0.3 to 1.5
Outputs:
- mixer_out: bfloat16 [32768, 2048], P(('ep', 'tp'))
- expert_mix: bfloat16 [32768, 2048], P(('ep', 'tp'))
The draws below stay inside these ranges and needn't reach their ends.
Inputs may be any that keep to these rules, and one draw needn't show every extreme that they name: `routes`: each row names 2 different experts. In the 128 rows of one device no expert is named more than 8 times, and in every draw some expert is named exactly 8 times in one device's rows.
All inputs are finite; a program needn't handle non-finite values.
Results may differ from the reference program's by a relative error of at most 0.012.
Values may be sent and summed in bfloat16 or wider, within the bound.
A program may use at most 128 MiB of HBM per device.

```python
import math
import jax
import jax.numpy as jnp
import numpy as np
from jax import lax

D = 2048
EH = 1024
SH = 1024
TOPK = 2
TAPS = 3
R2 = 128
EXPERTS = 64
CAP = 8
TOK1 = 32768
TOK2 = 32768
N_EP = 64
N_TP = 4


def block_scale(rng, dims, cuts, low, top_value):
    gain = 1.0
    for position, blocks in cuts:
        draws = jax.random.uniform(jax.random.fold_in(jax.random.fold_in(rng, 6), position), (blocks,), jnp.float32, low / len(cuts), top_value / len(cuts))
        gain = gain * jnp.repeat(jnp.exp(draws), dims[position] // blocks).reshape((-1,) + (1,) * (len(dims) - 1 - position))
    return gain


def assign_block(key, own, number, rows, number_of, top, limit, skew):
    ranking = jax.random.permutation(key, number_of)
    heavy_load, common = shares(number_of, rows * top, limit, skew, True), shares(number_of, rows * top, limit, skew, False)
    places = jnp.arange(number_of)

    def named(tallies, turn):
        used = int((tallies > 0).sum())
        fixed = max(1, used // 4)
        passed = fixed + (places - fixed + turn * (used - fixed)) % max(1, number_of - fixed)
        return jnp.zeros((number_of,), jnp.int32).at[ranking[jnp.where(places < fixed, places, passed)]].set(jnp.asarray(tallies, jnp.int32))

    tallies = jnp.where(number % 4 == 0, named(heavy_load, number // 4), named(common, number - number // 4 - 1))
    mixed = jax.random.permutation(jax.random.fold_in(own, 3), number_of)
    donor, receiver = mixed[0:number_of // 2 * 2:2], mixed[1:number_of // 2 * 2:2]
    room = jnp.minimum(tallies[donor] - 1, limit - tallies[receiver]) // 2
    room = jnp.where((donor == ranking[0]) | (receiver == ranking[0]) | (tallies[receiver] == 0), 0, jnp.maximum(room, 0))
    passed = jax.random.randint(jax.random.fold_in(own, 4), (number_of // 2,), 0, 1 << 20) % (room + 1)
    tallies = tallies.at[donor].add(-passed).at[receiver].add(passed)
    items = jnp.searchsorted(jnp.cumsum(tallies), jnp.arange(rows * top), side="right").astype(jnp.int32)
    table = items.reshape(top, rows).T
    table = table[jax.random.permutation(jax.random.fold_in(own, 1), rows)]
    turn = jax.random.randint(jax.random.fold_in(own, 2), (rows, 1), 0, top)
    return jnp.take_along_axis(table, (jnp.arange(top)[None, :] + turn) % top, axis=1)


def shares(count, total, bound, slope, full):
    weights = [(1 << 20) // math.isqrt(standing ** slope) + 1 for standing in range(1, count + 1)]
    largest = bound if full else min(bound, max(-(-total // count), total * weights[0] // sum(weights)))
    least = 1 if total - largest >= count - 1 else 0
    given, surplus = [largest] + [least] * (count - 1), total - largest - least * (count - 1)
    while surplus > 0:
        movable = [i for i in range(1, count) if given[i] < largest] or [i for i in range(1, count) if given[i] < bound]
        pool, budget = sum([weights[i] for i in movable]), surplus
        for i in movable:
            extra = min(bound - given[i], max(1, budget * weights[i] // pool), surplus)
            given[i] = given[i] + extra
            surplus = surplus - extra
    return np.array(given)


def normal_values(key, shape, spread, bound, split=(), held_as=jnp.bfloat16):
    drawn = jax.random.normal(key, shape, jnp.float32) * spread
    if len(split) > 0:
        drawn = block_scale(key, shape, split, -0.22, 0.18) * drawn
    return jnp.clip(drawn, min=-bound, max=bound).astype(held_as)


def setup_inputs(seed: int = 0) -> dict:
    key_of = jax.random.split(jax.random.key(seed), 16)
    outer_gate = normal_values(key_of[0], (TOK1, D), 1.0, 6.0, ((0, 64), (1, 4)))
    inner_gate = normal_values(key_of[1], (TOK1, D), 1.0, 6.0, ((0, 64), (1, 4)))
    conv_values = normal_values(key_of[2], (TOK1, D), 1.0, 6.0, ((0, 64), (1, 4)))
    conv_taps = normal_values(key_of[3], (TAPS, D), 0.577, 3.0, ((1, 4),))
    out_weight = normal_values(key_of[4], (D, D), D ** -0.5, 0.125, ((0, 4),))
    moe_input = normal_values(key_of[5], (TOK2, D), 1.0, 6.0, ((0, 256),))
    norm_gain = jnp.clip(1.0 + 0.18 * jax.random.normal(key_of[6], (D,), jnp.float32), 0.099609375, 1.8984375).astype(jnp.bfloat16)
    gate_proj = normal_values(key_of[7], (EXPERTS, D, EH), D ** -0.5, 0.125, ((0, 64), (2, 4)))
    up_proj = normal_values(key_of[8], (EXPERTS, D, EH), D ** -0.5, 0.125, ((0, 64), (2, 4)))
    down_proj = normal_values(key_of[9], (EXPERTS, EH, D), EH ** -0.5, 0.1875, ((0, 64), (1, 4)))
    shared_gate = normal_values(key_of[10], (D, SH), D ** -0.5, 0.125, ((1, 4),))
    shared_up = normal_values(key_of[11], (D, SH), D ** -0.5, 0.125, ((1, 4),))
    shared_down = normal_values(key_of[12], (SH, D), SH ** -0.5, 0.1875, ((0, 4),))
    routes_keys = jax.random.split(jax.random.fold_in(key_of[13], 1), TOK2 // R2)
    routes_turns = jax.random.permutation(jax.random.fold_in(key_of[13], 3), TOK2 // R2)
    routes = jax.vmap(lambda own, number: assign_block(jax.random.fold_in(key_of[13], 2), own, number, R2, N_EP, TOPK, CAP, 2))(routes_keys, routes_turns).reshape((TOK2, TOPK))
    route_weight = jnp.clip(0.3 + 1.2 * jax.random.uniform(key_of[14], (TOK2, TOPK), jnp.float32) ** block_scale(key_of[14], (TOK2, TOPK), ((0, 64),), -0.2, 0.2), 0.3, 1.5)
    return dict(outer_gate=outer_gate, inner_gate=inner_gate, conv_values=conv_values, conv_taps=conv_taps, out_weight=out_weight, moe_input=moe_input, norm_gain=norm_gain, gate_proj=gate_proj, up_proj=up_proj, down_proj=down_proj, shared_gate=shared_gate, shared_up=shared_up, shared_down=shared_down, routes=routes, route_weight=route_weight)


epsilon = 1e-06

def rms_norm(inputs, scales):
    values = inputs.astype(jnp.float32)
    square = lax.optimization_barrier(jnp.mean(values * values, axis=-1, keepdims=True))
    return (values * lax.rsqrt(square + epsilon) * scales.astype(jnp.float32)).astype(jnp.bfloat16)

def summed_parts(hidden, weight, pieces):
    stride = hidden.shape[1] // pieces
    result = jnp.zeros((hidden.shape[0], weight.shape[1]), jnp.float32)
    for piece_idx in range(pieces):
        partial_sum = jnp.dot(hidden[:, piece_idx * stride:(piece_idx + 1) * stride], weight[piece_idx * stride:(piece_idx + 1) * stride], preferred_element_type=jnp.float32).astype(jnp.bfloat16)
        partial_sum = lax.optimization_barrier(partial_sum)
        result = result + partial_sum.astype(jnp.float32)
    return result

def swiglu(inputs, gate_w, up_w):
    gate_term = jnp.dot(inputs, gate_w, preferred_element_type=jnp.float32)
    upward = jnp.dot(inputs, up_w, preferred_element_type=jnp.float32)
    return (jax.nn.silu(gate_term) * upward).astype(jnp.bfloat16)

def reference(outer_gate, inner_gate, conv_values, conv_taps, out_weight, moe_input, norm_gain, gate_proj, up_proj, down_proj, shared_gate, shared_up, shared_down, routes, route_weight):
    product = inner_gate.astype(jnp.float32) * conv_values.astype(jnp.float32)
    length = product.shape[0]
    padded = jnp.pad(product, ((TAPS - 1, 0), (0, 0)))
    tap_values = conv_taps.astype(jnp.float32)
    convolved = jnp.zeros_like(product)
    for offset in range(TAPS):
        convolved = convolved + tap_values[offset] * padded[offset:offset + length]
    gate_rows = (outer_gate.astype(jnp.float32) * convolved).astype(jnp.bfloat16)
    mixer_out = summed_parts(gate_rows, out_weight, N_TP).astype(jnp.bfloat16)
    normed = rms_norm(moe_input, norm_gain)
    tokens = normed.shape[0]
    slot_limit = N_EP * N_TP * CAP
    token_ids = jnp.arange(tokens, dtype=jnp.int32)

    def one_expert(running, operands):
        expert, gate_w, up_w, down_w = operands
        expert_hits = routes == expert
        chosen = jnp.any(expert_hits, axis=1)
        weight_sum = lax.optimization_barrier(jnp.sum(jnp.where(expert_hits, route_weight, jnp.float32(0.0)), axis=1))
        places = jnp.cumsum(chosen.astype(jnp.int32)) - 1
        targets = jnp.where(chosen, places, slot_limit).astype(jnp.int32)
        row_table = jnp.zeros((slot_limit,), jnp.int32).at[targets].set(token_ids, mode='drop')
        filled = jnp.zeros((slot_limit,), jnp.float32).at[targets].set(1.0, mode='drop')
        hidden = swiglu(normed[row_table], gate_w, up_w)
        result = summed_parts(hidden, down_w, N_TP).astype(jnp.bfloat16)
        result = lax.optimization_barrier(result)
        scaled = result.astype(jnp.float32) * (weight_sum[row_table] * filled)[:, None]
        return (running.at[row_table].add(scaled), None)
    routed, _ = lax.scan(one_expert, jnp.zeros((tokens, normed.shape[1]), jnp.float32), (jnp.arange(N_EP, dtype=jnp.int32), gate_proj, up_proj, down_proj))
    shared_hidden = swiglu(normed, shared_gate, shared_up)
    shared_sum = summed_parts(shared_hidden, shared_down, N_TP)
    expert_mix = (shared_sum + routed).astype(jnp.bfloat16)
    return (mixer_out, expert_mix)
```

```python
import functools

import jax
import jax.numpy as jnp
from jax import lax
from jax.experimental import pallas as pl
from jax.experimental.pallas import tpu as pltpu
from jax.sharding import PartitionSpec as P

MESH = pl.DeviceIdType.MESH
epsilon = 1e-06
bf16 = jnp.bfloat16
f32 = jnp.float32
HALO = 16


def remote(src, dst, send_sem, recv_sem, ep, tp):
    return pltpu.make_async_remote_copy(
        src_ref=src,
        dst_ref=dst,
        send_sem=send_sem,
        recv_sem=recv_sem,
        device_id={"ep": ep, "tp": tp},
        device_id_type=MESH,
    )


def dot(a, b):
    return jnp.dot(a, b, preferred_element_type=f32)


def kernel(
    experts,
    capacity,
    tile,
    outer_hbm,
    inner_hbm,
    values_hbm,
    taps,
    outw_hbm,
    moe_hbm,
    gain,
    gate_hbm,
    up_hbm,
    down_hbm,
    sgate_hbm,
    sup_hbm,
    sdown_hbm,
    routes,
    weights,
    mixer_out,
    expert_out,
    moe,
    outer,
    inner,
    values,
    halo_inner,
    halo_values,
    product,
    gated,
    outw,
    group,
    outgoing,
    landed,
    results,
    returned,
    rows,
    wgate,
    wup,
    wdown,
    sgate,
    sup,
    sdown,
    act,
    sact,
    pick,
    spread_hi,
    spread_lo,
    mixer_part,
    shared_part,
    first_in,
    second_out,
    second_in,
    load_sem,
    halo_send,
    halo_recv,
    group_send,
    group_recv,
    out_send,
    out_recv,
    own_sem,
    far_send,
    near_send,
    twin_send,
    weight_recv,
    first_send,
    first_recv,
    second_send,
    second_recv,
    back_send,
    back_recv,
):
    ep, x = lax.axis_index("ep"), lax.axis_index("tp")
    core, chip = lax.rem(ep, 2), lax.div(ep, 2)
    near = x + 1 - 2 * lax.rem(x, 2)
    far = 3 - x
    side = lax.div(x, 2)
    owner = 1 - lax.rem(core + side, 2)
    own_index = ep * owner - (1 - owner)
    twin = ep + 1 - 2 * core
    plane = x + (far - x) * (1 - owner)
    mine = 2 * chip + side
    block, width = moe.shape
    length, channels = inner.shape
    units = sgate.shape[1]
    slots = experts * capacity

    loads = [
        (moe_hbm, moe),
        (inner_hbm, inner),
        (values_hbm, values),
        (outer_hbm, outer),
        (outw_hbm, outw),
        (sgate_hbm, sgate),
        (sup_hbm, sup),
        (sdown_hbm, sdown),
    ]
    loads = [pltpu.make_async_copy(s, d, load_sem.at[i]) for i, (s, d) in enumerate(loads)]
    loads[0].start()

    own_pieces = [gate_hbm.at[0], up_hbm.at[0], down_hbm.at[0]]
    held = [wgate, wup, wdown]

    def to_near(j):
        return remote(
            own_pieces[j], held[j].at[1], near_send.at[j], weight_recv.at[3 + j], ep, near
        )

    def to_far(j):
        return remote(own_pieces[j], held[j].at[2], far_send.at[j], weight_recv.at[6 + j], ep, far)

    def onward(j):
        return remote(
            held[j].at[2], held[j].at[3], near_send.at[3 + j], weight_recv.at[9 + j], ep, near
        )

    def to_twin(k, j):
        source = own_pieces[j] if k == 0 else held[j].at[k]
        return remote(
            source, held[j].at[k], twin_send.at[3 * k + j], weight_recv.at[3 * k + j], twin, x
        )

    def keep_own(j):
        return pltpu.make_async_copy(own_pieces[j], held[j].at[0], own_sem.at[j])

    @pl.when(owner == 1)
    def _():
        for j in range(3):
            to_near(j).start()

    @pl.when(owner == 0)
    def _():
        for j in range(3):
            to_far(j).start()

    after = lax.rem(ep + 1, experts)
    tail = pl.ds(length - HALO, HALO)
    halos = [
        remote(inner_hbm.at[tail], halo_inner, halo_send.at[0], halo_recv.at[0], after, x),
        remote(values_hbm.at[tail], halo_values, halo_send.at[1], halo_recv.at[1], after, x),
    ]
    for h in halos:
        h.start()

    at = pl.ds(pl.multiple_of(x * block, block), block)
    chosen = [routes[k : k + 1, at].astype(f32) for k in range(2)]
    expert_ids = lax.broadcasted_iota(jnp.int32, (experts, block), 0).astype(f32)
    hits = [(expert_ids == chosen[k]).astype(f32) for k in range(2)]
    earlier = (
        lax.broadcasted_iota(jnp.int32, (block, block), 0)
        < lax.broadcasted_iota(jnp.int32, (block, block), 1)
    ).astype(f32)
    rank = dot((hits[0] + hits[1]).astype(bf16), earlier.astype(bf16))
    place = [
        chosen[k] * capacity + jnp.sum(rank * hits[k], axis=0, keepdims=True) for k in range(2)
    ]
    slot_ids = lax.broadcasted_iota(jnp.int32, (slots, block), 0).astype(f32)
    pick[...] = ((slot_ids == place[0]).astype(f32) + (slot_ids == place[1]).astype(f32)).astype(
        bf16
    )

    loads[0].wait()
    step = min(16, block)

    @pl.loop(0, block // step)
    def _(i):
        r = pl.ds(pl.multiple_of(i * step, step), step)
        v = moe[r, :].astype(f32)
        square = jnp.mean(v * v, axis=-1, keepdims=True)
        group[x, r, :] = (v * lax.rsqrt(square + epsilon) * gain[...].astype(f32)).astype(bf16)

    @pl.loop(0, width // tile)
    def _(i):
        cols = pl.ds(pl.multiple_of(i * tile, tile), tile)
        taken = dot(pick[...], group[x, :, cols])
        outgoing[:, :, cols] = taken.reshape(experts, capacity, tile).astype(bf16)

    def send_out(e):
        cross = lax.rem(lax.rem(e, 2) + side, 2)
        return remote(
            outgoing.at[e],
            landed.at[ep],
            out_send.at[0],
            out_recv.at[0],
            2 * lax.div(e, 2) + side,
            x + (far - x) * cross,
        )

    @pl.loop(0, experts)
    def _(i):
        e = lax.rem(ep + 1 + i, experts)

        @pl.when(e != own_index)
        def _():
            send_out(e).start()

    group_copies = [
        remote(group.at[x], group.at[x], group_send.at[0], group_recv.at[0], ep, near),
        remote(group.at[x], group.at[x], group_send.at[1], group_recv.at[1], ep, far),
        remote(group.at[near], group.at[near], group_send.at[2], group_recv.at[2], ep, far),
    ]
    group_copies[0].start()
    group_copies[1].start()

    @pl.when(owner == 1)
    def _():
        for j in range(3):
            to_twin(0, j).start()
            keep_own(j).start()

    for c in loads[1:]:
        c.start()

    def relay(j):
        @pl.when(owner == 1)
        def _():
            to_far(j).wait_recv()
            onward(j).start()
            to_twin(2, j).start()
            to_near(j).wait_recv()
            to_twin(1, j).start()

    @pl.when(owner == 1)
    def _():
        landed[ep] = outgoing[ep]

    share = [weights[k : k + 1, at] for k in range(2)]
    spread = jnp.where(slot_ids == place[0], share[0], 0.0) + jnp.where(
        slot_ids == place[1], share[1], 0.0
    )
    spread = spread.T
    high = spread.astype(bf16)
    spread_hi[...] = high
    spread_lo[...] = (spread - high.astype(f32)).astype(bf16)

    for c in loads[1:4]:
        c.wait()
    for h in halos:
        h.wait_recv()
    first = (ep > 0).astype(f32)
    product[0:HALO, :] = halo_inner[...].astype(f32) * halo_values[...].astype(f32) * first
    piece = min(64, length)

    @pl.loop(0, length // piece)
    def _(i):
        r = pl.ds(pl.multiple_of(i * piece, piece), piece)
        product[pl.ds(pl.multiple_of(HALO + i * piece, HALO), piece), :] = inner[r, :].astype(
            f32
        ) * values[r, :].astype(f32)

    tap = taps[...].astype(f32)
    for i in range(length // piece):
        lo = i * piece
        conv = tap[0:1] * product[HALO - 2 + lo : HALO - 2 + lo + piece, :]
        conv = conv + tap[1:2] * product[HALO - 1 + lo : HALO - 1 + lo + piece, :]
        conv = conv + tap[2:3] * product[HALO + lo : HALO + lo + piece, :]
        gated[lo : lo + piece, :] = (outer[lo : lo + piece, :].astype(f32) * conv).astype(bf16)
    loads[4].wait()

    @pl.loop(0, width // tile)
    def _(i):
        cols = pl.ds(pl.multiple_of(i * tile, tile), tile)
        part = dot(gated[...], outw[:, cols]).astype(bf16)
        mixer_part[:, :, cols] = part.reshape(4, block, tile)

    relay(0)

    group_copies[0].wait_recv()
    group_copies[2].start()
    group_copies[1].wait_recv()
    relay(1)
    group_copies[2].wait_recv()
    for c in loads[5:8]:
        c.wait()

    @pl.loop(0, 4)
    def _(b):
        g = dot(group[b], sgate[...])
        u = dot(group[b], sup[...])
        r = pl.ds(pl.multiple_of(b * block, block), block)
        sact[r, :] = (g / (1.0 + jnp.exp(-g)) * u).astype(bf16)

    @pl.loop(0, width // tile)
    def _(i):
        cols = pl.ds(pl.multiple_of(i * tile, tile), tile)
        part = dot(sact[...], sdown[:, cols]).astype(bf16)
        shared_part[:, :, cols] = part.reshape(4, block, tile)

    relay(2)

    @pl.when(owner == 1)
    def _():
        some = landed.at[pl.ds(0, experts - 1)]
        remote(some, some, out_send.at[0], out_recv.at[0], twin, x).wait_recv()

    @pl.when(owner == 0)
    def _():
        remote(landed, landed, out_send.at[0], out_recv.at[0], twin, x).wait_recv()

    half = slots // 2
    half_experts = experts // 2

    @pl.loop(0, width // tile)
    def _(i):
        cols = pl.ds(pl.multiple_of(i * tile, tile), tile)
        rows[:, cols] = landed[:, :, cols].reshape(slots, tile)

    def gate_up(k):
        cols = pl.ds(pl.multiple_of(k * units, units), units)

        @pl.loop(0, 2)
        def _(m):
            r = pl.ds(pl.multiple_of(m * half, half), half)
            g = dot(rows[r, :], wgate[k])
            u = dot(rows[r, :], wup[k])
            act[r, cols] = (g / (1.0 + jnp.exp(-g)) * u).astype(bf16)

    for k in range(3):

        @pl.when(owner == 0)
        def _():
            for j in range(2):
                to_twin(k, j).wait_recv()

        if k == 0:

            @pl.when(owner == 1)
            def _():
                for j in range(2):
                    keep_own(j).wait()

        gate_up(k)

    for j in range(2):

        @pl.when(owner == 1)
        def _():
            onward(j).wait_recv()
            to_twin(3, j).start()

        @pl.when(owner == 0)
        def _():
            to_twin(3, j).wait_recv()

    gate_up(3)

    @pl.when(owner == 1)
    def _():
        keep_own(2).wait()
        onward(2).wait_recv()
        to_twin(3, 2).start()

    @pl.when(owner == 0)
    def _():
        for k in range(4):
            to_twin(k, 2).wait_recv()

    def send_back(s):
        return remote(
            results.at[s], returned.at[mine], back_send.at[0], back_recv.at[0], s, plane
        )

    @pl.loop(0, 2)
    def _(m):
        r = pl.ds(pl.multiple_of(m * half, half), half)

        @pl.loop(0, width // tile)
        def _(i):
            cols = pl.ds(pl.multiple_of(i * tile, tile), tile)
            total = dot(act[r, 0:units], wdown[0, :, cols])
            for k in range(1, 4):
                total = total + dot(act[r, k * units : (k + 1) * units], wdown[k, :, cols])
            results[pl.ds(m * half_experts, half_experts), :, cols] = total.reshape(
                half_experts, capacity, tile
            ).astype(bf16)

        @pl.loop(0, half_experts)
        def _(i):
            s = m * half_experts + lax.rem(ep + 1 + i, half_experts)

            @pl.when(s != own_index)
            def _():
                send_back(s).start()

    parts = [mixer_part, shared_part]

    def first_copy(kind, b):
        src = near if b == 0 else 3 - near
        return remote(
            parts[kind].at[src],
            first_in.at[kind, b],
            first_send.at[2 * kind + b],
            first_recv.at[2 * kind + b],
            ep,
            near,
        )

    def second_copy(kind):
        return remote(
            second_out.at[kind],
            second_in.at[kind],
            second_send.at[kind],
            second_recv.at[kind],
            ep,
            far,
        )

    for kind in range(2):
        for b in (1, 0):
            first_copy(kind, b).start()

    @pl.when(owner == 1)
    def _():
        returned[ep] = results[ep]

    pieces = 4 if block % 64 == 0 else 1
    some_rows = block // pieces

    for kind in range(2):
        first_copy(kind, 1).wait_recv()

        @pl.loop(0, pieces)
        def _(i):
            r = pl.ds(pl.multiple_of(i * some_rows, some_rows), some_rows)
            second_out[kind, r, :] = (
                parts[kind][far, r, :].astype(f32) + first_in[kind, 1, r, :].astype(f32)
            ).astype(bf16)

        second_copy(kind).start()

    first_copy(0, 0).wait_recv()
    second_copy(0).wait_recv()

    @pl.loop(0, pieces)
    def _(i):
        r = pl.ds(pl.multiple_of(i * some_rows, some_rows), some_rows)
        mixer_out[r, :] = (
            mixer_part[x, r, :].astype(f32)
            + first_in[0, 0, r, :].astype(f32)
            + second_in[0, r, :].astype(f32)
        ).astype(bf16)

    first_copy(1, 0).wait_recv()
    second_copy(1).wait_recv()

    @pl.when(owner == 1)
    def _():
        some = returned.at[pl.ds(0, experts - 1)]
        remote(some, some, back_send.at[0], back_recv.at[0], twin, x).wait_recv()

    @pl.when(owner == 0)
    def _():
        remote(returned, returned, back_send.at[0], back_recv.at[0], twin, x).wait_recv()

    @pl.loop(0, width // tile)
    def _(i):
        cols = pl.ds(pl.multiple_of(i * tile, tile), tile)
        back = returned[:, :, cols].reshape(slots, tile)
        total = (
            shared_part[x, :, cols].astype(f32)
            + first_in[1, 0, :, cols].astype(f32)
            + second_in[1, :, cols].astype(f32)
        )
        total = total + dot(spread_hi[...], back) + dot(spread_lo[...], back)
        expert_out[:, cols] = total.astype(bf16)

    for h in halos:
        h.wait_send()
    for c in group_copies:
        c.wait_send()
    for kind in range(2):
        for b in range(2):
            first_copy(kind, b).wait_send()
        second_copy(kind).wait_send()

    @pl.when(owner == 1)
    def _():
        for j in range(3):
            to_near(j).wait_send()
            onward(j).wait_send()
            for k in range(4):
                to_twin(k, j).wait_send()
        some = outgoing.at[pl.ds(0, experts - 1)]
        remote(some, some, out_send.at[0], out_recv.at[0], twin, x).wait_send()
        some = results.at[pl.ds(0, experts - 1)]
        remote(some, some, back_send.at[0], back_recv.at[0], twin, x).wait_send()

    @pl.when(owner == 0)
    def _():
        for j in range(3):
            to_far(j).wait_send()
        remote(outgoing, outgoing, out_send.at[0], out_recv.at[0], twin, x).wait_send()
        remote(results, results, back_send.at[0], back_recv.at[0], twin, x).wait_send()


def per_device(
    outer_gate,
    inner_gate,
    conv_values,
    conv_taps,
    out_weight,
    moe_input,
    norm_gain,
    gate_proj,
    up_proj,
    down_proj,
    shared_gate,
    shared_up,
    shared_down,
    routes,
    route_weight,
):
    experts = lax.axis_size("ep")
    length, channels = inner_gate.shape
    block, width = moe_input.shape
    units = gate_proj.shape[2]
    capacity = 2 * block * routes.shape[1] // experts
    slots = experts * capacity
    tile = min(256, width)
    vmem = pl.BlockSpec(memory_space=pltpu.VMEM)
    hbm = pl.BlockSpec(memory_space=pl.ANY)
    dma = pltpu.SemaphoreType.DMA

    def space(*shape):
        return pltpu.VMEM(shape, bf16)

    out = jax.ShapeDtypeStruct((block, width), bf16)
    return pl.pallas_call(
        functools.partial(kernel, experts, capacity, tile),
        name="whole",
        out_shape=(out, out),
        in_specs=[hbm, hbm, hbm, vmem, hbm, hbm, vmem] + [hbm] * 6 + [vmem, vmem],
        out_specs=(vmem, vmem),
        scratch_shapes=[
            space(block, width),
            space(length, channels),
            space(length, channels),
            space(length, channels),
            space(HALO, channels),
            space(HALO, channels),
            pltpu.VMEM((HALO + length, channels), f32),
            space(length, channels),
            space(channels, width),
            space(4, block, width),
            space(experts, capacity, width),
            space(experts, capacity, width),
            space(experts, capacity, width),
            space(experts, capacity, width),
            space(slots, width),
            space(4, width, units),
            space(4, width, units),
            space(4, units, width),
            space(width, units),
            space(width, units),
            space(units, width),
            space(slots, 4 * units),
            space(4 * block, units),
            space(slots, block),
            space(block, slots),
            space(block, slots),
            space(4, block, width),
            space(4, block, width),
            space(2, 2, block, width),
            space(2, block, width),
            space(2, block, width),
            dma((8,)),
            dma((2,)),
            dma((2,)),
            dma((3,)),
            dma((3,)),
            dma((1,)),
            dma((1,)),
            dma((3,)),
            dma((3,)),
            dma((6,)),
            dma((12,)),
            dma((12,)),
            dma((4,)),
            dma((4,)),
            dma((2,)),
            dma((2,)),
            dma((1,)),
            dma((1,)),
        ],
        compiler_params=pltpu.CompilerParams(
            has_side_effects=True, vmem_limit_bytes=60 * 1024 * 1024
        ),
    )(
        outer_gate,
        inner_gate,
        conv_values,
        conv_taps,
        out_weight,
        moe_input,
        norm_gain.reshape(1, width),
        gate_proj,
        up_proj,
        down_proj,
        shared_gate,
        shared_up,
        shared_down,
        routes.T,
        route_weight.T,
    )


def solution(mesh):
    return jax.shard_map(
        per_device,
        mesh=mesh,
        in_specs=(
            P("ep", "tp"),
            P("ep", "tp"),
            P("ep", "tp"),
            P(None, "tp"),
            P("tp", None),
            P(("ep", "tp"), None),
            P(),
            P("ep", None, "tp"),
            P("ep", None, "tp"),
            P("ep", "tp", None),
            P(None, "tp"),
            P(None, "tp"),
            P("tp", None),
            P("ep", None),
            P("ep", None),
        ),
        out_specs=(P(("ep", "tp"), None), P(("ep", "tp"), None)),
        check_vma=False,
    )
```

```python
import functools

import jax
import jax.numpy as jnp
from jax import lax
from jax.experimental import pallas as pl
from jax.experimental.pallas import tpu as pltpu
from jax.sharding import PartitionSpec as P

MESH = pl.DeviceIdType.MESH
epsilon = 1e-06
bf16 = jnp.bfloat16
f32 = jnp.float32
HALO = 16


def remote(src, dst, send_sem, recv_sem, ep, tp):
    return pltpu.make_async_remote_copy(
        src_ref=src,
        dst_ref=dst,
        send_sem=send_sem,
        recv_sem=recv_sem,
        device_id={"ep": ep, "tp": tp},
        device_id_type=MESH,
    )


def dot(a, b):
    return jnp.dot(a, b, preferred_element_type=f32)


def kernel(
    experts,
    capacity,
    tile,
    outer_hbm,
    inner_hbm,
    values_hbm,
    taps,
    outw_hbm,
    moe_hbm,
    gain,
    gate_hbm,
    up_hbm,
    down_hbm,
    sgate_hbm,
    sup_hbm,
    sdown_hbm,
    routes,
    weights,
    mixer_out,
    expert_out,
    moe,
    outer,
    inner,
    values,
    halo_inner,
    halo_values,
    product,
    gated,
    outw,
    group,
    outgoing,
    landed,
    results,
    returned,
    rows,
    wgate,
    wup,
    wdown,
    sgate,
    sup,
    sdown,
    act,
    sact,
    pick,
    spread_hi,
    spread_lo,
    mixer_part,
    shared_part,
    first_in,
    second_out,
    second_in,
    load_sem,
    halo_send,
    halo_recv,
    group_send,
    group_recv,
    out_send,
    out_recv,
    own_sem,
    far_send,
    near_send,
    twin_send,
    weight_recv,
    first_send,
    first_recv,
    second_send,
    second_recv,
    back_send,
    back_recv,
):
    ep, x = lax.axis_index("ep"), lax.axis_index("tp")
    core, chip = lax.rem(ep, 2), lax.div(ep, 2)
    near = x + 1 - 2 * lax.rem(x, 2)
    far = 3 - x
    side = lax.div(x, 2)
    owner = 1 - lax.rem(core + side, 2)
    own_index = ep * owner - (1 - owner)
    twin = ep + 1 - 2 * core
    plane = x + (far - x) * (1 - owner)
    mine = 2 * chip + side
    block, width = moe.shape
    length, channels = inner.shape
    units = sgate.shape[1]
    slots = experts * capacity

    loads = [
        (moe_hbm, moe),
        (inner_hbm, inner),
        (values_hbm, values),
        (outer_hbm, outer),
        (outw_hbm, outw),
        (sgate_hbm, sgate),
        (sup_hbm, sup),
        (sdown_hbm, sdown),
    ]
    loads = [pltpu.make_async_copy(s, d, load_sem.at[i]) for i, (s, d) in enumerate(loads)]
    loads[0].start()

    own_pieces = [gate_hbm.at[0], up_hbm.at[0], down_hbm.at[0]]
    held = [wgate, wup, wdown]

    def to_near(j):
        return remote(
            own_pieces[j], held[j].at[1], near_send.at[j], weight_recv.at[3 + j], ep, near
        )

    def to_far(j):
        return remote(own_pieces[j], held[j].at[2], far_send.at[j], weight_recv.at[6 + j], ep, far)

    def onward(j):
        return remote(
            held[j].at[2], held[j].at[3], near_send.at[3 + j], weight_recv.at[9 + j], ep, near
        )

    def to_twin(k, j):
        source = own_pieces[j] if k == 0 else held[j].at[k]
        return remote(
            source, held[j].at[k], twin_send.at[3 * k + j], weight_recv.at[3 * k + j], twin, x
        )

    def keep_own(j):
        return pltpu.make_async_copy(own_pieces[j], held[j].at[0], own_sem.at[j])

    barrier = pltpu.get_barrier_semaphore()

    def greet(device, tp):
        pl.semaphore_signal(
            barrier, inc=1, device_id={"ep": device, "tp": tp}, device_id_type=MESH
        )

    greet(ep, near)
    greet(ep, far)
    greet(lax.rem(ep + experts - 1, experts), x)

    @pl.when(owner == 0)
    def _():
        greet(twin, x)

    @pl.loop(0, experts)
    def _(i):
        s = lax.rem(ep + 1 + i, experts)

        @pl.when(s != own_index)
        def _():
            greet(s, plane)

    @pl.when(owner == 1)
    def _():
        for j in range(3):
            keep_own(j).start()

    for c in loads[1:]:
        c.start()

    after = lax.rem(ep + 1, experts)
    tail = pl.ds(length - HALO, HALO)
    halos = [
        remote(inner_hbm.at[tail], halo_inner, halo_send.at[0], halo_recv.at[0], after, x),
        remote(values_hbm.at[tail], halo_values, halo_send.at[1], halo_recv.at[1], after, x),
    ]

    at = pl.ds(pl.multiple_of(x * block, block), block)
    chosen = [routes[k : k + 1, at].astype(f32) for k in range(2)]
    expert_ids = lax.broadcasted_iota(jnp.int32, (experts, block), 0).astype(f32)
    hits = [(expert_ids == chosen[k]).astype(f32) for k in range(2)]
    earlier = (
        lax.broadcasted_iota(jnp.int32, (block, block), 0)
        < lax.broadcasted_iota(jnp.int32, (block, block), 1)
    ).astype(f32)
    rank = dot((hits[0] + hits[1]).astype(bf16), earlier.astype(bf16))
    place = [
        chosen[k] * capacity + jnp.sum(rank * hits[k], axis=0, keepdims=True) for k in range(2)
    ]
    slot_ids = lax.broadcasted_iota(jnp.int32, (slots, block), 0).astype(f32)
    pick[...] = ((slot_ids == place[0]).astype(f32) + (slot_ids == place[1]).astype(f32)).astype(
        bf16
    )

    loads[0].wait()
    scale = gain[...].reshape(1, width).astype(f32)
    step = min(16, block)

    @pl.loop(0, block // step)
    def _(i):
        r = pl.ds(pl.multiple_of(i * step, step), step)
        v = moe[r, :].astype(f32)
        square = jnp.mean(v * v, axis=-1, keepdims=True)
        group[x, r, :] = (v * lax.rsqrt(square + epsilon) * scale).astype(bf16)

    @pl.loop(0, width // tile)
    def _(i):
        cols = pl.ds(pl.multiple_of(i * tile, tile), tile)
        taken = dot(pick[...], group[x, :, cols])
        outgoing[:, :, cols] = taken.reshape(experts, capacity, tile).astype(bf16)

    def send_out(e):
        cross = lax.rem(lax.rem(e, 2) + side, 2)
        return remote(
            outgoing.at[e],
            landed.at[ep],
            out_send.at[0],
            out_recv.at[0],
            2 * lax.div(e, 2) + side,
            x + (far - x) * cross,
        )

    pl.semaphore_wait(barrier, experts + 3)
    for h in halos:
        h.start()

    @pl.loop(0, experts)
    def _(i):
        e = lax.rem(ep + 1 + i, experts)

        @pl.when(e != own_index)
        def _():
            send_out(e).start()

    @pl.when(owner == 1)
    def _():
        for j in range(3):
            to_near(j).start()
        for j in range(3):
            to_twin(0, j).start()

    @pl.when(owner == 0)
    def _():
        for j in range(3):
            to_far(j).start()

    group_copies = [
        remote(group.at[x], group.at[x], group_send.at[0], group_recv.at[0], ep, near),
        remote(group.at[x], group.at[x], group_send.at[1], group_recv.at[1], ep, far),
        remote(group.at[near], group.at[near], group_send.at[2], group_recv.at[2], ep, far),
    ]

    def relay(j):
        @pl.when(owner == 1)
        def _():
            to_far(j).wait_recv()
            onward(j).start()
            to_twin(2, j).start()
            to_near(j).wait_recv()
            to_twin(1, j).start()

    @pl.when(owner == 1)
    def _():
        landed[ep] = outgoing[ep]

    share = [weights[k : k + 1, at] for k in range(2)]
    spread = jnp.where(slot_ids == place[0], share[0], 0.0) + jnp.where(
        slot_ids == place[1], share[1], 0.0
    )
    spread = spread.T
    high = spread.astype(bf16)
    spread_hi[...] = high
    spread_lo[...] = (spread - high.astype(f32)).astype(bf16)

    for c in loads[1:4]:
        c.wait()
    for h in halos:
        h.wait_recv()
    first = (ep > 0).astype(f32)
    product[0:HALO, :] = halo_inner[...].astype(f32) * halo_values[...].astype(f32) * first
    piece = min(64, length)

    @pl.loop(0, length // piece)
    def _(i):
        r = pl.ds(pl.multiple_of(i * piece, piece), piece)
        product[pl.ds(pl.multiple_of(HALO + i * piece, HALO), piece), :] = inner[r, :].astype(
            f32
        ) * values[r, :].astype(f32)

    tap = taps[...].astype(f32)
    for i in range(length // piece):
        lo = i * piece
        conv = tap[0:1] * product[HALO - 2 + lo : HALO - 2 + lo + piece, :]
        conv = conv + tap[1:2] * product[HALO - 1 + lo : HALO - 1 + lo + piece, :]
        conv = conv + tap[2:3] * product[HALO + lo : HALO + lo + piece, :]
        gated[lo : lo + piece, :] = (outer[lo : lo + piece, :].astype(f32) * conv).astype(bf16)
    loads[4].wait()

    @pl.loop(0, width // tile)
    def _(i):
        cols = pl.ds(pl.multiple_of(i * tile, tile), tile)
        part = dot(gated[...], outw[:, cols]).astype(bf16)
        mixer_part[:, :, cols] = part.reshape(4, block, tile)

    relay(0)

    relay(1)
    relay(2)

    @pl.when(owner == 1)
    def _():
        some = landed.at[pl.ds(0, experts - 1)]
        remote(some, some, out_send.at[0], out_recv.at[0], twin, x).wait_recv()

    @pl.when(owner == 0)
    def _():
        remote(landed, landed, out_send.at[0], out_recv.at[0], twin, x).wait_recv()

    half = slots // 2
    half_experts = experts // 2

    @pl.loop(0, width // tile)
    def _(i):
        cols = pl.ds(pl.multiple_of(i * tile, tile), tile)
        rows[:, cols] = landed[:, :, cols].reshape(slots, tile)

    def gate_up(k):
        cols = pl.ds(pl.multiple_of(k * units, units), units)

        @pl.loop(0, 2)
        def _(m):
            r = pl.ds(pl.multiple_of(m * half, half), half)
            g = dot(rows[r, :], wgate[k])
            u = dot(rows[r, :], wup[k])
            act[r, cols] = (g / (1.0 + jnp.exp(-g)) * u).astype(bf16)

    for k in range(3):

        @pl.when(owner == 0)
        def _():
            for j in range(2):
                to_twin(k, j).wait_recv()

        if k == 0:

            @pl.when(owner == 1)
            def _():
                for j in range(2):
                    keep_own(j).wait()

        gate_up(k)

    for j in range(2):

        @pl.when(owner == 1)
        def _():
            onward(j).wait_recv()
            to_twin(3, j).start()

        @pl.when(owner == 0)
        def _():
            to_twin(3, j).wait_recv()

    gate_up(3)

    parts = [mixer_part, shared_part]

    def first_copy(kind, b):
        src = near if b == 0 else 3 - near
        return remote(
            parts[kind].at[src],
            first_in.at[kind, b],
            first_send.at[2 * kind + b],
            first_recv.at[2 * kind + b],
            ep,
            near,
        )

    def second_copy(kind):
        return remote(
            second_out.at[kind],
            second_in.at[kind],
            second_send.at[kind],
            second_recv.at[kind],
            ep,
            far,
        )

    group_copies[0].start()
    group_copies[1].start()
    for b in (1, 0):
        first_copy(0, b).start()

    @pl.when(owner == 1)
    def _():
        keep_own(2).wait()
        onward(2).wait_recv()
        to_twin(3, 2).start()

    @pl.when(owner == 0)
    def _():
        for k in range(4):
            to_twin(k, 2).wait_recv()

    def send_back(s):
        return remote(
            results.at[s], returned.at[mine], back_send.at[0], back_recv.at[0], s, plane
        )

    @pl.loop(0, 2)
    def _(m):
        r = pl.ds(pl.multiple_of(m * half, half), half)

        @pl.loop(0, width // tile)
        def _(i):
            cols = pl.ds(pl.multiple_of(i * tile, tile), tile)
            total = dot(act[r, 0:units], wdown[0, :, cols])
            for k in range(1, 4):
                total = total + dot(act[r, k * units : (k + 1) * units], wdown[k, :, cols])
            results[pl.ds(m * half_experts, half_experts), :, cols] = total.reshape(
                half_experts, capacity, tile
            ).astype(bf16)

        @pl.loop(0, half_experts)
        def _(i):
            s = m * half_experts + lax.rem(ep + 1 + i, half_experts)

            @pl.when(s != own_index)
            def _():
                send_back(s).start()

    group_copies[0].wait_recv()
    group_copies[2].start()
    group_copies[1].wait_recv()
    group_copies[2].wait_recv()
    for c in loads[5:8]:
        c.wait()

    @pl.loop(0, 4)
    def _(b):
        g = dot(group[b], sgate[...])
        u = dot(group[b], sup[...])
        r = pl.ds(pl.multiple_of(b * block, block), block)
        sact[r, :] = (g / (1.0 + jnp.exp(-g)) * u).astype(bf16)

    @pl.loop(0, width // tile)
    def _(i):
        cols = pl.ds(pl.multiple_of(i * tile, tile), tile)
        part = dot(sact[...], sdown[:, cols]).astype(bf16)
        shared_part[:, :, cols] = part.reshape(4, block, tile)

    for b in (1, 0):
        first_copy(1, b).start()

    @pl.when(owner == 1)
    def _():
        returned[ep] = results[ep]

    pieces = 4 if block % 64 == 0 else 1
    some_rows = block // pieces

    for kind in range(2):
        first_copy(kind, 1).wait_recv()

        @pl.loop(0, pieces)
        def _(i):
            r = pl.ds(pl.multiple_of(i * some_rows, some_rows), some_rows)
            second_out[kind, r, :] = (
                parts[kind][far, r, :].astype(f32) + first_in[kind, 1, r, :].astype(f32)
            ).astype(bf16)

        second_copy(kind).start()

    first_copy(0, 0).wait_recv()
    second_copy(0).wait_recv()

    @pl.loop(0, pieces)
    def _(i):
        r = pl.ds(pl.multiple_of(i * some_rows, some_rows), some_rows)
        mixer_out[r, :] = (
            mixer_part[x, r, :].astype(f32)
            + first_in[0, 0, r, :].astype(f32)
            + second_in[0, r, :].astype(f32)
        ).astype(bf16)

    first_copy(1, 0).wait_recv()
    second_copy(1).wait_recv()

    @pl.when(owner == 1)
    def _():
        some = returned.at[pl.ds(0, experts - 1)]
        remote(some, some, back_send.at[0], back_recv.at[0], twin, x).wait_recv()

    @pl.when(owner == 0)
    def _():
        remote(returned, returned, back_send.at[0], back_recv.at[0], twin, x).wait_recv()

    @pl.loop(0, width // tile)
    def _(i):
        cols = pl.ds(pl.multiple_of(i * tile, tile), tile)
        back = returned[:, :, cols].reshape(slots, tile)
        total = (
            shared_part[x, :, cols].astype(f32)
            + first_in[1, 0, :, cols].astype(f32)
            + second_in[1, :, cols].astype(f32)
        )
        total = total + dot(spread_hi[...], back) + dot(spread_lo[...], back)
        expert_out[:, cols] = total.astype(bf16)

    for h in halos:
        h.wait_send()
    for c in group_copies:
        c.wait_send()
    for kind in range(2):
        for b in range(2):
            first_copy(kind, b).wait_send()
        second_copy(kind).wait_send()

    @pl.when(owner == 1)
    def _():
        for j in range(3):
            to_near(j).wait_send()
            onward(j).wait_send()
            for k in range(4):
                to_twin(k, j).wait_send()
        some = outgoing.at[pl.ds(0, experts - 1)]
        remote(some, some, out_send.at[0], out_recv.at[0], twin, x).wait_send()
        some = results.at[pl.ds(0, experts - 1)]
        remote(some, some, back_send.at[0], back_recv.at[0], twin, x).wait_send()

    @pl.when(owner == 0)
    def _():
        for j in range(3):
            to_far(j).wait_send()
        remote(outgoing, outgoing, out_send.at[0], out_recv.at[0], twin, x).wait_send()
        remote(results, results, back_send.at[0], back_recv.at[0], twin, x).wait_send()


def per_device(
    outer_gate,
    inner_gate,
    conv_values,
    conv_taps,
    out_weight,
    moe_input,
    norm_gain,
    gate_proj,
    up_proj,
    down_proj,
    shared_gate,
    shared_up,
    shared_down,
    routes,
    route_weight,
):
    experts = lax.axis_size("ep")
    length, channels = inner_gate.shape
    block, width = moe_input.shape
    units = gate_proj.shape[2]
    capacity = 2 * block * routes.shape[1] // experts
    slots = experts * capacity
    tile = min(256, width)
    vmem = pl.BlockSpec(memory_space=pltpu.VMEM)
    hbm = pl.BlockSpec(memory_space=pl.ANY)
    dma = pltpu.SemaphoreType.DMA

    def space(*shape):
        return pltpu.VMEM(shape, bf16)

    out = jax.ShapeDtypeStruct((block, width), bf16)
    return pl.pallas_call(
        functools.partial(kernel, experts, capacity, tile),
        name="whole",
        out_shape=(out, out),
        in_specs=[hbm, hbm, hbm, vmem, hbm, hbm, vmem] + [hbm] * 6 + [vmem, vmem],
        out_specs=(vmem, vmem),
        scratch_shapes=[
            space(block, width),
            space(length, channels),
            space(length, channels),
            space(length, channels),
            space(HALO, channels),
            space(HALO, channels),
            pltpu.VMEM((HALO + length, channels), f32),
            space(length, channels),
            space(channels, width),
            space(4, block, width),
            space(experts, capacity, width),
            space(experts, capacity, width),
            space(experts, capacity, width),
            space(experts, capacity, width),
            space(slots, width),
            space(4, width, units),
            space(4, width, units),
            space(4, units, width),
            space(width, units),
            space(width, units),
            space(units, width),
            space(slots, 4 * units),
            space(4 * block, units),
            space(slots, block),
            space(block, slots),
            space(block, slots),
            space(4, block, width),
            space(4, block, width),
            space(2, 2, block, width),
            space(2, block, width),
            space(2, block, width),
            dma((8,)),
            dma((2,)),
            dma((2,)),
            dma((3,)),
            dma((3,)),
            dma((1,)),
            dma((1,)),
            dma((3,)),
            dma((3,)),
            dma((6,)),
            dma((12,)),
            dma((12,)),
            dma((4,)),
            dma((4,)),
            dma((2,)),
            dma((2,)),
            dma((1,)),
            dma((1,)),
        ],
        compiler_params=pltpu.CompilerParams(
            collective_id=0, has_side_effects=True, vmem_limit_bytes=60 * 1024 * 1024
        ),
    )(
        outer_gate,
        inner_gate,
        conv_values,
        conv_taps,
        out_weight,
        moe_input,
        norm_gain,
        gate_proj,
        up_proj,
        down_proj,
        shared_gate,
        shared_up,
        shared_down,
        routes.T,
        route_weight.T,
    )


def solution(mesh):
    return jax.shard_map(
        per_device,
        mesh=mesh,
        in_specs=(
            P("ep", "tp"),
            P("ep", "tp"),
            P("ep", "tp"),
            P(None, "tp"),
            P("tp", None),
            P(("ep", "tp"), None),
            P(),
            P("ep", None, "tp"),
            P("ep", None, "tp"),
            P("ep", "tp", None),
            P(None, "tp"),
            P(None, "tp"),
            P("tp", None),
            P("ep", None),
            P("ep", None),
        ),
        out_specs=(P(("ep", "tp"), None), P(("ep", "tp"), None)),
        check_vma=False,
    )
```

```python
import functools

import jax
import jax.numpy as jnp
from jax import lax
from jax.experimental import pallas as pl
from jax.experimental.pallas import tpu as pltpu
from jax.sharding import PartitionSpec as P

MESH = pl.DeviceIdType.MESH
epsilon = 1e-06
bf16 = jnp.bfloat16
f32 = jnp.float32
HALO = 16


def remote(src, dst, send_sem, recv_sem, ep, tp):
    return pltpu.make_async_remote_copy(
        src_ref=src,
        dst_ref=dst,
        send_sem=send_sem,
        recv_sem=recv_sem,
        device_id={"ep": ep, "tp": tp},
        device_id_type=MESH,
    )


def dot(a, b):
    return jnp.dot(a, b, preferred_element_type=f32)


def kernel(
    experts,
    capacity,
    rings,
    tile,
    outer_hbm,
    inner_hbm,
    values_hbm,
    taps,
    outw_hbm,
    moe_hbm,
    gain,
    gate_hbm,
    up_hbm,
    down_hbm,
    sgate_hbm,
    sup_hbm,
    sdown_hbm,
    routes,
    weights,
    mixer_out,
    expert_out,
    moe,
    outer,
    inner,
    values,
    halo_inner,
    halo_values,
    product,
    gated,
    outw,
    group,
    outgoing,
    landed,
    results,
    returned,
    rows,
    wgate,
    wup,
    wdown,
    sgate,
    sup,
    sdown,
    act,
    sact,
    pick,
    spread_hi,
    spread_lo,
    total_down,
    mixer_part,
    shared_own,
    shared_near,
    shared_in,
    first_in,
    second_out,
    second_in,
    load_sem,
    halo_send,
    halo_recv,
    group_send,
    group_recv,
    out_send,
    out_recv,
    own_sem,
    far_send,
    near_send,
    twin_send,
    weight_recv,
    first_send,
    first_recv,
    second_send,
    second_recv,
    shared_send,
    shared_recv,
    eighth_send,
    ring_send,
    pass_send,
    eighth_recv,
    back_send,
    back_recv,
):
    ep, x = lax.axis_index("ep"), lax.axis_index("tp")
    core, chip = lax.rem(ep, 2), lax.div(ep, 2)
    near = x + 1 - 2 * lax.rem(x, 2)
    far = 3 - x
    side = lax.div(x, 2)
    owner = 1 - lax.rem(core + side, 2)
    own_index = ep * owner - (1 - owner)
    twin = ep + 1 - 2 * core
    plane = x + (far - x) * (1 - owner)
    mine = 2 * chip + side
    block, width = moe.shape
    length, channels = inner.shape
    units = sgate.shape[2]
    own_rows, near_rows = pl.ds(0, block), pl.ds(block, block)
    y = lax.rem(chip, rings)
    eighths = 2 * rings
    eighth = 2 * y + core
    slots = experts * capacity

    loads = [
        (moe_hbm, moe),
        (inner_hbm, inner),
        (values_hbm, values),
        (outer_hbm, outer),
        (outw_hbm, outw),
        (sgate_hbm, sgate.at[0]),
        (sup_hbm, sup.at[0]),
        (sdown_hbm, sdown.at[pl.ds(0, units)]),
    ]
    loads = [pltpu.make_async_copy(s, d, load_sem.at[i]) for i, (s, d) in enumerate(loads)]
    loads[0].start()

    own_pieces = [gate_hbm.at[0], up_hbm.at[0], down_hbm.at[0]]
    held = [wgate, wup, wdown]

    def to_near(j):
        return remote(
            own_pieces[j], held[j].at[1], near_send.at[j], weight_recv.at[3 + j], ep, near
        )

    def to_far(j):
        return remote(own_pieces[j], held[j].at[2], far_send.at[j], weight_recv.at[6 + j], ep, far)

    def onward(j):
        return remote(
            held[j].at[2], held[j].at[3], near_send.at[3 + j], weight_recv.at[9 + j], ep, near
        )

    def to_twin(k, j):
        source = own_pieces[j] if k == 0 else held[j].at[k]
        return remote(
            source, held[j].at[k], twin_send.at[3 * k + j], weight_recv.at[3 * k + j], twin, x
        )

    def keep_own(j):
        return pltpu.make_async_copy(own_pieces[j], held[j].at[0], own_sem.at[j])

    barrier = pltpu.get_barrier_semaphore()

    def greet(device, tp):
        pl.semaphore_signal(
            barrier, inc=1, device_id={"ep": device, "tp": tp}, device_id_type=MESH
        )

    greet(ep, near)
    greet(ep, far)
    greet(lax.rem(ep + experts - 1, experts), x)

    greet(twin, x)
    for d in range(1, rings):
        greet(2 * (chip - y + lax.rem(y + d, rings)) + core, x)

    @pl.loop(0, experts)
    def _(i):
        s = lax.rem(ep + 1 + i, experts)

        @pl.when(s != own_index)
        def _():
            greet(s, plane)

    @pl.when(owner == 1)
    def _():
        for j in range(3):
            keep_own(j).start()

    for c in loads[1:]:
        c.start()

    after = lax.rem(ep + 1, experts)
    tail = pl.ds(length - HALO, HALO)
    halos = [
        remote(inner_hbm.at[tail], halo_inner, halo_send.at[0], halo_recv.at[0], after, x),
        remote(values_hbm.at[tail], halo_values, halo_send.at[1], halo_recv.at[1], after, x),
    ]

    at = pl.ds(pl.multiple_of(x * block, block), block)
    chosen = [routes[k : k + 1, at].astype(f32) for k in range(2)]
    expert_ids = lax.broadcasted_iota(jnp.int32, (experts, block), 0).astype(f32)
    hits = [(expert_ids == chosen[k]).astype(f32) for k in range(2)]
    earlier = (
        lax.broadcasted_iota(jnp.int32, (block, block), 0)
        < lax.broadcasted_iota(jnp.int32, (block, block), 1)
    ).astype(f32)
    rank = dot((hits[0] + hits[1]).astype(bf16), earlier.astype(bf16))
    place = [
        chosen[k] * capacity + jnp.sum(rank * hits[k], axis=0, keepdims=True) for k in range(2)
    ]
    slot_ids = lax.broadcasted_iota(jnp.int32, (slots, block), 0).astype(f32)
    pick[...] = ((slot_ids == place[0]).astype(f32) + (slot_ids == place[1]).astype(f32)).astype(
        bf16
    )

    loads[0].wait()
    scale = gain[...].reshape(1, width).astype(f32)
    step = min(16, block)

    @pl.loop(0, block // step)
    def _(i):
        r = pl.ds(pl.multiple_of(i * step, step), step)
        v = moe[r, :].astype(f32)
        square = jnp.mean(v * v, axis=-1, keepdims=True)
        group[r, :] = (v * lax.rsqrt(square + epsilon) * scale).astype(bf16)

    @pl.loop(0, width // tile)
    def _(i):
        cols = pl.ds(pl.multiple_of(i * tile, tile), tile)
        taken = dot(pick[...], group[own_rows, cols])
        outgoing[:, :, cols] = taken.reshape(experts, capacity, tile).astype(bf16)

    def send_out(e):
        cross = lax.rem(lax.rem(e, 2) + side, 2)
        return remote(
            outgoing.at[e],
            landed.at[ep],
            out_send.at[0],
            out_recv.at[0],
            2 * lax.div(e, 2) + side,
            x + (far - x) * cross,
        )

    pl.semaphore_wait(barrier, experts + 3 + rings - owner)
    for h in halos:
        h.start()

    @pl.loop(0, experts)
    def _(i):
        e = lax.rem(ep + 1 + i, experts)

        @pl.when(e != own_index)
        def _():
            send_out(e).start()

    shared_hbm = [sgate_hbm, sup_hbm, sdown_hbm]

    def held_eighth(j, i):
        n = shared_hbm[j].shape[0] // eighths
        if j < 2:
            return [sgate, sup][j].at[1, pl.ds(pl.multiple_of(i * n, n), n)]
        return sdown.at[pl.ds(pl.multiple_of(units + i * n, n), n)]

    def to_far_eighth(j):
        n = shared_hbm[j].shape[0] // eighths
        return remote(
            shared_hbm[j].at[pl.ds(pl.multiple_of(eighth * n, n), n)],
            held_eighth(j, eighth),
            eighth_send.at[j],
            eighth_recv.at[3 * eighth + j],
            ep,
            far,
        )

    def round_ring(j, d):
        return remote(
            held_eighth(j, eighth),
            held_eighth(j, eighth),
            ring_send.at[3 * d + j],
            eighth_recv.at[3 * eighth + j],
            2 * (chip - y + lax.rem(y + d, rings)) + core,
            x,
        )

    def from_ring(j, d):
        i = 2 * lax.rem(y + d, rings) + core
        return remote(
            held_eighth(j, i),
            held_eighth(j, i),
            pass_send.at[3 * d + j],
            eighth_recv.at[3 * i + j],
            twin,
            x,
        )

    def from_twin(j, d):
        i = 2 * lax.rem(y + d, rings) + 1 - core
        return remote(
            held_eighth(j, i),
            held_eighth(j, i),
            pass_send.at[3 * d + j],
            eighth_recv.at[3 * i + j],
            twin,
            x,
        )

    @pl.when(owner == 1)
    def _():
        for j in range(3):
            to_near(j).start()
        for j in range(3):
            to_twin(0, j).start()

    @pl.when(owner == 0)
    def _():
        for j in range(3):
            to_far(j).start()
        for j in range(3):
            to_far_eighth(j).start()

    def relay(j):
        @pl.when(owner == 1)
        def _():
            to_far(j).wait_recv()
            onward(j).start()
            to_twin(2, j).start()
            to_near(j).wait_recv()
            to_twin(1, j).start()

    @pl.when(owner == 1)
    def _():
        landed[ep] = outgoing[ep]

    share = [weights[k : k + 1, at] for k in range(2)]
    spread = jnp.where(slot_ids == place[0], share[0], 0.0) + jnp.where(
        slot_ids == place[1], share[1], 0.0
    )
    spread = spread.T
    high = spread.astype(bf16)
    spread_hi[...] = high
    spread_lo[...] = (spread - high.astype(f32)).astype(bf16)

    for c in loads[1:4]:
        c.wait()
    for h in halos:
        h.wait_recv()
    first = (ep > 0).astype(f32)
    product[0:HALO, :] = halo_inner[...].astype(f32) * halo_values[...].astype(f32) * first
    piece = min(64, length)

    @pl.loop(0, length // piece)
    def _(i):
        r = pl.ds(pl.multiple_of(i * piece, piece), piece)
        product[pl.ds(pl.multiple_of(HALO + i * piece, HALO), piece), :] = inner[r, :].astype(
            f32
        ) * values[r, :].astype(f32)

    tap = taps[...].astype(f32)
    for i in range(length // piece):
        lo = i * piece
        conv = tap[0:1] * product[HALO - 2 + lo : HALO - 2 + lo + piece, :]
        conv = conv + tap[1:2] * product[HALO - 1 + lo : HALO - 1 + lo + piece, :]
        conv = conv + tap[2:3] * product[HALO + lo : HALO + lo + piece, :]
        gated[lo : lo + piece, :] = (outer[lo : lo + piece, :].astype(f32) * conv).astype(bf16)
    loads[4].wait()

    @pl.loop(0, width // tile)
    def _(i):
        cols = pl.ds(pl.multiple_of(i * tile, tile), tile)
        part = dot(gated[...], outw[:, cols]).astype(bf16)
        mixer_part[:, :, cols] = part.reshape(4, block, tile)

    relay(0)

    relay(1)
    relay(2)

    def passed(j):
        @pl.when(owner == 1)
        def _():
            onward(j).wait_recv()
            to_twin(3, j).start()

    @pl.when(owner == 1)
    def _():
        for j in range(3):
            to_far_eighth(j).start()

    passed(0)


    @pl.when(owner == 1)
    def _():
        some = landed.at[pl.ds(0, experts - 1)]
        remote(some, some, out_send.at[0], out_recv.at[0], twin, x).wait_recv()

    @pl.when(owner == 0)
    def _():
        remote(landed, landed, out_send.at[0], out_recv.at[0], twin, x).wait_recv()

    half = slots // 2

    @pl.loop(0, width // tile)
    def _(i):
        cols = pl.ds(pl.multiple_of(i * tile, tile), tile)
        rows[:, cols] = landed[:, :, cols].reshape(slots, tile)

    def gate_up(k):
        cols = pl.ds(pl.multiple_of(k * units, units), units)

        @pl.loop(0, 2)
        def _(m):
            r = pl.ds(pl.multiple_of(m * half, half), half)
            g = dot(rows[r, :], wgate[k])
            u = dot(rows[r, :], wup[k])
            act[r, cols] = (g / (1.0 + jnp.exp(-g)) * u).astype(bf16)

    for k in range(3):

        @pl.when(owner == 0)
        def _():
            for j in range(2):
                to_twin(k, j).wait_recv()

        if k == 0:

            @pl.when(owner == 1)
            def _():
                for j in range(2):
                    keep_own(j).wait()

        gate_up(k)
        if k == 1:
            passed(1)

    @pl.when(owner == 0)
    def _():
        for k in range(3):
            to_twin(k, 2).wait_recv()

    @pl.when(owner == 1)
    def _():
        keep_own(2).wait()

    @pl.loop(0, width // tile)
    def _(i):
        cols = pl.ds(pl.multiple_of(i * tile, tile), tile)
        for m in range(2):
            r = pl.ds(m * half, half)
            total = dot(act[r, 0:units], wdown[0, :, cols])
            for k in range(1, 3):
                total = total + dot(act[r, k * units : (k + 1) * units], wdown[k, :, cols])
            total_down[r, cols] = total

    for j in range(2):

        @pl.when(owner == 0)
        def _():
            to_twin(3, j).wait_recv()

    gate_up(3)

    group_copy = remote(
        group.at[own_rows], group.at[near_rows], group_send.at[0], group_recv.at[0], ep, near
    )

    def first_copy(b):
        src = near if b == 0 else 3 - near
        return remote(
            mixer_part.at[src], first_in.at[b], first_send.at[b], first_recv.at[b], ep, near
        )

    second_copy = remote(
        second_out, second_in, second_send.at[0], second_recv.at[0], ep, far
    )
    shared_copy = remote(
        shared_near, shared_in, shared_send.at[0], shared_recv.at[0], ep, near
    )

    group_copy.start()
    for b in (1, 0):
        first_copy(b).start()

    for j in range(3):
        to_far_eighth(j).wait_recv()
        for d in range(1, rings):
            round_ring(j, d).start()
        from_ring(j, 0).start()

    passed(2)

    @pl.when(owner == 0)
    def _():
        to_twin(3, 2).wait_recv()

    def send_back(s):
        return remote(
            results.at[s], returned.at[mine], back_send.at[0], back_recv.at[0], s, plane
        )

    chunks = 4 if slots % 64 == 0 and experts % 4 == 0 else 1
    chunk, chunk_experts = slots // chunks, experts // chunks

    @pl.loop(0, chunks)
    def _(m):
        r = pl.ds(pl.multiple_of(m * chunk, chunk), chunk)

        @pl.loop(0, width // tile)
        def _(i):
            cols = pl.ds(pl.multiple_of(i * tile, tile), tile)
            total = total_down[r, cols] + dot(act[r, 3 * units : 4 * units], wdown[3, :, cols])
            results[pl.ds(m * chunk_experts, chunk_experts), :, cols] = total.reshape(
                chunk_experts, capacity, tile
            ).astype(bf16)

        @pl.loop(0, chunk_experts)
        def _(i):
            s = m * chunk_experts + lax.rem(ep + 1 + i, chunk_experts)

            @pl.when(s != own_index)
            def _():
                send_back(s).start()

    @pl.when(owner == 1)
    def _():
        returned[ep] = results[ep]

    for d in range(1, rings):
        for j in range(3):
            from_ring(j, d).wait_recv()
            from_ring(j, d).start()

    group_copy.wait_recv()
    for c in loads[5:8]:
        c.wait()

    def shared_gate_up(k):
        g = dot(group[...], sgate[k])
        u = dot(group[...], sup[k])
        sact[:, k * units : (k + 1) * units] = (g / (1.0 + jnp.exp(-g)) * u).astype(bf16)

    shared_gate_up(0)

    pieces = 4 if block % 64 == 0 else 1
    some_rows = block // pieces
    first_copy(1).wait_recv()

    @pl.loop(0, pieces)
    def _(i):
        r = pl.ds(pl.multiple_of(i * some_rows, some_rows), some_rows)
        second_out[r, :] = (
            mixer_part[far, r, :].astype(f32) + first_in[1, r, :].astype(f32)
        ).astype(bf16)

    second_copy.start()

    for d in range(rings):
        for j in range(3):
            from_twin(j, d).wait_recv()
    shared_gate_up(1)

    @pl.loop(0, width // tile)
    def _(i):
        cols = pl.ds(pl.multiple_of(i * tile, tile), tile)
        shared_near[:, cols] = dot(sact[near_rows, :], sdown[:, cols]).astype(bf16)

    shared_copy.start()

    @pl.loop(0, width // tile)
    def _(i):
        cols = pl.ds(pl.multiple_of(i * tile, tile), tile)
        shared_own[:, cols] = dot(sact[own_rows, :], sdown[:, cols])

    first_copy(0).wait_recv()
    second_copy.wait_recv()

    @pl.loop(0, pieces)
    def _(i):
        r = pl.ds(pl.multiple_of(i * some_rows, some_rows), some_rows)
        mixer_out[r, :] = (
            mixer_part[x, r, :].astype(f32)
            + first_in[0, r, :].astype(f32)
            + second_in[r, :].astype(f32)
        ).astype(bf16)

    shared_copy.wait_recv()

    @pl.when(owner == 1)
    def _():
        some = returned.at[pl.ds(0, experts - 1)]
        remote(some, some, back_send.at[0], back_recv.at[0], twin, x).wait_recv()

    @pl.when(owner == 0)
    def _():
        remote(returned, returned, back_send.at[0], back_recv.at[0], twin, x).wait_recv()

    @pl.loop(0, width // tile)
    def _(i):
        cols = pl.ds(pl.multiple_of(i * tile, tile), tile)
        back = returned[:, :, cols].reshape(slots, tile)
        total = shared_own[:, cols] + shared_in[:, cols].astype(f32)
        total = total + dot(spread_hi[...], back) + dot(spread_lo[...], back)
        expert_out[:, cols] = total.astype(bf16)

    for h in halos:
        h.wait_send()
    group_copy.wait_send()
    for b in range(2):
        first_copy(b).wait_send()
    second_copy.wait_send()
    shared_copy.wait_send()
    for j in range(3):
        to_far_eighth(j).wait_send()
        for d in range(rings):
            from_ring(j, d).wait_send()
            if d > 0:
                round_ring(j, d).wait_send()

    @pl.when(owner == 1)
    def _():
        for j in range(3):
            to_near(j).wait_send()
            onward(j).wait_send()
            for k in range(4):
                to_twin(k, j).wait_send()
        some = outgoing.at[pl.ds(0, experts - 1)]
        remote(some, some, out_send.at[0], out_recv.at[0], twin, x).wait_send()
        some = results.at[pl.ds(0, experts - 1)]
        remote(some, some, back_send.at[0], back_recv.at[0], twin, x).wait_send()

    @pl.when(owner == 0)
    def _():
        for j in range(3):
            to_far(j).wait_send()
        remote(outgoing, outgoing, out_send.at[0], out_recv.at[0], twin, x).wait_send()
        remote(results, results, back_send.at[0], back_recv.at[0], twin, x).wait_send()


def per_device(
    outer_gate,
    inner_gate,
    conv_values,
    conv_taps,
    out_weight,
    moe_input,
    norm_gain,
    gate_proj,
    up_proj,
    down_proj,
    shared_gate,
    shared_up,
    shared_down,
    routes,
    route_weight,
):
    experts = lax.axis_size("ep")
    length, channels = inner_gate.shape
    block, width = moe_input.shape
    units = gate_proj.shape[2]
    capacity = 2 * block * routes.shape[1] // experts
    slots = experts * capacity
    rings = 4 if experts % 8 == 0 else experts // 2
    tile = min(256, width)
    vmem = pl.BlockSpec(memory_space=pltpu.VMEM)
    hbm = pl.BlockSpec(memory_space=pl.ANY)
    dma = pltpu.SemaphoreType.DMA

    def space(*shape):
        return pltpu.VMEM(shape, bf16)

    out = jax.ShapeDtypeStruct((block, width), bf16)
    return pl.pallas_call(
        functools.partial(kernel, experts, capacity, rings, tile),
        name="whole",
        out_shape=(out, out),
        in_specs=[hbm, hbm, hbm, vmem, hbm, hbm, vmem] + [hbm] * 6 + [vmem, vmem],
        out_specs=(vmem, vmem),
        scratch_shapes=[
            space(block, width),
            space(length, channels),
            space(length, channels),
            space(length, channels),
            space(HALO, channels),
            space(HALO, channels),
            pltpu.VMEM((HALO + length, channels), f32),
            space(length, channels),
            space(channels, width),
            space(2 * block, width),
            space(experts, capacity, width),
            space(experts, capacity, width),
            space(experts, capacity, width),
            space(experts, capacity, width),
            space(slots, width),
            space(4, width, units),
            space(4, width, units),
            space(4, units, width),
            space(2, width, units),
            space(2, width, units),
            space(2 * units, width),
            space(slots, 4 * units),
            space(2 * block, 2 * units),
            space(slots, block),
            space(block, slots),
            space(block, slots),
            pltpu.VMEM((slots, width), f32),
            space(4, block, width),
            pltpu.VMEM((block, width), f32),
            space(block, width),
            space(block, width),
            space(2, block, width),
            space(block, width),
            space(block, width),
            dma((8,)),
            dma((2,)),
            dma((2,)),
            dma((1,)),
            dma((1,)),
            dma((1,)),
            dma((1,)),
            dma((3,)),
            dma((3,)),
            dma((6,)),
            dma((12,)),
            dma((12,)),
            dma((2,)),
            dma((2,)),
            dma((1,)),
            dma((1,)),
            dma((1,)),
            dma((1,)),
            dma((3,)),
            dma((3 * rings,)),
            dma((3 * rings,)),
            dma((6 * rings,)),
            dma((1,)),
            dma((1,)),
        ],
        compiler_params=pltpu.CompilerParams(
            collective_id=0, has_side_effects=True, vmem_limit_bytes=60 * 1024 * 1024
        ),
    )(
        outer_gate,
        inner_gate,
        conv_values,
        conv_taps,
        out_weight,
        moe_input,
        norm_gain,
        gate_proj,
        up_proj,
        down_proj,
        shared_gate,
        shared_up,
        shared_down,
        routes.T,
        route_weight.T,
    )


def solution(mesh):
    return jax.shard_map(
        per_device,
        mesh=mesh,
        in_specs=(
            P("ep", "tp"),
            P("ep", "tp"),
            P("ep", "tp"),
            P(None, "tp"),
            P("tp", None),
            P(("ep", "tp"), None),
            P(),
            P("ep", None, "tp"),
            P("ep", None, "tp"),
            P("ep", "tp", None),
            P(None, "tp"),
            P(None, "tp"),
            P("tp", None),
            P("ep", None),
            P("ep", None),
        ),
        out_specs=(P(("ep", "tp"), None), P(("ep", "tp"), None)),
        check_vma=False,
    )
```

```python
import functools

import jax
import jax.numpy as jnp
from jax import lax
from jax.experimental import pallas as pl
from jax.experimental.pallas import tpu as pltpu
from jax.sharding import PartitionSpec as P

MESH = pl.DeviceIdType.MESH
epsilon = 1e-06
bf16 = jnp.bfloat16
f32 = jnp.float32
HALO = 16
PIECES = 6


def remote(src, dst, send_sem, recv_sem, ep, tp):
    return pltpu.make_async_remote_copy(
        src_ref=src,
        dst_ref=dst,
        send_sem=send_sem,
        recv_sem=recv_sem,
        device_id={"ep": ep, "tp": tp},
        device_id_type=MESH,
    )


def dot(a, b):
    return jnp.dot(a, b, preferred_element_type=f32)


def kernel(
    experts,
    capacity,
    rings,
    layers,
    tile,
    outer_hbm,
    inner_hbm,
    values_hbm,
    taps,
    outw_hbm,
    moe_hbm,
    gain,
    gate_hbm,
    up_hbm,
    down_hbm,
    sgate_hbm,
    sup_hbm,
    sdown_hbm,
    routes,
    weights,
    mixer_out,
    expert_out,
    moe,
    outer,
    inner,
    values,
    halo_inner,
    halo_values,
    product,
    gated,
    outw,
    group,
    outgoing,
    landed,
    results,
    returned,
    rows,
    wgate,
    wup,
    wdown,
    sgate,
    sup,
    sdown,
    act,
    sact,
    pick,
    spread_hi,
    spread_lo,
    total_down,
    mixer_part,
    shared_own,
    shared_near,
    shared_in,
    first_in,
    second_out,
    second_in,
    load_sem,
    halo_send,
    halo_recv,
    group_send,
    group_recv,
    out_send,
    out_recv,
    own_sem,
    far_send,
    near_send,
    twin_send,
    weight_recv,
    first_send,
    first_recv,
    second_send,
    second_recv,
    shared_send,
    shared_recv,
    eighth_send,
    layer_send,
    layer_recv,
    ring_send,
    pass_send,
    eighth_recv,
    back_send,
    back_recv,
):
    ep, x = lax.axis_index("ep"), lax.axis_index("tp")
    core, chip = lax.rem(ep, 2), lax.div(ep, 2)
    near = x + 1 - 2 * lax.rem(x, 2)
    far = 3 - x
    side = lax.div(x, 2)
    owner = 1 - lax.rem(core + side, 2)
    own_index = ep * owner - (1 - owner)
    twin = ep + 1 - 2 * core
    plane = x + (far - x) * (1 - owner)
    mine = 2 * chip + side
    block, width = moe.shape
    length, channels = inner.shape
    units = sgate.shape[2]
    own_rows, near_rows = pl.ds(0, block), pl.ds(block, block)
    y = lax.rem(chip, rings)
    z = lax.div(chip, rings)
    layer = lax.rem(z, layers)
    eighths = 2 * rings
    eighth = 2 * y + core
    slots = experts * capacity

    loads = [
        (moe_hbm, moe),
        (inner_hbm, inner),
        (values_hbm, values),
        (outer_hbm, outer),
        (outw_hbm, outw),
        (sgate_hbm, sgate.at[0]),
        (sup_hbm, sup.at[0]),
        (sdown_hbm, sdown.at[pl.ds(0, units)]),
    ]
    loads = [pltpu.make_async_copy(s, d, load_sem.at[i]) for i, (s, d) in enumerate(loads)]
    loads[0].start()

    quarter = units // 4

    def own_piece(j):
        if j < 2:
            return [gate_hbm, up_hbm][j].at[0]
        return down_hbm.at[0, pl.ds((j - 2) * quarter, quarter)]

    def held_piece(k, j):
        if j < 2:
            return [wgate, wup][j].at[k]
        return wdown.at[k, pl.ds((j - 2) * quarter, quarter)]

    def weight_copy(src, k, j, send, device, tp):
        return remote(src, held_piece(k, j), send, weight_recv.at[PIECES * k + j], device, tp)

    def to_near(j):
        return weight_copy(own_piece(j), 1, j, near_send.at[j], ep, near)

    def to_far(j):
        return weight_copy(own_piece(j), 2, j, far_send.at[j], ep, far)

    def onward(j):
        return weight_copy(held_piece(2, j), 3, j, near_send.at[PIECES + j], ep, near)

    def to_twin(k, j):
        source = own_piece(j) if k == 0 else held_piece(k, j)
        return weight_copy(source, k, j, twin_send.at[PIECES * k + j], twin, x)

    def keep_own(j):
        return pltpu.make_async_copy(own_piece(j), held_piece(0, j), own_sem.at[j])

    barrier = pltpu.get_barrier_semaphore()

    def greet(device, tp):
        pl.semaphore_signal(
            barrier, inc=1, device_id={"ep": device, "tp": tp}, device_id_type=MESH
        )

    greet(ep, near)
    greet(ep, far)
    greet(lax.rem(ep + experts - 1, experts), x)

    greet(twin, x)
    sides = [1, rings - 1] if rings > 2 else [1]
    for d in sides:
        greet(2 * (chip - y + lax.rem(y + d, rings)) + core, x)
    for d in range(1, layers):
        greet(2 * ((z - layer + lax.rem(layer + d, layers)) * rings + y) + core, x)

    @pl.loop(0, experts)
    def _(i):
        s = lax.rem(ep + 1 + i, experts)

        @pl.when(s != own_index)
        def _():
            greet(s, plane)

    @pl.when(owner == 1)
    def _():
        for j in range(PIECES):
            keep_own(j).start()

    for c in loads[1:]:
        c.start()

    after = lax.rem(ep + 1, experts)
    tail = pl.ds(length - HALO, HALO)
    halos = [
        remote(inner_hbm.at[tail], halo_inner, halo_send.at[0], halo_recv.at[0], after, x),
        remote(values_hbm.at[tail], halo_values, halo_send.at[1], halo_recv.at[1], after, x),
    ]

    at = pl.ds(pl.multiple_of(x * block, block), block)
    chosen = [routes[k : k + 1, at].astype(f32) for k in range(2)]
    expert_ids = lax.broadcasted_iota(jnp.int32, (experts, block), 0).astype(f32)
    hits = [(expert_ids == chosen[k]).astype(f32) for k in range(2)]
    earlier = (
        lax.broadcasted_iota(jnp.int32, (block, block), 0)
        < lax.broadcasted_iota(jnp.int32, (block, block), 1)
    ).astype(f32)
    rank = dot((hits[0] + hits[1]).astype(bf16), earlier.astype(bf16))
    place = [
        chosen[k] * capacity + jnp.sum(rank * hits[k], axis=0, keepdims=True) for k in range(2)
    ]
    slot_ids = lax.broadcasted_iota(jnp.int32, (slots, block), 0).astype(f32)
    pick[...] = ((slot_ids == place[0]).astype(f32) + (slot_ids == place[1]).astype(f32)).astype(
        bf16
    )

    loads[0].wait()
    scale = gain[...].reshape(1, width).astype(f32)
    step = min(16, block)

    @pl.loop(0, block // step)
    def _(i):
        r = pl.ds(pl.multiple_of(i * step, step), step)
        v = moe[r, :].astype(f32)
        square = jnp.mean(v * v, axis=-1, keepdims=True)
        group[r, :] = (v * lax.rsqrt(square + epsilon) * scale).astype(bf16)

    @pl.loop(0, width // tile)
    def _(i):
        cols = pl.ds(pl.multiple_of(i * tile, tile), tile)
        taken = dot(pick[...], group[own_rows, cols])
        outgoing[:, :, cols] = taken.reshape(experts, capacity, tile).astype(bf16)

    def send_out(e):
        cross = lax.rem(lax.rem(e, 2) + side, 2)
        return remote(
            outgoing.at[e],
            landed.at[ep],
            out_send.at[0],
            out_recv.at[0],
            2 * lax.div(e, 2) + side,
            x + (far - x) * cross,
        )

    pl.semaphore_wait(barrier, experts + 3 + len(sides) + layers - owner)
    for h in halos:
        h.start()

    shared_hbm = [sgate_hbm, sup_hbm, sdown_hbm]

    def held_eighth(j, i):
        n = shared_hbm[j].shape[0] // eighths
        if j < 2:
            return [sgate, sup][j].at[1, pl.ds(pl.multiple_of(i * n, n), n)]
        return sdown.at[pl.ds(pl.multiple_of(units + i * n, n), n)]

    def held_layer(j, at_layer):
        n = shared_hbm[j].shape[0] // (eighths * layers)
        first = pl.multiple_of((eighth * layers + at_layer) * n, n)
        if j < 2:
            return [sgate, sup][j].at[1, pl.ds(first, n)]
        return sdown.at[pl.ds(pl.multiple_of(units + first, n), n)]

    def to_far_layer(j):
        n = shared_hbm[j].shape[0] // (eighths * layers)
        first = pl.multiple_of((eighth * layers + layer) * n, n)
        return remote(
            shared_hbm[j].at[pl.ds(first, n)],
            held_layer(j, layer),
            eighth_send.at[j],
            layer_recv.at[3 * layer + j],
            ep,
            far,
        )

    def layer_device(d):
        return 2 * ((z - layer + lax.rem(layer + d, layers)) * rings + y) + core

    def to_layer(j, d):
        return remote(
            held_layer(j, layer),
            held_layer(j, layer),
            layer_send.at[3 * d + j],
            layer_recv.at[3 * layer + j],
            layer_device(d),
            x,
        )

    def from_layer(j, d):
        source = lax.rem(layer + d, layers)
        return remote(
            held_layer(j, source),
            held_layer(j, source),
            layer_send.at[3 * d + j],
            layer_recv.at[3 * source + j],
            layer_device(d),
            x,
        )

    tiles = width // tile // 2

    def round_ring(j, d):
        return remote(
            held_eighth(j, eighth),
            held_eighth(j, eighth),
            ring_send.at[3 * d + j],
            eighth_recv.at[3 * eighth + j],
            2 * (chip - y + lax.rem(y + d, rings)) + core,
            x,
        )

    def opposite(j):
        d = 1 if j == 1 else rings - 1
        i = 2 * lax.rem(y + d, rings) + core
        return remote(
            held_eighth(j, i),
            held_eighth(j, i),
            ring_send.at[j],
            eighth_recv.at[3 * i + j],
            2 * (chip - y + lax.rem(y + rings - d, rings)) + core,
            x,
        )

    def from_ring(j, d):
        i = 2 * lax.rem(y + d, rings) + core
        return remote(
            held_eighth(j, i),
            held_eighth(j, i),
            pass_send.at[3 * d + j],
            eighth_recv.at[3 * i + j],
            twin,
            x,
        )

    def from_twin(j, d):
        i = 2 * lax.rem(y + d, rings) + 1 - core
        return remote(
            held_eighth(j, i),
            held_eighth(j, i),
            pass_send.at[3 * d + j],
            eighth_recv.at[3 * i + j],
            twin,
            x,
        )

    for j in range(3):
        to_far_layer(j).start()

    @pl.loop(0, experts)
    def _(i):
        e = lax.rem(ep + 1 + i, experts)

        @pl.when(e != own_index)
        def _():
            send_out(e).start()

    @pl.when(owner == 1)
    def _():
        for j in range(PIECES):
            to_near(j).start()
        for j in range(PIECES):
            to_twin(0, j).start()

    @pl.when(owner == 0)
    def _():
        for j in range(PIECES):
            to_far(j).start()

    def relay(j):
        @pl.when(owner == 1)
        def _():
            to_far(j).wait_recv()
            onward(j).start()
            to_twin(2, j).start()

    def pass_near(j):
        @pl.when(owner == 1)
        def _():
            to_near(j).wait_recv()
            to_twin(1, j).start()

    @pl.when(owner == 1)
    def _():
        landed[ep] = outgoing[ep]

    share = [weights[k : k + 1, at] for k in range(2)]
    spread = jnp.where(slot_ids == place[0], share[0], 0.0) + jnp.where(
        slot_ids == place[1], share[1], 0.0
    )
    spread = spread.T
    high = spread.astype(bf16)
    spread_hi[...] = high
    spread_lo[...] = (spread - high.astype(f32)).astype(bf16)

    for c in loads[1:4]:
        c.wait()
    for h in halos:
        h.wait_recv()
    first = (ep > 0).astype(f32)
    product[0:HALO, :] = halo_inner[...].astype(f32) * halo_values[...].astype(f32) * first
    piece = min(64, length)

    @pl.loop(0, length // piece)
    def _(i):
        r = pl.ds(pl.multiple_of(i * piece, piece), piece)
        product[pl.ds(pl.multiple_of(HALO + i * piece, HALO), piece), :] = inner[r, :].astype(
            f32
        ) * values[r, :].astype(f32)

    tap = taps[...].astype(f32)
    for i in range(length // piece):
        lo = i * piece
        conv = tap[0:1] * product[HALO - 2 + lo : HALO - 2 + lo + piece, :]
        conv = conv + tap[1:2] * product[HALO - 1 + lo : HALO - 1 + lo + piece, :]
        conv = conv + tap[2:3] * product[HALO + lo : HALO + lo + piece, :]
        gated[lo : lo + piece, :] = (outer[lo : lo + piece, :].astype(f32) * conv).astype(bf16)
    loads[4].wait()

    @pl.loop(0, width // tile)
    def _(i):
        cols = pl.ds(pl.multiple_of(i * tile, tile), tile)
        some = pl.ds(pl.multiple_of(lax.rem(i, tiles) * tile, tile), tile)
        part = dot(gated[...], outw[:, cols]).astype(bf16)
        mixer_part[lax.div(i, tiles), :, :, some] = part.reshape(4, block, tile)

    for j in range(3):
        to_far_layer(j).wait_recv()
        for d in range(1, layers):
            to_layer(j, d).start()
    pass_near(0)
    pass_near(1)
    relay(0)
    for j in range(2, PIECES):
        pass_near(j)

    relay(1)
    relay(2)
    relay(3)

    for j in range(3):
        for d in range(1, layers):
            from_layer(j, d).wait_recv()
        for d in sides:
            round_ring(j, d).start()
        from_ring(j, 0).start()
    relay(4)
    relay(5)

    def passed(j):
        @pl.when(owner == 1)
        def _():
            onward(j).wait_recv()
            to_twin(3, j).start()

    passed(0)


    @pl.when(owner == 1)
    def _():
        some = landed.at[pl.ds(0, experts - 1)]
        remote(some, some, out_send.at[0], out_recv.at[0], twin, x).wait_recv()

    @pl.when(owner == 0)
    def _():
        remote(landed, landed, out_send.at[0], out_recv.at[0], twin, x).wait_recv()

    half = slots // 2
    half_experts = experts // 2

    @pl.loop(0, width // tile)
    def _(i):
        cols = pl.ds(pl.multiple_of(i * tile, tile), tile)
        rows[:, cols] = landed[:, :, cols].reshape(slots, tile)

    def gate_up(k):
        cols = pl.ds(pl.multiple_of(k * units, units), units)

        @pl.loop(0, 2)
        def _(m):
            r = pl.ds(pl.multiple_of(m * half, half), half)
            g = dot(rows[r, :], wgate[k])
            u = dot(rows[r, :], wup[k])
            act[r, cols] = (g / (1.0 + jnp.exp(-g)) * u).astype(bf16)

    for k in range(3):

        @pl.when(owner == 0)
        def _():
            for j in range(2):
                to_twin(k, j).wait_recv()

        if k == 0:

            @pl.when(owner == 1)
            def _():
                for j in range(2):
                    keep_own(j).wait()

        gate_up(k)
        if k == 1:
            passed(1)

    @pl.when(owner == 0)
    def _():
        for k in range(3):
            for j in range(2, PIECES):
                to_twin(k, j).wait_recv()

    @pl.when(owner == 1)
    def _():
        for j in range(2, PIECES):
            keep_own(j).wait()

    @pl.loop(0, width // tile)
    def _(i):
        cols = pl.ds(pl.multiple_of(i * tile, tile), tile)
        for m in range(2):
            r = pl.ds(m * half, half)
            total = dot(act[r, 0:units], wdown[0, :, cols])
            for k in range(1, 3):
                total = total + dot(act[r, k * units : (k + 1) * units], wdown[k, :, cols])
            total_down[r, cols] = total

    for j in range(3):
        for d in sides:
            from_ring(j, d).wait_recv()
        if rings > 2:
            opposite(j).start()
        for d in sides:
            from_ring(j, d).start()

    for j in range(2):

        @pl.when(owner == 0)
        def _():
            to_twin(3, j).wait_recv()

    gate_up(3)

    group_copy = remote(
        group.at[own_rows], group.at[near_rows], group_send.at[0], group_recv.at[0], ep, near
    )

    partners = [near, far]

    def first_copy(h, b):
        src = partners[h] if b == 0 else 3 - near
        return remote(
            mixer_part.at[h, src],
            first_in.at[h, b],
            first_send.at[2 * h + b],
            first_recv.at[2 * h + b],
            ep,
            partners[h],
        )

    def second_copy(h):
        return remote(
            second_out.at[h],
            second_in.at[h],
            second_send.at[h],
            second_recv.at[h],
            ep,
            partners[1 - h],
        )

    shared_copy = remote(
        shared_near, shared_in, shared_send.at[0], shared_recv.at[0], ep, near
    )

    for j in range(2, PIECES):
        passed(j)

    @pl.when(owner == 0)
    def _():
        for j in range(2, PIECES):
            to_twin(3, j).wait_recv()

    group_copy.start()
    for b in (1, 0):
        first_copy(0, b).start()

    def send_back(s):
        return remote(
            results.at[s], returned.at[mine], back_send.at[0], back_recv.at[0], s, plane
        )

    def down(m):
        r = pl.ds(m * half, half)
        e = pl.ds(m * half_experts, half_experts)
        for i in range(width // tile):
            cols = pl.ds(i * tile, tile)
            total = total_down[r, cols] + dot(act[r, 3 * units : 4 * units], wdown[3, :, cols])
            results[e, :, cols] = total.reshape(half_experts, capacity, tile).astype(bf16)

        @pl.loop(0, half_experts)
        def _(i):
            s = m * half_experts + lax.rem(ep + 1 + i, half_experts)

            @pl.when(s != own_index)
            def _():
                send_back(s).start()

    down(0)

    down(1)

    for b in (1, 0):
        first_copy(1, b).start()

    @pl.when(owner == 1)
    def _():
        returned[ep] = results[ep]

    for d in range(2, rings - 1):
        for j in range(3):
            from_ring(j, d).wait_recv()
            from_ring(j, d).start()

    group_copy.wait_recv()
    for c in loads[5:8]:
        c.wait()

    def shared_gate_up(k):
        g = dot(group[...], sgate[k])
        u = dot(group[...], sup[k])
        sact[:, k * units : (k + 1) * units] = (g / (1.0 + jnp.exp(-g)) * u).astype(bf16)

    shared_gate_up(0)

    pieces = 4 if block % 64 == 0 else 1
    some_rows = block // pieces

    def pass_sum(h):
        first_copy(h, 1).wait_recv()

        @pl.loop(0, pieces)
        def _(i):
            r = pl.ds(pl.multiple_of(i * some_rows, some_rows), some_rows)
            second_out[h, r, :] = (
                mixer_part[h, partners[1 - h], r, :].astype(f32)
                + first_in[h, 1, r, :].astype(f32)
            ).astype(bf16)

        second_copy(h).start()

    for d in range(rings):
        for j in range(3):
            from_twin(j, d).wait_recv()
    shared_gate_up(1)

    for i in range(width // tile):
        cols = pl.ds(i * tile, tile)
        shared_near[:, cols] = dot(sact[near_rows, :], sdown[:, cols]).astype(bf16)

    shared_copy.start()

    for i in range(width // tile):
        cols = pl.ds(i * tile, tile)
        shared_own[:, cols] = dot(sact[own_rows, :], sdown[:, cols])

    pass_sum(0)
    pass_sum(1)

    for h in range(2):
        first_copy(h, 0).wait_recv()
        second_copy(h).wait_recv()

        @pl.loop(0, pieces)
        def _(i):
            r = pl.ds(pl.multiple_of(i * some_rows, some_rows), some_rows)
            mixer_out[r, h * (width // 2) : (h + 1) * (width // 2)] = (
                mixer_part[h, x, r, :].astype(f32)
                + first_in[h, 0, r, :].astype(f32)
                + second_in[h, r, :].astype(f32)
            ).astype(bf16)

    shared_copy.wait_recv()

    @pl.when(owner == 1)
    def _():
        some = returned.at[pl.ds(0, experts - 1)]
        remote(some, some, back_send.at[0], back_recv.at[0], twin, x).wait_recv()

    @pl.when(owner == 0)
    def _():
        remote(returned, returned, back_send.at[0], back_recv.at[0], twin, x).wait_recv()

    for i in range(width // tile):
        cols = pl.ds(i * tile, tile)
        back = returned[:, :, cols].reshape(slots, tile)
        total = shared_own[:, cols] + shared_in[:, cols].astype(f32)
        total = total + dot(spread_hi[...], back) + dot(spread_lo[...], back)
        expert_out[:, cols] = total.astype(bf16)

    for h in halos:
        h.wait_send()
    group_copy.wait_send()
    for h in range(2):
        for b in range(2):
            first_copy(h, b).wait_send()
        second_copy(h).wait_send()
    shared_copy.wait_send()
    for j in range(3):
        to_far_layer(j).wait_send()
        for d in range(1, layers):
            to_layer(j, d).wait_send()
        for d in range(rings):
            from_ring(j, d).wait_send()
        for d in sides:
            round_ring(j, d).wait_send()
        if rings > 2:
            opposite(j).wait_send()

    @pl.when(owner == 1)
    def _():
        for j in range(PIECES):
            to_near(j).wait_send()
            onward(j).wait_send()
            for k in range(4):
                to_twin(k, j).wait_send()
        some = outgoing.at[pl.ds(0, experts - 1)]
        remote(some, some, out_send.at[0], out_recv.at[0], twin, x).wait_send()
        some = results.at[pl.ds(0, experts - 1)]
        remote(some, some, back_send.at[0], back_recv.at[0], twin, x).wait_send()

    @pl.when(owner == 0)
    def _():
        for j in range(PIECES):
            to_far(j).wait_send()
        remote(outgoing, outgoing, out_send.at[0], out_recv.at[0], twin, x).wait_send()
        remote(results, results, back_send.at[0], back_recv.at[0], twin, x).wait_send()


def per_device(
    outer_gate,
    inner_gate,
    conv_values,
    conv_taps,
    out_weight,
    moe_input,
    norm_gain,
    gate_proj,
    up_proj,
    down_proj,
    shared_gate,
    shared_up,
    shared_down,
    routes,
    route_weight,
):
    experts = lax.axis_size("ep")
    length, channels = inner_gate.shape
    block, width = moe_input.shape
    units = gate_proj.shape[2]
    capacity = 2 * block * routes.shape[1] // experts
    slots = experts * capacity
    rings = 4 if experts % 32 == 0 else 2
    layers = min(4, experts // (2 * rings))
    tile = min(256, width)
    vmem = pl.BlockSpec(memory_space=pltpu.VMEM)
    hbm = pl.BlockSpec(memory_space=pl.ANY)
    dma = pltpu.SemaphoreType.DMA

    def space(*shape):
        return pltpu.VMEM(shape, bf16)

    out = jax.ShapeDtypeStruct((block, width), bf16)
    return pl.pallas_call(
        functools.partial(kernel, experts, capacity, rings, layers, tile),
        name="whole",
        out_shape=(out, out),
        in_specs=[hbm, hbm, hbm, vmem, hbm, hbm, vmem] + [hbm] * 6 + [vmem, vmem],
        out_specs=(vmem, vmem),
        scratch_shapes=[
            space(block, width),
            space(length, channels),
            space(length, channels),
            space(length, channels),
            space(HALO, channels),
            space(HALO, channels),
            pltpu.VMEM((HALO + length, channels), f32),
            space(length, channels),
            space(channels, width),
            space(2 * block, width),
            space(experts, capacity, width),
            space(experts, capacity, width),
            space(experts, capacity, width),
            space(experts, capacity, width),
            space(slots, width),
            space(4, width, units),
            space(4, width, units),
            space(4, units, width),
            space(2, width, units),
            space(2, width, units),
            space(2 * units, width),
            space(slots, 4 * units),
            space(2 * block, 2 * units),
            space(slots, block),
            space(block, slots),
            space(block, slots),
            pltpu.VMEM((slots, width), f32),
            space(2, 4, block, width // 2),
            pltpu.VMEM((block, width), f32),
            space(block, width),
            space(block, width),
            space(2, 2, block, width // 2),
            space(2, block, width // 2),
            space(2, block, width // 2),
            dma((8,)),
            dma((2,)),
            dma((2,)),
            dma((1,)),
            dma((1,)),
            dma((1,)),
            dma((1,)),
            dma((PIECES,)),
            dma((PIECES,)),
            dma((2 * PIECES,)),
            dma((4 * PIECES,)),
            dma((4 * PIECES,)),
            dma((4,)),
            dma((4,)),
            dma((2,)),
            dma((2,)),
            dma((1,)),
            dma((1,)),
            dma((3,)),
            dma((3 * layers,)),
            dma((3 * layers,)),
            dma((3 * rings,)),
            dma((3 * rings,)),
            dma((6 * rings,)),
            dma((1,)),
            dma((1,)),
        ],
        compiler_params=pltpu.CompilerParams(
            collective_id=0, has_side_effects=True, vmem_limit_bytes=60 * 1024 * 1024
        ),
    )(
        outer_gate,
        inner_gate,
        conv_values,
        conv_taps,
        out_weight,
        moe_input,
        norm_gain,
        gate_proj,
        up_proj,
        down_proj,
        shared_gate,
        shared_up,
        shared_down,
        routes.T,
        route_weight.T,
    )


def solution(mesh):
    return jax.shard_map(
        per_device,
        mesh=mesh,
        in_specs=(
            P("ep", "tp"),
            P("ep", "tp"),
            P("ep", "tp"),
            P(None, "tp"),
            P("tp", None),
            P(("ep", "tp"), None),
            P(),
            P("ep", None, "tp"),
            P("ep", None, "tp"),
            P("ep", "tp", None),
            P(None, "tp"),
            P(None, "tp"),
            P("tp", None),
            P("ep", None),
            P("ep", None),
        ),
        out_specs=(P(("ep", "tp"), None), P(("ep", "tp"), None)),
        check_vma=False,
    )
```

```python
import functools

import jax
import jax.numpy as jnp
from jax import lax
from jax.experimental import pallas as pl
from jax.experimental.pallas import tpu as pltpu
from jax.sharding import PartitionSpec as P

MESH = pl.DeviceIdType.MESH
epsilon = 1e-06
bf16 = jnp.bfloat16
f32 = jnp.float32
HALO = 16
PIECES = 6


def remote(src, dst, send_sem, recv_sem, ep, tp):
    return pltpu.make_async_remote_copy(
        src_ref=src,
        dst_ref=dst,
        send_sem=send_sem,
        recv_sem=recv_sem,
        device_id={"ep": ep, "tp": tp},
        device_id_type=MESH,
    )


def dot(a, b):
    return jnp.dot(a, b, preferred_element_type=f32)


def kernel(
    experts,
    capacity,
    rings,
    layers,
    tile,
    outer_hbm,
    inner_hbm,
    values_hbm,
    taps,
    outw_hbm,
    moe_hbm,
    gain,
    gate_hbm,
    up_hbm,
    down_hbm,
    sgate_hbm,
    sup_hbm,
    sdown_hbm,
    routes,
    weights,
    mixer_out,
    expert_out,
    moe,
    outer,
    inner,
    values,
    halo_inner,
    halo_values,
    product,
    gated,
    outw,
    group,
    outgoing,
    landed,
    results,
    returned,
    rows,
    wgate,
    wup,
    wdown,
    sgate,
    sup,
    sdown,
    act,
    sact,
    pick,
    spread_hi,
    spread_lo,
    total_down,
    mixer_part,
    shared_own,
    shared_near,
    shared_in,
    first_in,
    second_out,
    second_in,
    load_sem,
    halo_send,
    halo_recv,
    group_send,
    group_recv,
    out_send,
    out_recv,
    own_sem,
    far_send,
    near_send,
    twin_send,
    weight_recv,
    first_send,
    first_recv,
    second_send,
    second_recv,
    shared_send,
    shared_recv,
    eighth_send,
    layer_send,
    layer_recv,
    ring_send,
    pass_send,
    eighth_recv,
    back_send,
    back_recv,
):
    ep, x = lax.axis_index("ep"), lax.axis_index("tp")
    core, chip = lax.rem(ep, 2), lax.div(ep, 2)
    near = x + 1 - 2 * lax.rem(x, 2)
    far = 3 - x
    side = lax.div(x, 2)
    owner = 1 - lax.rem(core + side, 2)
    own_index = ep * owner - (1 - owner)
    twin = ep + 1 - 2 * core
    plane = x + (far - x) * (1 - owner)
    mine = 2 * chip + side
    block, width = moe.shape
    length, channels = inner.shape
    units = sgate.shape[2]
    own_rows, near_rows = pl.ds(0, block), pl.ds(block, block)
    y = lax.rem(chip, rings)
    z = lax.div(chip, rings)
    layer = lax.rem(z, layers)
    eighths = 2 * rings
    eighth = 2 * y + core
    slots = experts * capacity

    loads = [
        (moe_hbm, moe),
        (inner_hbm, inner),
        (values_hbm, values),
        (outer_hbm, outer),
        (outw_hbm, outw),
        (sgate_hbm, sgate.at[0]),
        (sup_hbm, sup.at[0]),
        (sdown_hbm, sdown.at[pl.ds(0, units)]),
    ]
    loads = [pltpu.make_async_copy(s, d, load_sem.at[i]) for i, (s, d) in enumerate(loads)]
    loads[0].start()

    quarter = units // 4

    def own_piece(j):
        if j < 2:
            return [gate_hbm, up_hbm][j].at[0]
        return down_hbm.at[0, pl.ds((j - 2) * quarter, quarter)]

    def held_piece(k, j):
        if j < 2:
            return [wgate, wup][j].at[k]
        return wdown.at[k, pl.ds((j - 2) * quarter, quarter)]

    def weight_copy(src, k, j, send, device, tp):
        return remote(src, held_piece(k, j), send, weight_recv.at[PIECES * k + j], device, tp)

    def to_near(j):
        return weight_copy(own_piece(j), 1, j, near_send.at[j], ep, near)

    def to_far(j):
        return weight_copy(own_piece(j), 2, j, far_send.at[j], ep, far)

    def onward(j):
        return weight_copy(held_piece(2, j), 3, j, near_send.at[PIECES + j], ep, near)

    def to_twin(k, j):
        source = own_piece(j) if k == 0 else held_piece(k, j)
        return weight_copy(source, k, j, twin_send.at[PIECES * k + j], twin, x)

    def keep_own(j):
        return pltpu.make_async_copy(own_piece(j), held_piece(0, j), own_sem.at[j])

    barrier = pltpu.get_barrier_semaphore()

    def greet(device, tp):
        pl.semaphore_signal(
            barrier, inc=1, device_id={"ep": device, "tp": tp}, device_id_type=MESH
        )

    greet(ep, near)
    greet(ep, far)
    greet(lax.rem(ep + experts - 1, experts), x)

    greet(twin, x)
    sides = [1, rings - 1] if rings > 2 else [1]
    for d in sides:
        greet(2 * (chip - y + lax.rem(y + d, rings)) + core, x)
    for d in range(1, layers):
        greet(2 * ((z - layer + lax.rem(layer + d, layers)) * rings + y) + core, x)

    @pl.loop(0, experts)
    def _(i):
        s = lax.rem(ep + 1 + i, experts)

        @pl.when(s != own_index)
        def _():
            greet(s, plane)

    @pl.when(owner == 1)
    def _():
        for j in range(PIECES):
            keep_own(j).start()

    for c in loads[1:]:
        c.start()

    after = lax.rem(ep + 1, experts)
    tail = pl.ds(length - HALO, HALO)
    halos = [
        remote(inner_hbm.at[tail], halo_inner, halo_send.at[0], halo_recv.at[0], after, x),
        remote(values_hbm.at[tail], halo_values, halo_send.at[1], halo_recv.at[1], after, x),
    ]

    at = pl.ds(pl.multiple_of(x * block, block), block)
    chosen = [routes[k : k + 1, at].astype(f32) for k in range(2)]
    expert_ids = lax.broadcasted_iota(jnp.int32, (experts, block), 0).astype(f32)
    hits = [(expert_ids == chosen[k]).astype(f32) for k in range(2)]
    earlier = (
        lax.broadcasted_iota(jnp.int32, (block, block), 0)
        < lax.broadcasted_iota(jnp.int32, (block, block), 1)
    ).astype(f32)
    rank = dot((hits[0] + hits[1]).astype(bf16), earlier.astype(bf16))
    place = [
        chosen[k] * capacity + jnp.sum(rank * hits[k], axis=0, keepdims=True) for k in range(2)
    ]
    slot_ids = lax.broadcasted_iota(jnp.int32, (slots, block), 0).astype(f32)
    pick[...] = ((slot_ids == place[0]).astype(f32) + (slot_ids == place[1]).astype(f32)).astype(
        bf16
    )

    loads[0].wait()
    scale = gain[...].reshape(1, width).astype(f32)
    step = min(16, block)

    @pl.loop(0, block // step)
    def _(i):
        r = pl.ds(pl.multiple_of(i * step, step), step)
        v = moe[r, :].astype(f32)
        square = jnp.mean(v * v, axis=-1, keepdims=True)
        group[r, :] = (v * lax.rsqrt(square + epsilon) * scale).astype(bf16)

    @pl.loop(0, width // tile)
    def _(i):
        cols = pl.ds(pl.multiple_of(i * tile, tile), tile)
        taken = dot(pick[...], group[own_rows, cols])
        outgoing[:, :, cols] = taken.reshape(experts, capacity, tile).astype(bf16)

    def spread_order(i):
        per = min(8, experts)
        deep = experts // per
        dz, dw = lax.rem(3 * lax.rem(i, deep), deep), lax.div(i, deep)
        return lax.rem(lax.div(ep, per) + dz, deep) * per + lax.rem(ep + dw, per)

    def send_out(e):
        cross = lax.rem(lax.rem(e, 2) + side, 2)
        return remote(
            outgoing.at[e],
            landed.at[ep],
            out_send.at[0],
            out_recv.at[0],
            2 * lax.div(e, 2) + side,
            x + (far - x) * cross,
        )

    pl.semaphore_wait(barrier, experts + 3 + len(sides) + layers - owner)
    for h in halos:
        h.start()

    shared_hbm = [sgate_hbm, sup_hbm, sdown_hbm]

    def held_eighth(j, i):
        n = shared_hbm[j].shape[0] // eighths
        if j < 2:
            return [sgate, sup][j].at[1, pl.ds(pl.multiple_of(i * n, n), n)]
        return sdown.at[pl.ds(pl.multiple_of(units + i * n, n), n)]

    def held_layer(j, at_layer):
        n = shared_hbm[j].shape[0] // (eighths * layers)
        first = pl.multiple_of((eighth * layers + at_layer) * n, n)
        if j < 2:
            return [sgate, sup][j].at[1, pl.ds(first, n)]
        return sdown.at[pl.ds(pl.multiple_of(units + first, n), n)]

    def to_far_layer(j):
        n = shared_hbm[j].shape[0] // (eighths * layers)
        first = pl.multiple_of((eighth * layers + layer) * n, n)
        return remote(
            shared_hbm[j].at[pl.ds(first, n)],
            held_layer(j, layer),
            eighth_send.at[j],
            layer_recv.at[3 * layer + j],
            ep,
            far,
        )

    def layer_device(d):
        return 2 * ((z - layer + lax.rem(layer + d, layers)) * rings + y) + core

    def to_layer(j, d):
        return remote(
            held_layer(j, layer),
            held_layer(j, layer),
            layer_send.at[3 * d + j],
            layer_recv.at[3 * layer + j],
            layer_device(d),
            x,
        )

    def from_layer(j, d):
        source = lax.rem(layer + d, layers)
        return remote(
            held_layer(j, source),
            held_layer(j, source),
            layer_send.at[3 * d + j],
            layer_recv.at[3 * source + j],
            layer_device(d),
            x,
        )

    tiles = width // tile // 2

    def round_ring(j, d):
        return remote(
            held_eighth(j, eighth),
            held_eighth(j, eighth),
            ring_send.at[3 * d + j],
            eighth_recv.at[3 * eighth + j],
            2 * (chip - y + lax.rem(y + d, rings)) + core,
            x,
        )

    def opposite(j):
        d = 1 if j == 1 else rings - 1
        i = 2 * lax.rem(y + d, rings) + core
        return remote(
            held_eighth(j, i),
            held_eighth(j, i),
            ring_send.at[j],
            eighth_recv.at[3 * i + j],
            2 * (chip - y + lax.rem(y + rings - d, rings)) + core,
            x,
        )

    def from_ring(j, d):
        i = 2 * lax.rem(y + d, rings) + core
        return remote(
            held_eighth(j, i),
            held_eighth(j, i),
            pass_send.at[3 * d + j],
            eighth_recv.at[3 * i + j],
            twin,
            x,
        )

    def from_twin(j, d):
        i = 2 * lax.rem(y + d, rings) + 1 - core
        return remote(
            held_eighth(j, i),
            held_eighth(j, i),
            pass_send.at[3 * d + j],
            eighth_recv.at[3 * i + j],
            twin,
            x,
        )

    for j in range(3):
        to_far_layer(j).start()

    @pl.loop(0, experts)
    def _(i):
        e = spread_order(i)

        @pl.when(e != own_index)
        def _():
            send_out(e).start()

    @pl.when(owner == 1)
    def _():
        for j in range(PIECES):
            to_near(j).start()
        for j in range(PIECES):
            to_twin(0, j).start()

    @pl.when(owner == 0)
    def _():
        for j in range(PIECES):
            to_far(j).start()

    def relay(j):
        @pl.when(owner == 1)
        def _():
            to_far(j).wait_recv()
            onward(j).start()
            to_twin(2, j).start()

    def pass_near(j):
        @pl.when(owner == 1)
        def _():
            to_near(j).wait_recv()
            to_twin(1, j).start()

    @pl.when(owner == 1)
    def _():
        landed[ep] = outgoing[ep]

    share = [weights[k : k + 1, at] for k in range(2)]
    spread = jnp.where(slot_ids == place[0], share[0], 0.0) + jnp.where(
        slot_ids == place[1], share[1], 0.0
    )
    spread = spread.T
    high = spread.astype(bf16)
    spread_hi[...] = high
    spread_lo[...] = (spread - high.astype(f32)).astype(bf16)

    for c in loads[1:4]:
        c.wait()
    for h in halos:
        h.wait_recv()
    first = (ep > 0).astype(f32)
    product[0:HALO, :] = halo_inner[...].astype(f32) * halo_values[...].astype(f32) * first
    piece = min(64, length)

    @pl.loop(0, length // piece)
    def _(i):
        r = pl.ds(pl.multiple_of(i * piece, piece), piece)
        product[pl.ds(pl.multiple_of(HALO + i * piece, HALO), piece), :] = inner[r, :].astype(
            f32
        ) * values[r, :].astype(f32)

    tap = taps[...].astype(f32)
    for i in range(length // piece):
        lo = i * piece
        conv = tap[0:1] * product[HALO - 2 + lo : HALO - 2 + lo + piece, :]
        conv = conv + tap[1:2] * product[HALO - 1 + lo : HALO - 1 + lo + piece, :]
        conv = conv + tap[2:3] * product[HALO + lo : HALO + lo + piece, :]
        gated[lo : lo + piece, :] = (outer[lo : lo + piece, :].astype(f32) * conv).astype(bf16)
    loads[4].wait()

    @pl.loop(0, width // tile)
    def _(i):
        cols = pl.ds(pl.multiple_of(i * tile, tile), tile)
        some = pl.ds(pl.multiple_of(lax.rem(i, tiles) * tile, tile), tile)
        part = dot(gated[...], outw[:, cols]).astype(bf16)
        mixer_part[lax.div(i, tiles), :, :, some] = part.reshape(4, block, tile)

    for j in range(3):
        to_far_layer(j).wait_recv()
        for d in range(1, layers):
            to_layer(j, d).start()
    pass_near(0)
    pass_near(1)
    relay(0)
    for j in range(2, PIECES):
        pass_near(j)

    relay(1)
    relay(2)
    relay(3)

    for j in range(3):
        for d in range(1, layers):
            from_layer(j, d).wait_recv()
        for d in sides:
            round_ring(j, d).start()
        from_ring(j, 0).start()
    relay(4)
    relay(5)

    def passed(j):
        @pl.when(owner == 1)
        def _():
            onward(j).wait_recv()
            to_twin(3, j).start()

    passed(0)


    @pl.when(owner == 1)
    def _():
        some = landed.at[pl.ds(0, experts - 1)]
        remote(some, some, out_send.at[0], out_recv.at[0], twin, x).wait_recv()

    @pl.when(owner == 0)
    def _():
        remote(landed, landed, out_send.at[0], out_recv.at[0], twin, x).wait_recv()

    half = slots // 2
    half_experts = experts // 2

    @pl.loop(0, width // tile)
    def _(i):
        cols = pl.ds(pl.multiple_of(i * tile, tile), tile)
        rows[:, cols] = landed[:, :, cols].reshape(slots, tile)

    def gate_up(k):
        cols = pl.ds(pl.multiple_of(k * units, units), units)

        @pl.loop(0, 2)
        def _(m):
            r = pl.ds(pl.multiple_of(m * half, half), half)
            g = dot(rows[r, :], wgate[k])
            u = dot(rows[r, :], wup[k])
            act[r, cols] = (g / (1.0 + jnp.exp(-g)) * u).astype(bf16)

    for k in range(3):

        @pl.when(owner == 0)
        def _():
            for j in range(2):
                to_twin(k, j).wait_recv()

        if k == 0:

            @pl.when(owner == 1)
            def _():
                for j in range(2):
                    keep_own(j).wait()

        gate_up(k)
        if k == 1:
            passed(1)

    @pl.when(owner == 0)
    def _():
        for k in range(3):
            for j in range(2, PIECES):
                to_twin(k, j).wait_recv()

    @pl.when(owner == 1)
    def _():
        for j in range(2, PIECES):
            keep_own(j).wait()

    @pl.loop(0, width // tile)
    def _(i):
        cols = pl.ds(pl.multiple_of(i * tile, tile), tile)
        for m in range(2):
            r = pl.ds(m * half, half)
            total = dot(act[r, 0:units], wdown[0, :, cols])
            for k in range(1, 3):
                total = total + dot(act[r, k * units : (k + 1) * units], wdown[k, :, cols])
            total_down[r, cols] = total

    for j in range(3):
        for d in sides:
            from_ring(j, d).wait_recv()
        if rings > 2:
            opposite(j).start()
        for d in sides:
            from_ring(j, d).start()

    for j in range(2):

        @pl.when(owner == 0)
        def _():
            to_twin(3, j).wait_recv()

    gate_up(3)

    group_copy = remote(
        group.at[own_rows], group.at[near_rows], group_send.at[0], group_recv.at[0], ep, near
    )

    partners = [near, far]

    def first_copy(h, b):
        src = partners[h] if b == 0 else 3 - near
        return remote(
            mixer_part.at[h, src],
            first_in.at[h, b],
            first_send.at[2 * h + b],
            first_recv.at[2 * h + b],
            ep,
            partners[h],
        )

    def second_copy(h):
        return remote(
            second_out.at[h],
            second_in.at[h],
            second_send.at[h],
            second_recv.at[h],
            ep,
            partners[1 - h],
        )

    shared_copy = remote(
        shared_near, shared_in, shared_send.at[0], shared_recv.at[0], ep, near
    )

    for j in range(2, PIECES):
        passed(j)

    @pl.when(owner == 0)
    def _():
        for j in range(2, PIECES):
            to_twin(3, j).wait_recv()

    group_copy.start()
    for b in (1, 0):
        first_copy(0, b).start()

    def send_back(s):
        return remote(
            results.at[s], returned.at[mine], back_send.at[0], back_recv.at[0], s, plane
        )

    def down(m):
        r = pl.ds(m * half, half)
        e = pl.ds(m * half_experts, half_experts)
        for i in range(width // tile):
            cols = pl.ds(i * tile, tile)
            total = total_down[r, cols] + dot(act[r, 3 * units : 4 * units], wdown[3, :, cols])
            results[e, :, cols] = total.reshape(half_experts, capacity, tile).astype(bf16)

    down(0)
    down(1)

    @pl.loop(0, experts)
    def _(i):
        s = spread_order(i)

        @pl.when(s != own_index)
        def _():
            send_back(s).start()

    for b in (1, 0):
        first_copy(1, b).start()

    @pl.when(owner == 1)
    def _():
        returned[ep] = results[ep]

    for d in range(2, rings - 1):
        for j in range(3):
            from_ring(j, d).wait_recv()
            from_ring(j, d).start()

    group_copy.wait_recv()
    for c in loads[5:8]:
        c.wait()

    def shared_gate_up(k):
        g = dot(group[...], sgate[k])
        u = dot(group[...], sup[k])
        sact[:, k * units : (k + 1) * units] = (g / (1.0 + jnp.exp(-g)) * u).astype(bf16)

    shared_gate_up(0)

    pieces = 4 if block % 64 == 0 else 1
    some_rows = block // pieces

    def pass_sum(h):
        first_copy(h, 1).wait_recv()

        @pl.loop(0, pieces)
        def _(i):
            r = pl.ds(pl.multiple_of(i * some_rows, some_rows), some_rows)
            second_out[h, r, :] = (
                mixer_part[h, partners[1 - h], r, :].astype(f32)
                + first_in[h, 1, r, :].astype(f32)
            ).astype(bf16)

        second_copy(h).start()

    for d in range(rings):
        for j in range(3):
            from_twin(j, d).wait_recv()
    shared_gate_up(1)

    for i in range(width // tile):
        cols = pl.ds(i * tile, tile)
        shared_near[:, cols] = dot(sact[near_rows, :], sdown[:, cols]).astype(bf16)

    shared_copy.start()

    for i in range(width // tile):
        cols = pl.ds(i * tile, tile)
        shared_own[:, cols] = dot(sact[own_rows, :], sdown[:, cols])

    pass_sum(0)
    pass_sum(1)

    for h in range(2):
        first_copy(h, 0).wait_recv()
        second_copy(h).wait_recv()

        @pl.loop(0, pieces)
        def _(i):
            r = pl.ds(pl.multiple_of(i * some_rows, some_rows), some_rows)
            mixer_out[r, h * (width // 2) : (h + 1) * (width // 2)] = (
                mixer_part[h, x, r, :].astype(f32)
                + first_in[h, 0, r, :].astype(f32)
                + second_in[h, r, :].astype(f32)
            ).astype(bf16)

    shared_copy.wait_recv()

    @pl.when(owner == 1)
    def _():
        some = returned.at[pl.ds(0, experts - 1)]
        remote(some, some, back_send.at[0], back_recv.at[0], twin, x).wait_recv()

    @pl.when(owner == 0)
    def _():
        remote(returned, returned, back_send.at[0], back_recv.at[0], twin, x).wait_recv()

    for i in range(width // tile):
        cols = pl.ds(i * tile, tile)
        back = returned[:, :, cols].reshape(slots, tile)
        total = shared_own[:, cols] + shared_in[:, cols].astype(f32)
        total = total + dot(spread_hi[...], back) + dot(spread_lo[...], back)
        expert_out[:, cols] = total.astype(bf16)

    for h in halos:
        h.wait_send()
    group_copy.wait_send()
    for h in range(2):
        for b in range(2):
            first_copy(h, b).wait_send()
        second_copy(h).wait_send()
    shared_copy.wait_send()
    for j in range(3):
        to_far_layer(j).wait_send()
        for d in range(1, layers):
            to_layer(j, d).wait_send()
        for d in range(rings):
            from_ring(j, d).wait_send()
        for d in sides:
            round_ring(j, d).wait_send()
        if rings > 2:
            opposite(j).wait_send()

    @pl.when(owner == 1)
    def _():
        for j in range(PIECES):
            to_near(j).wait_send()
            onward(j).wait_send()
            for k in range(4):
                to_twin(k, j).wait_send()
        some = outgoing.at[pl.ds(0, experts - 1)]
        remote(some, some, out_send.at[0], out_recv.at[0], twin, x).wait_send()
        some = results.at[pl.ds(0, experts - 1)]
        remote(some, some, back_send.at[0], back_recv.at[0], twin, x).wait_send()

    @pl.when(owner == 0)
    def _():
        for j in range(PIECES):
            to_far(j).wait_send()
        remote(outgoing, outgoing, out_send.at[0], out_recv.at[0], twin, x).wait_send()
        remote(results, results, back_send.at[0], back_recv.at[0], twin, x).wait_send()


def leave(mixer_in, expert_in, mixer_out, expert_out, mixer, expert, in_sem, out_sem):
    ins = [
        pltpu.make_async_copy(mixer_in, mixer, in_sem.at[0]),
        pltpu.make_async_copy(expert_in, expert, in_sem.at[1]),
    ]
    outs = [
        pltpu.make_async_copy(mixer, mixer_out, out_sem.at[0]),
        pltpu.make_async_copy(expert, expert_out, out_sem.at[1]),
    ]
    for c in ins:
        c.start()
    for i, o in zip(ins, outs):
        i.wait()
        o.start()
    for c in outs:
        c.wait()


def per_device(
    outer_gate,
    inner_gate,
    conv_values,
    conv_taps,
    out_weight,
    moe_input,
    norm_gain,
    gate_proj,
    up_proj,
    down_proj,
    shared_gate,
    shared_up,
    shared_down,
    routes,
    route_weight,
):
    experts = lax.axis_size("ep")
    length, channels = inner_gate.shape
    block, width = moe_input.shape
    units = gate_proj.shape[2]
    capacity = 2 * block * routes.shape[1] // experts
    slots = experts * capacity
    rings = 4 if experts % 32 == 0 else 2
    layers = min(4, experts // (2 * rings))
    tile = min(256, width)
    vmem = pl.BlockSpec(memory_space=pltpu.VMEM)
    hbm = pl.BlockSpec(memory_space=pl.ANY)
    dma = pltpu.SemaphoreType.DMA

    def space(*shape):
        return pltpu.VMEM(shape, bf16)

    out = jax.ShapeDtypeStruct((block, width), bf16)
    outs = pl.pallas_call(
        functools.partial(kernel, experts, capacity, rings, layers, tile),
        name="whole",
        out_shape=(out, out),
        in_specs=[hbm, hbm, hbm, vmem, hbm, hbm, vmem] + [hbm] * 6 + [vmem, vmem],
        out_specs=(vmem, vmem),
        scratch_shapes=[
            space(block, width),
            space(length, channels),
            space(length, channels),
            space(length, channels),
            space(HALO, channels),
            space(HALO, channels),
            pltpu.VMEM((HALO + length, channels), f32),
            space(length, channels),
            space(channels, width),
            space(2 * block, width),
            space(experts, capacity, width),
            space(experts, capacity, width),
            space(experts, capacity, width),
            space(experts, capacity, width),
            space(slots, width),
            space(4, width, units),
            space(4, width, units),
            space(4, units, width),
            space(2, width, units),
            space(2, width, units),
            space(2 * units, width),
            space(slots, 4 * units),
            space(2 * block, 2 * units),
            space(slots, block),
            space(block, slots),
            space(block, slots),
            pltpu.VMEM((slots, width), f32),
            space(2, 4, block, width // 2),
            pltpu.VMEM((block, width), f32),
            space(block, width),
            space(block, width),
            space(2, 2, block, width // 2),
            space(2, block, width // 2),
            space(2, block, width // 2),
            dma((8,)),
            dma((2,)),
            dma((2,)),
            dma((1,)),
            dma((1,)),
            dma((1,)),
            dma((1,)),
            dma((PIECES,)),
            dma((PIECES,)),
            dma((2 * PIECES,)),
            dma((4 * PIECES,)),
            dma((4 * PIECES,)),
            dma((4,)),
            dma((4,)),
            dma((2,)),
            dma((2,)),
            dma((1,)),
            dma((1,)),
            dma((3,)),
            dma((3 * layers,)),
            dma((3 * layers,)),
            dma((3 * rings,)),
            dma((3 * rings,)),
            dma((6 * rings,)),
            dma((1,)),
            dma((1,)),
        ],
        compiler_params=pltpu.CompilerParams(
            collective_id=0, has_side_effects=True, vmem_limit_bytes=60 * 1024 * 1024
        ),
    )(
        outer_gate,
        inner_gate,
        conv_values,
        conv_taps,
        out_weight,
        moe_input,
        norm_gain,
        gate_proj,
        up_proj,
        down_proj,
        shared_gate,
        shared_up,
        shared_down,
        routes.T,
        route_weight.T,
    )
    return pl.pallas_call(
        leave,
        name="leave",
        out_shape=(out, out),
        in_specs=[hbm, hbm],
        out_specs=(hbm, hbm),
        scratch_shapes=[space(block, width), space(block, width), dma((2,)), dma((2,))],
    )(*outs)


def solution(mesh):
    return jax.shard_map(
        per_device,
        mesh=mesh,
        in_specs=(
            P("ep", "tp"),
            P("ep", "tp"),
            P("ep", "tp"),
            P(None, "tp"),
            P("tp", None),
            P(("ep", "tp"), None),
            P(),
            P("ep", None, "tp"),
            P("ep", None, "tp"),
            P("ep", "tp", None),
            P(None, "tp"),
            P(None, "tp"),
            P("tp", None),
            P("ep", None),
            P("ep", None),
        ),
        out_specs=(P(("ep", "tp"), None), P(("ep", "tp"), None)),
        check_vma=False,
    )
```

```python
import functools

import jax
import jax.numpy as jnp
from jax import lax
from jax.experimental import pallas as pl
from jax.experimental.pallas import tpu as pltpu
from jax.sharding import PartitionSpec as P

MESH = pl.DeviceIdType.MESH
epsilon = 1e-06
bf16 = jnp.bfloat16
f32 = jnp.float32
HALO = 16
PIECES = 6


def remote(src, dst, send_sem, recv_sem, ep, tp):
    return pltpu.make_async_remote_copy(
        src_ref=src,
        dst_ref=dst,
        send_sem=send_sem,
        recv_sem=recv_sem,
        device_id={"ep": ep, "tp": tp},
        device_id_type=MESH,
    )


def dot(a, b):
    return jnp.dot(a, b, preferred_element_type=f32)


def kernel(
    experts,
    capacity,
    rings,
    layers,
    tile,
    outer_hbm,
    inner_hbm,
    values_hbm,
    taps,
    outw_hbm,
    moe_hbm,
    gain,
    gate_hbm,
    up_hbm,
    down_hbm,
    sgate_hbm,
    sup_hbm,
    sdown_hbm,
    routes,
    weights,
    mixer_out,
    expert_out,
    moe,
    outer,
    inner,
    values,
    halo_inner,
    halo_values,
    product,
    gated,
    outw,
    group,
    outgoing,
    landed,
    results,
    returned,
    rows,
    wgate,
    wup,
    wdown,
    sgate,
    sup,
    sdown,
    act,
    sact,
    pick,
    spread_hi,
    spread_lo,
    total_down,
    mixer_part,
    shared_own,
    shared_near,
    shared_in,
    first_in,
    second_out,
    second_in,
    load_sem,
    halo_send,
    halo_recv,
    group_send,
    group_recv,
    out_send,
    out_recv,
    own_sem,
    far_send,
    near_send,
    twin_send,
    weight_recv,
    first_send,
    first_recv,
    second_send,
    second_recv,
    shared_send,
    shared_recv,
    eighth_send,
    layer_send,
    layer_recv,
    ring_send,
    pass_send,
    eighth_recv,
    back_send,
    back_recv,
    met,
):
    ep, x = lax.axis_index("ep"), lax.axis_index("tp")
    core, chip = lax.rem(ep, 2), lax.div(ep, 2)
    near = x + 1 - 2 * lax.rem(x, 2)
    far = 3 - x
    side = lax.div(x, 2)
    owner = 1 - lax.rem(core + side, 2)
    twin = ep + 1 - 2 * core
    plane = x + (far - x) * (1 - owner)
    mine = 2 * chip + side
    block, width = moe.shape
    length, channels = inner.shape
    units = sgate.shape[2]
    own_rows, near_rows = pl.ds(0, block), pl.ds(block, block)
    y = lax.rem(chip, rings)
    z = lax.div(chip, rings)
    layer = lax.rem(z, layers)
    eighths = 2 * rings
    eighth = 2 * y + core
    slots = experts * capacity

    loads = [
        (moe_hbm, moe),
        (inner_hbm, inner),
        (values_hbm, values),
        (outer_hbm, outer),
        (outw_hbm, outw),
        (sgate_hbm, sgate.at[0]),
        (sup_hbm, sup.at[0]),
        (sdown_hbm, sdown.at[pl.ds(0, units)]),
    ]
    loads = [pltpu.make_async_copy(s, d, load_sem.at[i]) for i, (s, d) in enumerate(loads)]
    loads[0].start()

    quarter = units // 4

    def own_piece(j):
        if j < 2:
            return [gate_hbm, up_hbm][j].at[0]
        return down_hbm.at[0, pl.ds((j - 2) * quarter, quarter)]

    def held_piece(k, j):
        if j < 2:
            return [wgate, wup][j].at[k]
        return wdown.at[k, pl.ds((j - 2) * quarter, quarter)]

    def weight_copy(src, k, j, send, device, tp):
        return remote(src, held_piece(k, j), send, weight_recv.at[PIECES * k + j], device, tp)

    def to_near(j):
        return weight_copy(own_piece(j), 1, j, near_send.at[j], ep, near)

    def to_far(j):
        return weight_copy(own_piece(j), 2, j, far_send.at[j], ep, far)

    def onward(j):
        return weight_copy(held_piece(2, j), 3, j, near_send.at[PIECES + j], ep, near)

    def to_twin(k, j):
        source = own_piece(j) if k == 0 else held_piece(k, j)
        return weight_copy(source, k, j, twin_send.at[PIECES * k + j], twin, x)

    def keep_own(j):
        return pltpu.make_async_copy(own_piece(j), held_piece(0, j), own_sem.at[j])

    barrier = pltpu.get_barrier_semaphore()

    def greet(device, tp):
        pl.semaphore_signal(
            barrier, inc=1, device_id={"ep": device, "tp": tp}, device_id_type=MESH
        )

    greet(ep, near)
    greet(ep, far)
    greet(twin, x)
    sides = [1, rings - 1] if rings > 2 else [1]
    deep = experts // (2 * rings)

    def along_y(d):
        return 2 * (chip - y + lax.rem(y + d, rings)) + core

    def along_z(d):
        return ep + 2 * rings * d

    def below(d):
        return lax.div(z + deep - d, deep)

    def above(d):
        return lax.div(2 * deep - 1 - z - d, deep)

    for d in sides:
        greet(along_y(d), x)

    def tell_z(d, tell):
        @pl.when(below(d) == 1)
        def _():
            tell(along_z(-d), x)

        @pl.when(above(d) == 1)
        def _():
            tell(along_z(d), x)

    tell_z(1, greet)

    @pl.when(owner == 1)
    def _():
        for j in range(PIECES):
            keep_own(j).start()

    for c in loads[1:]:
        c.start()

    after = lax.rem(ep + 1, experts)
    tail = pl.ds(length - HALO, HALO)
    halos = [
        remote(inner_hbm.at[tail], halo_inner, halo_send.at[0], halo_recv.at[0], after, x),
        remote(values_hbm.at[tail], halo_values, halo_send.at[1], halo_recv.at[1], after, x),
    ]

    shared_hbm = [sgate_hbm, sup_hbm, sdown_hbm]

    def held_eighth(j, i):
        n = shared_hbm[j].shape[0] // eighths
        if j < 2:
            return [sgate, sup][j].at[1, pl.ds(pl.multiple_of(i * n, n), n)]
        return sdown.at[pl.ds(pl.multiple_of(units + i * n, n), n)]

    def held_layer(j, at_layer):
        n = shared_hbm[j].shape[0] // (eighths * layers)
        first = pl.multiple_of((eighth * layers + at_layer) * n, n)
        if j < 2:
            return [sgate, sup][j].at[1, pl.ds(first, n)]
        return sdown.at[pl.ds(pl.multiple_of(units + first, n), n)]

    def to_far_layer(j):
        n = shared_hbm[j].shape[0] // (eighths * layers)
        first = pl.multiple_of((eighth * layers + layer) * n, n)
        return remote(
            shared_hbm[j].at[pl.ds(first, n)],
            held_layer(j, layer),
            eighth_send.at[j],
            layer_recv.at[3 * layer + j],
            ep,
            far,
        )

    def layer_device(d):
        return 2 * ((z - layer + lax.rem(layer + d, layers)) * rings + y) + core

    def to_layer(j, d):
        return remote(
            held_layer(j, layer),
            held_layer(j, layer),
            layer_send.at[3 * d + j],
            layer_recv.at[3 * layer + j],
            layer_device(d),
            x,
        )

    def from_layer(j, d):
        source = lax.rem(layer + d, layers)
        return remote(
            held_layer(j, source),
            held_layer(j, source),
            layer_send.at[3 * d + j],
            layer_recv.at[3 * source + j],
            layer_device(d),
            x,
        )

    tiles = width // tile // 2

    def round_ring(j, d):
        return remote(
            held_eighth(j, eighth),
            held_eighth(j, eighth),
            ring_send.at[3 * d + j],
            eighth_recv.at[3 * eighth + j],
            2 * (chip - y + lax.rem(y + d, rings)) + core,
            x,
        )

    def opposite(j):
        d = 1 if j == 1 else rings - 1
        i = 2 * lax.rem(y + d, rings) + core
        return remote(
            held_eighth(j, i),
            held_eighth(j, i),
            ring_send.at[j],
            eighth_recv.at[3 * i + j],
            2 * (chip - y + lax.rem(y + rings - d, rings)) + core,
            x,
        )

    def from_ring(j, d):
        i = 2 * lax.rem(y + d, rings) + core
        return remote(
            held_eighth(j, i),
            held_eighth(j, i),
            pass_send.at[3 * d + j],
            eighth_recv.at[3 * i + j],
            twin,
            x,
        )

    def from_twin(j, d):
        i = 2 * lax.rem(y + d, rings) + 1 - core
        return remote(
            held_eighth(j, i),
            held_eighth(j, i),
            pass_send.at[3 * d + j],
            eighth_recv.at[3 * i + j],
            twin,
            x,
        )

    pl.semaphore_wait(barrier, 3 + len(sides) + below(1) + above(1))
    for j in range(3):
        to_far_layer(j).start()

    @pl.when(owner == 1)
    def _():
        for j in range(PIECES):
            to_near(j).start()
        for j in range(PIECES):
            to_twin(0, j).start()

    @pl.when(owner == 0)
    def _():
        to_far(0).start()

    stages = [None] + [sides] * (2 if rings > 2 else 1)
    stages += [d for d in (1, 2, 4) if d < deep]

    def announce(n):
        def tell(device, tp):
            pl.semaphore_signal(
                met.at[n], inc=1, device_id={"ep": device, "tp": tp}, device_id_type=MESH
            )

        if n == 0:
            tell(twin, x)
        elif isinstance(stages[n], list):
            for d in stages[n]:
                tell(along_y(d), x)
        else:
            tell_z(stages[n], tell)

    def meet(n):
        if n == 0:
            count = 1
        elif isinstance(stages[n], list):
            count = len(stages[n])
        else:
            count = below(stages[n]) + above(stages[n])
        pl.semaphore_wait(met.at[n], count)

    announce(0)

    at = pl.ds(pl.multiple_of(x * block, block), block)
    chosen = [routes[k : k + 1, at].astype(f32) for k in range(2)]
    expert_ids = lax.broadcasted_iota(jnp.int32, (experts, block), 0).astype(f32)
    hits = [(expert_ids == chosen[k]).astype(f32) for k in range(2)]
    earlier = (
        lax.broadcasted_iota(jnp.int32, (block, block), 0)
        < lax.broadcasted_iota(jnp.int32, (block, block), 1)
    ).astype(f32)
    rank = dot((hits[0] + hits[1]).astype(bf16), earlier.astype(bf16))
    place = [
        chosen[k] * capacity + jnp.sum(rank * hits[k], axis=0, keepdims=True) for k in range(2)
    ]
    slot_ids = lax.broadcasted_iota(jnp.int32, (slots, block), 0).astype(f32)
    pick[...] = ((slot_ids == place[0]).astype(f32) + (slot_ids == place[1]).astype(f32)).astype(
        bf16
    )

    meet(0)
    announce(1)

    loads[0].wait()
    scale = gain[...].reshape(1, width).astype(f32)
    step = min(16, block)

    @pl.loop(0, block // step)
    def _(i):
        r = pl.ds(pl.multiple_of(i * step, step), step)
        v = moe[r, :].astype(f32)
        square = jnp.mean(v * v, axis=-1, keepdims=True)
        group[r, :] = (v * lax.rsqrt(square + epsilon) * scale).astype(bf16)

    meet(1)
    if len(stages) > 2:
        announce(2)

    @pl.loop(0, width // tile)
    def _(i):
        cols = pl.ds(pl.multiple_of(i * tile, tile), tile)
        taken = dot(pick[...], group[own_rows, cols])
        outgoing[:, :, cols] = taken.reshape(experts, capacity, tile).astype(bf16)

    def spread_order(i):
        per = min(8, experts)
        deep = experts // per
        dz, dw = lax.rem(3 * lax.rem(i, deep), deep), lax.div(i, deep)
        return lax.rem(lax.div(ep, per) + dz, deep) * per + lax.rem(ep + dw, per)

    def source_order(i):
        per = min(8, experts)
        deep = experts // per
        dz, dw = lax.rem(3 * lax.rem(i, deep), deep), lax.div(i, deep)
        return lax.rem(lax.div(mine, per) + deep - dz, deep) * per + lax.rem(
            lax.rem(mine, per) + per - dw, per
        )

    half = slots // 2
    half_experts = experts // 2

    def send_out(i):
        e = spread_order(i)
        cross = lax.rem(lax.rem(e, 2) + side, 2)
        return remote(
            outgoing.at[e],
            landed.at[i],
            out_send.at[0],
            out_recv.at[lax.div(i, half_experts)],
            2 * lax.div(e, 2) + side,
            x + (far - x) * cross,
        )

    for n in range(2, len(stages)):
        meet(n)
        if n + 1 < len(stages):
            announce(n + 1)
    for j in range(3):
        to_far_layer(j).wait_recv()
        for d in range(1, layers):
            to_layer(j, d).start()
    for h in halos:
        h.start()

    @pl.loop(0, experts)
    def _(i):

        @pl.when(i + 1 - owner > 0)
        def _():
            send_out(i).start()

    @pl.when(owner == 0)
    def _():
        for j in range(1, PIECES):
            to_far(j).start()

    def relay(j):
        @pl.when(owner == 1)
        def _():
            to_far(j).wait_recv()
            onward(j).start()
            to_twin(2, j).start()

    def pass_near(j):
        @pl.when(owner == 1)
        def _():
            to_near(j).wait_recv()
            to_twin(1, j).start()

    @pl.when(owner == 1)
    def _():
        landed[0] = outgoing[ep]

    share = [weights[k : k + 1, at] for k in range(2)]
    spread = jnp.where(slot_ids == place[0], share[0], 0.0) + jnp.where(
        slot_ids == place[1], share[1], 0.0
    )
    spread = spread.T
    high = spread.astype(bf16)
    spread_hi[...] = high
    spread_lo[...] = (spread - high.astype(f32)).astype(bf16)

    for c in loads[1:4]:
        c.wait()
    for h in halos:
        h.wait_recv()
    first = (ep > 0).astype(f32)
    product[0:HALO, :] = halo_inner[...].astype(f32) * halo_values[...].astype(f32) * first
    piece = min(64, length)

    @pl.loop(0, length // piece)
    def _(i):
        r = pl.ds(pl.multiple_of(i * piece, piece), piece)
        product[pl.ds(pl.multiple_of(HALO + i * piece, HALO), piece), :] = inner[r, :].astype(
            f32
        ) * values[r, :].astype(f32)

    tap = taps[...].astype(f32)
    for i in range(length // piece):
        lo = i * piece
        conv = tap[0:1] * product[HALO - 2 + lo : HALO - 2 + lo + piece, :]
        conv = conv + tap[1:2] * product[HALO - 1 + lo : HALO - 1 + lo + piece, :]
        conv = conv + tap[2:3] * product[HALO + lo : HALO + lo + piece, :]
        gated[lo : lo + piece, :] = (outer[lo : lo + piece, :].astype(f32) * conv).astype(bf16)
    loads[4].wait()

    @pl.loop(0, width // tile)
    def _(i):
        cols = pl.ds(pl.multiple_of(i * tile, tile), tile)
        some = pl.ds(pl.multiple_of(lax.rem(i, tiles) * tile, tile), tile)
        part = dot(gated[...], outw[:, cols]).astype(bf16)
        mixer_part[lax.div(i, tiles), :, :, some] = part.reshape(4, block, tile)

    pass_near(0)
    pass_near(1)
    relay(0)
    for j in range(2, PIECES):
        pass_near(j)

    relay(1)
    relay(2)
    relay(3)

    for j in range(3):
        for d in range(1, layers):
            from_layer(j, d).wait_recv()
        for d in sides:
            round_ring(j, d).start()
        from_ring(j, 0).start()
    relay(4)
    relay(5)

    def passed(j):
        @pl.when(owner == 1)
        def _():
            onward(j).wait_recv()
            to_twin(3, j).start()

    passed(0)


    @pl.when(owner == 1)
    def _():
        some = landed.at[pl.ds(0, half_experts - 1)]
        remote(some, some, out_send.at[0], out_recv.at[0], twin, x).wait_recv()
        for j in range(PIECES):
            keep_own(j).wait()

    @pl.when(owner == 0)
    def _():
        some = landed.at[pl.ds(0, half_experts)]
        remote(some, some, out_send.at[0], out_recv.at[0], twin, x).wait_recv()

    def take_rows(m):
        @pl.loop(0, width // tile)
        def _(i):
            cols = pl.ds(pl.multiple_of(i * tile, tile), tile)
            rows[m * half : (m + 1) * half, cols] = landed[
                m * half_experts : (m + 1) * half_experts, :, cols
            ].reshape(half, tile)

    def gate_up(k, m):
        r = pl.ds(m * half, half)
        g = dot(rows[r, :], wgate[k])
        u = dot(rows[r, :], wup[k])
        act[r, k * units : (k + 1) * units] = (g / (1.0 + jnp.exp(-g)) * u).astype(bf16)

    take_rows(0)
    for k in range(3):

        @pl.when(owner == 0)
        def _():
            for j in range(PIECES):
                to_twin(k, j).wait_recv()

        gate_up(k, 0)
    passed(1)

    for i in range(width // tile):
        cols = pl.ds(i * tile, tile)
        total = dot(act[0:half, 0:units], wdown[0, :, cols])
        for k in range(1, 3):
            total = total + dot(act[0:half, k * units : (k + 1) * units], wdown[k, :, cols])
        total_down[:, cols] = total

    some = landed.at[pl.ds(half_experts, half_experts)]
    remote(some, some, out_send.at[0], out_recv.at[1], twin, x).wait_recv()
    take_rows(1)
    for k in range(3):
        gate_up(k, 1)

    for j in range(3):
        for d in sides:
            from_ring(j, d).wait_recv()
        if rings > 2:
            opposite(j).start()
        for d in sides:
            from_ring(j, d).start()

    for j in range(2):

        @pl.when(owner == 0)
        def _():
            to_twin(3, j).wait_recv()

    gate_up(3, 0)
    gate_up(3, 1)

    group_copy = remote(
        group.at[own_rows], group.at[near_rows], group_send.at[0], group_recv.at[0], ep, near
    )

    partners = [near, far]

    def first_copy(h, b):
        src = partners[h] if b == 0 else 3 - near
        return remote(
            mixer_part.at[h, src],
            first_in.at[h, b],
            first_send.at[2 * h + b],
            first_recv.at[2 * h + b],
            ep,
            partners[h],
        )

    def second_copy(h):
        return remote(
            second_out.at[h],
            second_in.at[h],
            second_send.at[h],
            second_recv.at[h],
            ep,
            partners[1 - h],
        )

    shared_copy = remote(
        shared_near, shared_in, shared_send.at[0], shared_recv.at[0], ep, near
    )

    for j in range(2, PIECES):
        passed(j)

    @pl.when(owner == 0)
    def _():
        for j in range(2, PIECES):
            to_twin(3, j).wait_recv()

    group_copy.start()
    for b in (1, 0):
        first_copy(0, b).start()

    def send_back(i):
        return remote(
            results.at[i],
            returned.at[mine],
            back_send.at[0],
            back_recv.at[0],
            source_order(i),
            plane,
        )

    def down(m):
        r = pl.ds(m * half, half)
        for i in range(width // tile):
            cols = pl.ds(i * tile, tile)
            total = dot(act[r, 3 * units : 4 * units], wdown[3, :, cols])
            if m == 0:
                total = total + total_down[:, cols]
            else:
                for k in range(3):
                    total = total + dot(act[r, k * units : (k + 1) * units], wdown[k, :, cols])
            results[m * half_experts : (m + 1) * half_experts, :, cols] = total.reshape(
                half_experts, capacity, tile
            ).astype(bf16)

        @pl.loop(m * half_experts, (m + 1) * half_experts)
        def _(i):
            @pl.when(i + 1 - owner > 0)
            def _():
                send_back(i).start()

    down(0)
    down(1)

    for b in (1, 0):
        first_copy(1, b).start()

    @pl.when(owner == 1)
    def _():
        returned[ep] = results[0]

    for d in range(2, rings - 1):
        for j in range(3):
            from_ring(j, d).wait_recv()
            from_ring(j, d).start()

    group_copy.wait_recv()
    for c in loads[5:8]:
        c.wait()

    def shared_gate_up(k):
        g = dot(group[...], sgate[k])
        u = dot(group[...], sup[k])
        sact[:, k * units : (k + 1) * units] = (g / (1.0 + jnp.exp(-g)) * u).astype(bf16)

    shared_gate_up(0)

    pieces = 4 if block % 64 == 0 else 1
    some_rows = block // pieces

    def pass_sum(h):
        first_copy(h, 1).wait_recv()

        @pl.loop(0, pieces)
        def _(i):
            r = pl.ds(pl.multiple_of(i * some_rows, some_rows), some_rows)
            second_out[h, r, :] = (
                mixer_part[h, partners[1 - h], r, :].astype(f32)
                + first_in[h, 1, r, :].astype(f32)
            ).astype(bf16)

        second_copy(h).start()

    for d in range(rings):
        for j in range(3):
            from_twin(j, d).wait_recv()
    shared_gate_up(1)

    for i in range(width // tile):
        cols = pl.ds(i * tile, tile)
        shared_near[:, cols] = dot(sact[near_rows, :], sdown[:, cols]).astype(bf16)

    shared_copy.start()

    for i in range(width // tile):
        cols = pl.ds(i * tile, tile)
        shared_own[:, cols] = dot(sact[own_rows, :], sdown[:, cols])

    pass_sum(0)
    pass_sum(1)

    for h in range(2):
        first_copy(h, 0).wait_recv()
        second_copy(h).wait_recv()

        @pl.loop(0, pieces)
        def _(i):
            r = pl.ds(pl.multiple_of(i * some_rows, some_rows), some_rows)
            mixer_out[r, h * (width // 2) : (h + 1) * (width // 2)] = (
                mixer_part[h, x, r, :].astype(f32)
                + first_in[h, 0, r, :].astype(f32)
                + second_in[h, r, :].astype(f32)
            ).astype(bf16)

    shared_copy.wait_recv()

    @pl.when(owner == 1)
    def _():
        some = returned.at[pl.ds(0, experts - 1)]
        remote(some, some, back_send.at[0], back_recv.at[0], twin, x).wait_recv()

    @pl.when(owner == 0)
    def _():
        remote(returned, returned, back_send.at[0], back_recv.at[0], twin, x).wait_recv()

    for i in range(width // tile):
        cols = pl.ds(i * tile, tile)
        back = returned[:, :, cols].reshape(slots, tile)
        total = shared_own[:, cols] + shared_in[:, cols].astype(f32)
        total = total + dot(spread_hi[...], back) + dot(spread_lo[...], back)
        expert_out[:, cols] = total.astype(bf16)

    for h in halos:
        h.wait_send()
    group_copy.wait_send()
    for h in range(2):
        for b in range(2):
            first_copy(h, b).wait_send()
        second_copy(h).wait_send()
    shared_copy.wait_send()
    for j in range(3):
        to_far_layer(j).wait_send()
        for d in range(1, layers):
            to_layer(j, d).wait_send()
        for d in range(rings):
            from_ring(j, d).wait_send()
        for d in sides:
            round_ring(j, d).wait_send()
        if rings > 2:
            opposite(j).wait_send()

    @pl.when(owner == 1)
    def _():
        for j in range(PIECES):
            to_near(j).wait_send()
            onward(j).wait_send()
            for k in range(4):
                to_twin(k, j).wait_send()
        some = outgoing.at[pl.ds(0, experts - 1)]
        remote(some, some, out_send.at[0], out_recv.at[0], twin, x).wait_send()
        some = results.at[pl.ds(0, experts - 1)]
        remote(some, some, back_send.at[0], back_recv.at[0], twin, x).wait_send()

    @pl.when(owner == 0)
    def _():
        for j in range(PIECES):
            to_far(j).wait_send()
        remote(outgoing, outgoing, out_send.at[0], out_recv.at[0], twin, x).wait_send()
        remote(results, results, back_send.at[0], back_recv.at[0], twin, x).wait_send()


def leave(mixer_in, expert_in, mixer_out, expert_out, mixer, expert, in_sem, out_sem):
    ins = [
        pltpu.make_async_copy(mixer_in, mixer, in_sem.at[0]),
        pltpu.make_async_copy(expert_in, expert, in_sem.at[1]),
    ]
    outs = [
        pltpu.make_async_copy(mixer, mixer_out, out_sem.at[0]),
        pltpu.make_async_copy(expert, expert_out, out_sem.at[1]),
    ]
    for c in ins:
        c.start()
    for i, o in zip(ins, outs):
        i.wait()
        o.start()
    for c in outs:
        c.wait()


def per_device(
    outer_gate,
    inner_gate,
    conv_values,
    conv_taps,
    out_weight,
    moe_input,
    norm_gain,
    gate_proj,
    up_proj,
    down_proj,
    shared_gate,
    shared_up,
    shared_down,
    routes,
    route_weight,
):
    experts = lax.axis_size("ep")
    length, channels = inner_gate.shape
    block, width = moe_input.shape
    units = gate_proj.shape[2]
    capacity = 2 * block * routes.shape[1] // experts
    slots = experts * capacity
    rings = 4 if experts % 32 == 0 else 2
    layers = min(2, experts // (2 * rings))
    tile = min(256, width)
    vmem = pl.BlockSpec(memory_space=pltpu.VMEM)
    hbm = pl.BlockSpec(memory_space=pl.ANY)
    dma = pltpu.SemaphoreType.DMA

    def space(*shape):
        return pltpu.VMEM(shape, bf16)

    out = jax.ShapeDtypeStruct((block, width), bf16)
    outs = pl.pallas_call(
        functools.partial(kernel, experts, capacity, rings, layers, tile),
        name="whole",
        out_shape=(out, out),
        in_specs=[hbm, hbm, hbm, vmem, hbm, hbm, vmem] + [hbm] * 6 + [vmem, vmem],
        out_specs=(vmem, vmem),
        scratch_shapes=[
            space(block, width),
            space(length, channels),
            space(length, channels),
            space(length, channels),
            space(HALO, channels),
            space(HALO, channels),
            pltpu.VMEM((HALO + length, channels), f32),
            space(length, channels),
            space(channels, width),
            space(2 * block, width),
            space(experts, capacity, width),
            space(experts, capacity, width),
            space(experts, capacity, width),
            space(experts, capacity, width),
            space(slots, width),
            space(4, width, units),
            space(4, width, units),
            space(4, units, width),
            space(2, width, units),
            space(2, width, units),
            space(2 * units, width),
            space(slots, 4 * units),
            space(2 * block, 2 * units),
            space(slots, block),
            space(block, slots),
            space(block, slots),
            pltpu.VMEM((slots // 2, width), f32),
            space(2, 4, block, width // 2),
            pltpu.VMEM((block, width), f32),
            space(block, width),
            space(block, width),
            space(2, 2, block, width // 2),
            space(2, block, width // 2),
            space(2, block, width // 2),
            dma((8,)),
            dma((2,)),
            dma((2,)),
            dma((1,)),
            dma((1,)),
            dma((1,)),
            dma((2,)),
            dma((PIECES,)),
            dma((PIECES,)),
            dma((2 * PIECES,)),
            dma((4 * PIECES,)),
            dma((4 * PIECES,)),
            dma((4,)),
            dma((4,)),
            dma((2,)),
            dma((2,)),
            dma((1,)),
            dma((1,)),
            dma((3,)),
            dma((3 * layers,)),
            dma((3 * layers,)),
            dma((3 * rings,)),
            dma((3 * rings,)),
            dma((6 * rings,)),
            dma((1,)),
            dma((1,)),
            pltpu.SemaphoreType.REGULAR((8,)),
        ],
        compiler_params=pltpu.CompilerParams(
            collective_id=0, has_side_effects=True, vmem_limit_bytes=60 * 1024 * 1024
        ),
    )(
        outer_gate,
        inner_gate,
        conv_values,
        conv_taps,
        out_weight,
        moe_input,
        norm_gain,
        gate_proj,
        up_proj,
        down_proj,
        shared_gate,
        shared_up,
        shared_down,
        routes.T,
        route_weight.T,
    )
    return pl.pallas_call(
        leave,
        name="leave",
        out_shape=(out, out),
        in_specs=[hbm, hbm],
        out_specs=(hbm, hbm),
        scratch_shapes=[space(block, width), space(block, width), dma((2,)), dma((2,))],
    )(*outs)


def solution(mesh):
    return jax.shard_map(
        per_device,
        mesh=mesh,
        in_specs=(
            P("ep", "tp"),
            P("ep", "tp"),
            P("ep", "tp"),
            P(None, "tp"),
            P("tp", None),
            P(("ep", "tp"), None),
            P(),
            P("ep", None, "tp"),
            P("ep", None, "tp"),
            P("ep", "tp", None),
            P(None, "tp"),
            P(None, "tp"),
            P("tp", None),
            P("ep", None),
            P("ep", None),
        ),
        out_specs=(P(("ep", "tp"), None), P(("ep", "tp"), None)),
        check_vma=False,
    )
```

```python
import functools

import jax
import jax.numpy as jnp
from jax import lax
from jax.experimental import pallas as pl
from jax.experimental.pallas import tpu as pltpu
from jax.sharding import PartitionSpec as P

MESH = pl.DeviceIdType.MESH
epsilon = 1e-06
bf16 = jnp.bfloat16
f32 = jnp.float32
HALO = 16
PIECES = 7


def remote(src, dst, send_sem, recv_sem, ep, tp):
    return pltpu.make_async_remote_copy(
        src_ref=src,
        dst_ref=dst,
        send_sem=send_sem,
        recv_sem=recv_sem,
        device_id={"ep": ep, "tp": tp},
        device_id_type=MESH,
    )


def dot(a, b):
    return jnp.dot(a, b, preferred_element_type=f32)


def kernel(
    experts,
    capacity,
    rings,
    layers,
    tile,
    outer_hbm,
    inner_hbm,
    values_hbm,
    taps_hbm,
    outw_hbm,
    moe_hbm,
    gain_hbm,
    gate_hbm,
    up_hbm,
    down_hbm,
    sgate_hbm,
    sup_hbm,
    sdown_hbm,
    routes_hbm,
    weights_hbm,
    mixer_out,
    expert_out,
    moe,
    outer,
    inner,
    values,
    halo_inner,
    halo_values,
    product,
    gated,
    outw,
    group,
    outgoing,
    landed,
    results,
    returned,
    rows,
    wgate,
    wup,
    wdown,
    sgate,
    sup,
    sdown,
    act,
    sact,
    pick,
    spread_hi,
    spread_lo,
    total_down,
    mixer_part,
    shared_own,
    shared_near,
    shared_in,
    first_in,
    second_out,
    second_in,
    load_sem,
    halo_send,
    halo_recv,
    group_send,
    group_recv,
    out_send,
    out_recv,
    own_sem,
    far_send,
    near_send,
    twin_send,
    weight_recv,
    first_send,
    first_recv,
    second_send,
    second_recv,
    shared_send,
    shared_recv,
    eighth_send,
    layer_send,
    layer_recv,
    ring_send,
    pass_send,
    eighth_recv,
    back_send,
    back_recv,
    met,
    taps,
    gain,
    routes,
    weights,
    small_sem,
):
    ep, x = lax.axis_index("ep"), lax.axis_index("tp")
    core, chip = lax.rem(ep, 2), lax.div(ep, 2)
    near = x + 1 - 2 * lax.rem(x, 2)
    far = 3 - x
    side = lax.div(x, 2)
    owner = 1 - lax.rem(core + side, 2)
    twin = ep + 1 - 2 * core
    plane = x + (far - x) * (1 - owner)
    mine = 2 * chip + side
    block, width = moe.shape
    length, channels = inner.shape
    units = sgate.shape[2]
    own_rows, near_rows = pl.ds(0, block), pl.ds(block, block)
    y = lax.rem(chip, rings)
    z = lax.div(chip, rings)
    layer = lax.rem(z, layers)
    eighths = 2 * rings
    eighth = 2 * y + core
    slots = experts * capacity

    loads = [
        (moe_hbm, moe),
        (inner_hbm, inner),
        (values_hbm, values),
        (outer_hbm, outer),
        (outw_hbm, outw),
        (sgate_hbm, sgate.at[0]),
        (sup_hbm, sup.at[0]),
        (sdown_hbm, sdown.at[pl.ds(0, units)]),
    ]
    loads = [pltpu.make_async_copy(s, d, load_sem.at[i]) for i, (s, d) in enumerate(loads)]
    loads[0].start()
    small = [(routes_hbm, routes), (gain_hbm, gain), (weights_hbm, weights), (taps_hbm, taps)]
    small = [pltpu.make_async_copy(s, d, small_sem.at[i]) for i, (s, d) in enumerate(small)]

    cuts = [units * c // 8 for c in (0, 2, 4, 6, 7, 8)]

    def down_rows(j):
        return pl.ds(cuts[j - 2], cuts[j - 1] - cuts[j - 2])

    def own_piece(j):
        if j < 2:
            return [gate_hbm, up_hbm][j].at[0]
        return down_hbm.at[0, down_rows(j)]

    def held_piece(k, j):
        if j < 2:
            return [wgate, wup][j].at[k]
        return wdown.at[k, down_rows(j)]

    def weight_copy(src, k, j, send, device, tp):
        return remote(src, held_piece(k, j), send, weight_recv.at[PIECES * k + j], device, tp)

    def to_near(j):
        return weight_copy(own_piece(j), 1, j, near_send.at[j], ep, near)

    def to_far(j):
        return weight_copy(own_piece(j), 2, j, far_send.at[j], ep, far)

    def onward(j):
        return weight_copy(held_piece(2, j), 3, j, near_send.at[PIECES + j], ep, near)

    def to_twin(k, j):
        source = own_piece(j) if k == 0 else held_piece(k, j)
        return weight_copy(source, k, j, twin_send.at[PIECES * k + j], twin, x)

    def keep_own(j):
        return pltpu.make_async_copy(own_piece(j), held_piece(0, j), own_sem.at[j])

    barrier = pltpu.get_barrier_semaphore()

    def greet(device, tp):
        pl.semaphore_signal(
            barrier, inc=1, device_id={"ep": device, "tp": tp}, device_id_type=MESH
        )

    greet(ep, near)
    greet(ep, far)
    greet(twin, x)
    sides = [1, rings - 1] if rings > 2 else [1]
    deep = experts // (2 * rings)

    def along_y(d):
        return 2 * (chip - y + lax.rem(y + d, rings)) + core

    def along_z(d):
        return ep + 2 * rings * d

    def below(d):
        return lax.div(z + deep - d, deep)

    def above(d):
        return lax.div(2 * deep - 1 - z - d, deep)

    ring = list(range(1, rings))
    for d in ring:
        greet(along_y(d), x)

    def tell_z(d, tell):
        @pl.when(below(d) == 1)
        def _():
            tell(along_z(-d), x)

        @pl.when(above(d) == 1)
        def _():
            tell(along_z(d), x)

    tell_z(1, greet)

    @pl.when(owner == 1)
    def _():
        for j in range(PIECES):
            keep_own(j).start()

    for c in small + loads[1:]:
        c.start()

    after = lax.rem(ep + 1, experts)
    tail = pl.ds(length - HALO, HALO)
    halos = [
        remote(inner_hbm.at[tail], halo_inner, halo_send.at[0], halo_recv.at[0], after, x),
        remote(values_hbm.at[tail], halo_values, halo_send.at[1], halo_recv.at[1], after, x),
    ]

    shared_hbm = [sgate_hbm, sup_hbm, sdown_hbm]

    def held_eighth(j, i):
        n = shared_hbm[j].shape[0] // eighths
        if j < 2:
            return [sgate, sup][j].at[1, pl.ds(pl.multiple_of(i * n, n), n)]
        return sdown.at[pl.ds(pl.multiple_of(units + i * n, n), n)]

    def held_layer(j, at_layer):
        n = shared_hbm[j].shape[0] // (eighths * layers)
        first = pl.multiple_of((eighth * layers + at_layer) * n, n)
        if j < 2:
            return [sgate, sup][j].at[1, pl.ds(first, n)]
        return sdown.at[pl.ds(pl.multiple_of(units + first, n), n)]

    def to_far_layer(j):
        n = shared_hbm[j].shape[0] // (eighths * layers)
        first = pl.multiple_of((eighth * layers + layer) * n, n)
        return remote(
            shared_hbm[j].at[pl.ds(first, n)],
            held_layer(j, layer),
            eighth_send.at[j],
            layer_recv.at[3 * layer + j],
            ep,
            far,
        )

    def layer_device(d):
        return 2 * ((z - layer + lax.rem(layer + d, layers)) * rings + y) + core

    def to_layer(j, d):
        return remote(
            held_layer(j, layer),
            held_layer(j, layer),
            layer_send.at[3 * d + j],
            layer_recv.at[3 * layer + j],
            layer_device(d),
            x,
        )

    def from_layer(j, d):
        source = lax.rem(layer + d, layers)
        return remote(
            held_layer(j, source),
            held_layer(j, source),
            layer_send.at[3 * d + j],
            layer_recv.at[3 * source + j],
            layer_device(d),
            x,
        )

    tiles = width // tile // 2

    def round_ring(j, d):
        return remote(
            held_eighth(j, eighth),
            held_eighth(j, eighth),
            ring_send.at[3 * d + j],
            eighth_recv.at[3 * eighth + j],
            2 * (chip - y + lax.rem(y + d, rings)) + core,
            x,
        )

    def opposite(j):
        d = 1 if j == 1 else rings - 1
        i = 2 * lax.rem(y + d, rings) + core
        return remote(
            held_eighth(j, i),
            held_eighth(j, i),
            ring_send.at[j],
            eighth_recv.at[3 * i + j],
            2 * (chip - y + lax.rem(y + rings - d, rings)) + core,
            x,
        )

    def from_ring(j, d):
        i = 2 * lax.rem(y + d, rings) + core
        return remote(
            held_eighth(j, i),
            held_eighth(j, i),
            pass_send.at[3 * d + j],
            eighth_recv.at[3 * i + j],
            twin,
            x,
        )

    def from_twin(j, d):
        i = 2 * lax.rem(y + d, rings) + 1 - core
        return remote(
            held_eighth(j, i),
            held_eighth(j, i),
            pass_send.at[3 * d + j],
            eighth_recv.at[3 * i + j],
            twin,
            x,
        )

    pl.semaphore_wait(barrier, 3 + len(ring) + below(1) + above(1))
    for j in range(3):
        to_far_layer(j).start()

    @pl.when(owner == 1)
    def _():
        for j in range(PIECES):
            to_near(j).start()
        for j in range(PIECES):
            to_twin(0, j).start()

    @pl.when(owner == 0)
    def _():
        to_far(0).start()

    stages = [None, ring]
    stages += [d for d in (1, 2, 4) if d < deep]

    def announce(n):
        def tell(device, tp):
            pl.semaphore_signal(
                met.at[n], inc=1, device_id={"ep": device, "tp": tp}, device_id_type=MESH
            )

        if n == 0:
            tell(twin, x)
        elif isinstance(stages[n], list):
            for d in stages[n]:
                tell(along_y(d), x)
        else:
            tell_z(stages[n], tell)

    def meet(n):
        if n == 0:
            count = 1
        elif isinstance(stages[n], list):
            count = len(stages[n])
        else:
            count = below(stages[n]) + above(stages[n])
        pl.semaphore_wait(met.at[n], count)

    announce(0)

    small[0].wait()
    at = pl.ds(pl.multiple_of(x * block, block), block)
    chosen = [routes[k : k + 1, at].astype(f32) for k in range(2)]
    expert_ids = lax.broadcasted_iota(jnp.int32, (experts, block), 0).astype(f32)
    hits = [(expert_ids == chosen[k]).astype(f32) for k in range(2)]
    earlier = (
        lax.broadcasted_iota(jnp.int32, (block, block), 0)
        < lax.broadcasted_iota(jnp.int32, (block, block), 1)
    ).astype(f32)
    rank = dot((hits[0] + hits[1]).astype(bf16), earlier.astype(bf16))
    place = [
        chosen[k] * capacity + jnp.sum(rank * hits[k], axis=0, keepdims=True) for k in range(2)
    ]
    slot_ids = lax.broadcasted_iota(jnp.int32, (slots, block), 0).astype(f32)
    pick[...] = ((slot_ids == place[0]).astype(f32) + (slot_ids == place[1]).astype(f32)).astype(
        bf16
    )

    meet(0)
    announce(1)

    loads[0].wait()
    small[1].wait()
    scale = gain[...].reshape(1, width).astype(f32)
    step = min(16, block)

    @pl.loop(0, block // step)
    def _(i):
        r = pl.ds(pl.multiple_of(i * step, step), step)
        v = moe[r, :].astype(f32)
        square = jnp.mean(v * v, axis=-1, keepdims=True)
        group[r, :] = (v * lax.rsqrt(square + epsilon) * scale).astype(bf16)

    meet(1)
    if len(stages) > 2:
        announce(2)

    @pl.loop(0, width // tile)
    def _(i):
        cols = pl.ds(pl.multiple_of(i * tile, tile), tile)
        taken = dot(pick[...], group[own_rows, cols])
        outgoing[:, :, cols] = taken.reshape(experts, capacity, tile).astype(bf16)

    def spread_order(i):
        per = min(8, experts)
        deep = experts // per
        dz, dw = lax.rem(3 * lax.rem(i, deep), deep), lax.div(i, deep)
        return lax.rem(lax.div(ep, per) + dz, deep) * per + lax.rem(ep + dw, per)

    def source_order(i):
        per = min(8, experts)
        deep = experts // per
        dz, dw = lax.rem(3 * lax.rem(i, deep), deep), lax.div(i, deep)
        return lax.rem(lax.div(mine, per) + deep - dz, deep) * per + lax.rem(
            lax.rem(mine, per) + per - dw, per
        )

    half = slots // 2
    half_experts = experts // 2

    def send_out(i):
        e = spread_order(i)
        cross = lax.rem(lax.rem(e, 2) + side, 2)
        return remote(
            outgoing.at[e],
            landed.at[i],
            out_send.at[0],
            out_recv.at[lax.div(i, half_experts)],
            2 * lax.div(e, 2) + side,
            x + (far - x) * cross,
        )

    for n in range(2, len(stages)):
        meet(n)
        if n + 1 < len(stages):
            announce(n + 1)
    for j in range(3):
        to_far_layer(j).wait_recv()
        for d in range(1, layers):
            to_layer(j, d).start()
    for h in halos:
        h.start()

    @pl.loop(0, experts)
    def _(i):

        @pl.when(i + 1 - owner > 0)
        def _():
            send_out(i).start()

    @pl.when(owner == 0)
    def _():
        for j in range(1, PIECES):
            to_far(j).start()

    def relay(j):
        @pl.when(owner == 1)
        def _():
            to_far(j).wait_recv()
            onward(j).start()
            to_twin(2, j).start()

    def pass_near(j):
        @pl.when(owner == 1)
        def _():
            to_near(j).wait_recv()
            to_twin(1, j).start()

    @pl.when(owner == 1)
    def _():
        landed[0] = outgoing[ep]

    small[2].wait()
    share = [weights[k : k + 1, at] for k in range(2)]
    spread = jnp.where(slot_ids == place[0], share[0], 0.0) + jnp.where(
        slot_ids == place[1], share[1], 0.0
    )
    spread = spread.T
    high = spread.astype(bf16)
    spread_hi[...] = high
    spread_lo[...] = (spread - high.astype(f32)).astype(bf16)

    for c in loads[1:4] + small[3:]:
        c.wait()
    for h in halos:
        h.wait_recv()
    first = (ep > 0).astype(f32)
    product[0:HALO, :] = halo_inner[...].astype(f32) * halo_values[...].astype(f32) * first
    piece = min(64, length)

    @pl.loop(0, length // piece)
    def _(i):
        r = pl.ds(pl.multiple_of(i * piece, piece), piece)
        product[pl.ds(pl.multiple_of(HALO + i * piece, HALO), piece), :] = inner[r, :].astype(
            f32
        ) * values[r, :].astype(f32)

    tap = taps[...].astype(f32)
    for i in range(length // piece):
        lo = i * piece
        conv = tap[0:1] * product[HALO - 2 + lo : HALO - 2 + lo + piece, :]
        conv = conv + tap[1:2] * product[HALO - 1 + lo : HALO - 1 + lo + piece, :]
        conv = conv + tap[2:3] * product[HALO + lo : HALO + lo + piece, :]
        gated[lo : lo + piece, :] = (outer[lo : lo + piece, :].astype(f32) * conv).astype(bf16)
    loads[4].wait()

    @pl.loop(0, width // tile)
    def _(i):
        cols = pl.ds(pl.multiple_of(i * tile, tile), tile)
        some = pl.ds(pl.multiple_of(lax.rem(i, tiles) * tile, tile), tile)
        part = dot(gated[...], outw[:, cols]).astype(bf16)
        mixer_part[lax.div(i, tiles), :, :, some] = part.reshape(4, block, tile)

    pass_near(0)
    pass_near(1)
    relay(0)
    for j in range(2, PIECES):
        pass_near(j)

    relay(1)
    relay(2)
    relay(3)

    for j in range(3):
        for d in range(1, layers):
            from_layer(j, d).wait_recv()
        for d in sides:
            round_ring(j, d).start()
        from_ring(j, 0).start()
    for j in range(4, PIECES):
        relay(j)

    def passed(j):
        @pl.when(owner == 1)
        def _():
            onward(j).wait_recv()
            to_twin(3, j).start()

    passed(0)


    @pl.when(owner == 1)
    def _():
        some = landed.at[pl.ds(0, half_experts - 1)]
        remote(some, some, out_send.at[0], out_recv.at[0], twin, x).wait_recv()
        for j in range(PIECES):
            keep_own(j).wait()

    @pl.when(owner == 0)
    def _():
        some = landed.at[pl.ds(0, half_experts)]
        remote(some, some, out_send.at[0], out_recv.at[0], twin, x).wait_recv()

    def take_rows(m):
        @pl.loop(0, width // tile)
        def _(i):
            cols = pl.ds(pl.multiple_of(i * tile, tile), tile)
            rows[m * half : (m + 1) * half, cols] = landed[
                m * half_experts : (m + 1) * half_experts, :, cols
            ].reshape(half, tile)

    def gate_up(k, m):
        r = pl.ds(m * half, half)
        g = dot(rows[r, :], wgate[k])
        u = dot(rows[r, :], wup[k])
        act[r, k * units : (k + 1) * units] = (g / (1.0 + jnp.exp(-g)) * u).astype(bf16)

    take_rows(0)
    for k in range(3):

        @pl.when(owner == 0)
        def _():
            for j in range(PIECES):
                to_twin(k, j).wait_recv()

        gate_up(k, 0)
    passed(1)

    for i in range(width // tile):
        cols = pl.ds(i * tile, tile)
        total = dot(act[0:half, 0:units], wdown[0, :, cols])
        for k in range(1, 3):
            total = total + dot(act[0:half, k * units : (k + 1) * units], wdown[k, :, cols])
        total_down[:, cols] = total

    some = landed.at[pl.ds(half_experts, half_experts)]
    remote(some, some, out_send.at[0], out_recv.at[1], twin, x).wait_recv()
    take_rows(1)
    for k in range(3):
        gate_up(k, 1)

    for j in range(3):
        for d in sides:
            from_ring(j, d).wait_recv()
        if rings > 2:
            opposite(j).start()
        for d in sides:
            from_ring(j, d).start()

    for j in range(2):

        @pl.when(owner == 0)
        def _():
            to_twin(3, j).wait_recv()

    gate_up(3, 0)
    gate_up(3, 1)

    group_copy = remote(
        group.at[own_rows], group.at[near_rows], group_send.at[0], group_recv.at[0], ep, near
    )

    partners = [near, far]

    def first_copy(h, b):
        src = partners[h] if b == 0 else 3 - near
        return remote(
            mixer_part.at[h, src],
            first_in.at[h, b],
            first_send.at[2 * h + b],
            first_recv.at[2 * h + b],
            ep,
            partners[h],
        )

    def second_copy(h):
        return remote(
            second_out.at[h],
            second_in.at[h],
            second_send.at[h],
            second_recv.at[h],
            ep,
            partners[1 - h],
        )

    shared_copy = remote(
        shared_near, shared_in, shared_send.at[0], shared_recv.at[0], ep, near
    )

    for j in range(2, PIECES):
        passed(j)

    @pl.when(owner == 0)
    def _():
        for j in range(2, PIECES):
            to_twin(3, j).wait_recv()

    group_copy.start()
    for b in (1, 0):
        first_copy(0, b).start()

    def send_back(i):
        return remote(
            results.at[i],
            returned.at[mine],
            back_send.at[0],
            back_recv.at[0],
            source_order(i),
            plane,
        )

    def down(m):
        r = pl.ds(m * half, half)
        for i in range(width // tile):
            cols = pl.ds(i * tile, tile)
            total = dot(act[r, 3 * units : 4 * units], wdown[3, :, cols])
            if m == 0:
                total = total + total_down[:, cols]
            else:
                for k in range(3):
                    total = total + dot(act[r, k * units : (k + 1) * units], wdown[k, :, cols])
            results[m * half_experts : (m + 1) * half_experts, :, cols] = total.reshape(
                half_experts, capacity, tile
            ).astype(bf16)

        @pl.loop(m * half_experts, (m + 1) * half_experts)
        def _(i):
            @pl.when(i + 1 - owner > 0)
            def _():
                send_back(i).start()

    down(0)
    down(1)

    for b in (1, 0):
        first_copy(1, b).start()

    @pl.when(owner == 1)
    def _():
        returned[ep] = results[0]

    for d in range(2, rings - 1):
        for j in range(3):
            from_ring(j, d).wait_recv()
            from_ring(j, d).start()

    group_copy.wait_recv()
    for c in loads[5:8]:
        c.wait()

    def shared_gate_up(k):
        g = dot(group[...], sgate[k])
        u = dot(group[...], sup[k])
        sact[:, k * units : (k + 1) * units] = (g / (1.0 + jnp.exp(-g)) * u).astype(bf16)

    shared_gate_up(0)

    pieces = 4 if block % 64 == 0 else 1
    some_rows = block // pieces

    def pass_sum(h):
        first_copy(h, 1).wait_recv()

        @pl.loop(0, pieces)
        def _(i):
            r = pl.ds(pl.multiple_of(i * some_rows, some_rows), some_rows)
            second_out[h, r, :] = (
                mixer_part[h, partners[1 - h], r, :].astype(f32)
                + first_in[h, 1, r, :].astype(f32)
            ).astype(bf16)

        second_copy(h).start()

    for d in range(rings):
        for j in range(3):
            from_twin(j, d).wait_recv()
    shared_gate_up(1)

    for i in range(width // tile):
        cols = pl.ds(i * tile, tile)
        shared_near[:, cols] = dot(sact[near_rows, :], sdown[:, cols]).astype(bf16)

    shared_copy.start()

    for i in range(width // tile):
        cols = pl.ds(i * tile, tile)
        shared_own[:, cols] = dot(sact[own_rows, :], sdown[:, cols])

    pass_sum(0)
    pass_sum(1)

    for h in range(2):
        first_copy(h, 0).wait_recv()
        second_copy(h).wait_recv()

        @pl.loop(0, pieces)
        def _(i):
            r = pl.ds(pl.multiple_of(i * some_rows, some_rows), some_rows)
            mixer_out[r, h * (width // 2) : (h + 1) * (width // 2)] = (
                mixer_part[h, x, r, :].astype(f32)
                + first_in[h, 0, r, :].astype(f32)
                + second_in[h, r, :].astype(f32)
            ).astype(bf16)

    shared_copy.wait_recv()

    @pl.when(owner == 1)
    def _():
        some = returned.at[pl.ds(0, experts - 1)]
        remote(some, some, back_send.at[0], back_recv.at[0], twin, x).wait_recv()

    @pl.when(owner == 0)
    def _():
        remote(returned, returned, back_send.at[0], back_recv.at[0], twin, x).wait_recv()

    for i in range(width // tile):
        cols = pl.ds(i * tile, tile)
        back = returned[:, :, cols].reshape(slots, tile)
        total = shared_own[:, cols] + shared_in[:, cols].astype(f32)
        total = total + dot(spread_hi[...], back) + dot(spread_lo[...], back)
        expert_out[:, cols] = total.astype(bf16)

    for h in halos:
        h.wait_send()
    group_copy.wait_send()
    for h in range(2):
        for b in range(2):
            first_copy(h, b).wait_send()
        second_copy(h).wait_send()
    shared_copy.wait_send()
    for j in range(3):
        to_far_layer(j).wait_send()
        for d in range(1, layers):
            to_layer(j, d).wait_send()
        for d in range(rings):
            from_ring(j, d).wait_send()
        for d in sides:
            round_ring(j, d).wait_send()
        if rings > 2:
            opposite(j).wait_send()

    @pl.when(owner == 1)
    def _():
        for j in range(PIECES):
            to_near(j).wait_send()
            onward(j).wait_send()
            for k in range(4):
                to_twin(k, j).wait_send()
        some = outgoing.at[pl.ds(0, experts - 1)]
        remote(some, some, out_send.at[0], out_recv.at[0], twin, x).wait_send()
        some = results.at[pl.ds(0, experts - 1)]
        remote(some, some, back_send.at[0], back_recv.at[0], twin, x).wait_send()

    @pl.when(owner == 0)
    def _():
        for j in range(PIECES):
            to_far(j).wait_send()
        remote(outgoing, outgoing, out_send.at[0], out_recv.at[0], twin, x).wait_send()
        remote(results, results, back_send.at[0], back_recv.at[0], twin, x).wait_send()


def leave(mixer, expert, mixer_out, expert_out, sem):
    copies = [
        pltpu.make_async_copy(mixer, mixer_out, sem.at[0]),
        pltpu.make_async_copy(expert, expert_out, sem.at[1]),
    ]
    for c in copies:
        c.start()
    for c in copies:
        c.wait()


def per_device(
    outer_gate,
    inner_gate,
    conv_values,
    conv_taps,
    out_weight,
    moe_input,
    norm_gain,
    gate_proj,
    up_proj,
    down_proj,
    shared_gate,
    shared_up,
    shared_down,
    routes,
    route_weight,
):
    experts = lax.axis_size("ep")
    length, channels = inner_gate.shape
    block, width = moe_input.shape
    units = gate_proj.shape[2]
    capacity = 2 * block * routes.shape[1] // experts
    slots = experts * capacity
    rings = 4 if experts % 32 == 0 else 2
    layers = min(2, experts // (2 * rings))
    tile = min(256, width)
    vmem = pl.BlockSpec(memory_space=pltpu.VMEM)
    hbm = pl.BlockSpec(memory_space=pl.ANY)
    dma = pltpu.SemaphoreType.DMA

    def space(*shape):
        return pltpu.VMEM(shape, bf16)

    out = jax.ShapeDtypeStruct((block, width), bf16)
    outs = pl.pallas_call(
        functools.partial(kernel, experts, capacity, rings, layers, tile),
        name="whole",
        out_shape=(pltpu.VMEM(out.shape, bf16), pltpu.VMEM(out.shape, bf16)),
        in_specs=[hbm] * 15,
        out_specs=(vmem, vmem),
        scratch_shapes=[
            space(block, width),
            space(length, channels),
            space(length, channels),
            space(length, channels),
            space(HALO, channels),
            space(HALO, channels),
            pltpu.VMEM((HALO + length, channels), f32),
            space(length, channels),
            space(channels, width),
            space(2 * block, width),
            space(experts, capacity, width),
            space(experts, capacity, width),
            space(experts, capacity, width),
            space(experts, capacity, width),
            space(slots, width),
            space(4, width, units),
            space(4, width, units),
            space(4, units, width),
            space(2, width, units),
            space(2, width, units),
            space(2 * units, width),
            space(slots, 4 * units),
            space(2 * block, 2 * units),
            space(slots, block),
            space(block, slots),
            space(block, slots),
            pltpu.VMEM((slots // 2, width), f32),
            space(2, 4, block, width // 2),
            pltpu.VMEM((block, width), f32),
            space(block, width),
            space(block, width),
            space(2, 2, block, width // 2),
            space(2, block, width // 2),
            space(2, block, width // 2),
            dma((8,)),
            dma((2,)),
            dma((2,)),
            dma((1,)),
            dma((1,)),
            dma((1,)),
            dma((2,)),
            dma((PIECES,)),
            dma((PIECES,)),
            dma((2 * PIECES,)),
            dma((4 * PIECES,)),
            dma((4 * PIECES,)),
            dma((4,)),
            dma((4,)),
            dma((2,)),
            dma((2,)),
            dma((1,)),
            dma((1,)),
            dma((3,)),
            dma((3 * layers,)),
            dma((3 * layers,)),
            dma((3 * rings,)),
            dma((3 * rings,)),
            dma((6 * rings,)),
            dma((1,)),
            dma((1,)),
            pltpu.SemaphoreType.REGULAR((8,)),
            space(*conv_taps.shape),
            space(width),
            pltpu.VMEM(routes.shape[::-1], jnp.int32),
            pltpu.VMEM(route_weight.shape[::-1], f32),
            dma((4,)),
        ],
        compiler_params=pltpu.CompilerParams(
            collective_id=0, has_side_effects=True, vmem_limit_bytes=60 * 1024 * 1024
        ),
    )(
        outer_gate,
        inner_gate,
        conv_values,
        conv_taps,
        out_weight,
        moe_input,
        norm_gain,
        gate_proj,
        up_proj,
        down_proj,
        shared_gate,
        shared_up,
        shared_down,
        routes.T,
        route_weight.T,
    )
    return pl.pallas_call(
        leave,
        name="leave",
        out_shape=(out, out),
        in_specs=[vmem, vmem],
        out_specs=(hbm, hbm),
        scratch_shapes=[dma((2,))],
    )(*[pltpu.with_memory_space_constraint(o, pltpu.VMEM) for o in outs])


def solution(mesh):
    return jax.shard_map(
        per_device,
        mesh=mesh,
        in_specs=(
            P("ep", "tp"),
            P("ep", "tp"),
            P("ep", "tp"),
            P(None, "tp"),
            P("tp", None),
            P(("ep", "tp"), None),
            P(),
            P("ep", None, "tp"),
            P("ep", None, "tp"),
            P("ep", "tp", None),
            P(None, "tp"),
            P(None, "tp"),
            P("tp", None),
            P("ep", None),
            P("ep", None),
        ),
        out_specs=(P(("ep", "tp"), None), P(("ep", "tp"), None)),
        check_vma=False,
    )
```

```python
import functools

import jax
import jax.numpy as jnp
from jax import lax
from jax.experimental import pallas as pl
from jax.experimental.pallas import tpu as pltpu
from jax.sharding import PartitionSpec as P

MESH = pl.DeviceIdType.MESH
epsilon = 1e-06
bf16 = jnp.bfloat16
f32 = jnp.float32
HALO = 16
PIECES = 7


def remote(src, dst, send_sem, recv_sem, ep, tp):
    return pltpu.make_async_remote_copy(
        src_ref=src,
        dst_ref=dst,
        send_sem=send_sem,
        recv_sem=recv_sem,
        device_id={"ep": ep, "tp": tp},
        device_id_type=MESH,
    )


def dot(a, b):
    return jnp.dot(a, b, preferred_element_type=f32)


def kernel(
    experts,
    capacity,
    rings,
    layers,
    tile,
    outer_hbm,
    inner_hbm,
    values_hbm,
    taps_hbm,
    outw_hbm,
    moe_hbm,
    gain_hbm,
    gate_hbm,
    up_hbm,
    down_hbm,
    sgate_hbm,
    sup_hbm,
    sdown_hbm,
    routes_hbm,
    weights_hbm,
    mixer_out,
    expert_out,
    moe,
    outer,
    inner,
    values,
    halo_inner,
    halo_values,
    product,
    gated,
    outw,
    group,
    outgoing,
    landed,
    results,
    returned,
    rows,
    wgate,
    wup,
    wdown,
    sgate,
    sup,
    sdown,
    act,
    sact,
    pick,
    spread_hi,
    spread_lo,
    total_down,
    mixer_part,
    shared_own,
    shared_near,
    shared_in,
    first_in,
    second_out,
    second_in,
    load_sem,
    halo_send,
    halo_recv,
    group_send,
    group_recv,
    out_send,
    out_recv,
    own_sem,
    far_send,
    near_send,
    twin_send,
    weight_recv,
    first_send,
    first_recv,
    second_send,
    second_recv,
    shared_send,
    shared_recv,
    eighth_send,
    layer_send,
    layer_recv,
    ring_send,
    pass_send,
    eighth_recv,
    back_send,
    back_recv,
    met,
    taps,
    gain,
    routes,
    weights,
    small_sem,
):
    ep, x = lax.axis_index("ep"), lax.axis_index("tp")
    core, chip = lax.rem(ep, 2), lax.div(ep, 2)
    near = x + 1 - 2 * lax.rem(x, 2)
    far = 3 - x
    side = lax.div(x, 2)
    owner = 1 - lax.rem(core + side, 2)
    twin = ep + 1 - 2 * core
    plane = x + (far - x) * (1 - owner)
    mine = 2 * chip + side
    block, width = moe.shape
    length, channels = inner.shape
    units = sgate.shape[2]
    own_rows, near_rows = pl.ds(0, block), pl.ds(block, block)
    y = lax.rem(chip, rings)
    z = lax.div(chip, rings)
    layer = lax.rem(z, layers)
    eighths = 2 * rings
    eighth = 2 * y + core
    slots = experts * capacity

    loads = [
        (moe_hbm, moe),
        (inner_hbm, inner),
        (values_hbm, values),
        (outer_hbm, outer),
        (outw_hbm, outw),
        (sgate_hbm, sgate.at[0]),
        (sup_hbm, sup.at[0]),
        (sdown_hbm, sdown.at[pl.ds(0, units)]),
    ]
    loads = [pltpu.make_async_copy(s, d, load_sem.at[i]) for i, (s, d) in enumerate(loads)]
    loads[0].start()
    small = [(routes_hbm, routes), (gain_hbm, gain), (weights_hbm, weights), (taps_hbm, taps)]
    small = [pltpu.make_async_copy(s, d, small_sem.at[i]) for i, (s, d) in enumerate(small)]

    cuts = [units * c // 8 for c in (0, 2, 4, 6, 7, 8)]

    def down_rows(j):
        return pl.ds(cuts[j - 2], cuts[j - 1] - cuts[j - 2])

    def own_piece(j):
        if j < 2:
            return [gate_hbm, up_hbm][j].at[0]
        return down_hbm.at[0, down_rows(j)]

    def held_piece(k, j):
        if j < 2:
            return [wgate, wup][j].at[k]
        return wdown.at[k, down_rows(j)]

    def weight_copy(src, k, j, send, device, tp):
        return remote(src, held_piece(k, j), send, weight_recv.at[PIECES * k + j], device, tp)

    def to_near(j):
        return weight_copy(own_piece(j), 1, j, near_send.at[j], ep, near)

    def to_far(j):
        return weight_copy(own_piece(j), 2, j, far_send.at[j], ep, far)

    def onward(j):
        return weight_copy(held_piece(2, j), 3, j, near_send.at[PIECES + j], ep, near)

    def to_twin(k, j):
        source = own_piece(j) if k == 0 else held_piece(k, j)
        return weight_copy(source, k, j, twin_send.at[PIECES * k + j], twin, x)

    def keep_own(j):
        return pltpu.make_async_copy(own_piece(j), held_piece(0, j), own_sem.at[j])

    barrier = pltpu.get_barrier_semaphore()

    def greet(device, tp):
        pl.semaphore_signal(
            barrier, inc=1, device_id={"ep": device, "tp": tp}, device_id_type=MESH
        )

    greet(ep, near)
    greet(ep, far)
    greet(twin, x)
    sides = [1, rings - 1] if rings > 2 else [1]
    deep = experts // (2 * rings)

    def along_y(d):
        return 2 * (chip - y + lax.rem(y + d, rings)) + core

    def along_z(d):
        return ep + 2 * rings * d

    def below(d):
        return lax.div(z + deep - d, deep)

    def above(d):
        return lax.div(2 * deep - 1 - z - d, deep)

    ring = list(range(1, rings))
    for d in ring:
        greet(along_y(d), x)

    def tell_z(d, tell):
        @pl.when(below(d) == 1)
        def _():
            tell(along_z(-d), x)

        @pl.when(above(d) == 1)
        def _():
            tell(along_z(d), x)

    tell_z(1, greet)

    @pl.when(owner == 1)
    def _():
        for j in range(PIECES):
            keep_own(j).start()

    for c in small + loads[1:]:
        c.start()

    after = lax.rem(ep + 1, experts)
    tail = pl.ds(length - HALO, HALO)
    halos = [
        remote(inner_hbm.at[tail], halo_inner, halo_send.at[0], halo_recv.at[0], after, x),
        remote(values_hbm.at[tail], halo_values, halo_send.at[1], halo_recv.at[1], after, x),
    ]

    shared_hbm = [sgate_hbm, sup_hbm, sdown_hbm]

    def held_eighth(j, i):
        n = shared_hbm[j].shape[0] // eighths
        if j < 2:
            return [sgate, sup][j].at[1, pl.ds(pl.multiple_of(i * n, n), n)]
        return sdown.at[pl.ds(pl.multiple_of(units + i * n, n), n)]

    def held_layer(j, at_layer):
        n = shared_hbm[j].shape[0] // (eighths * layers)
        first = pl.multiple_of((eighth * layers + at_layer) * n, n)
        if j < 2:
            return [sgate, sup][j].at[1, pl.ds(first, n)]
        return sdown.at[pl.ds(pl.multiple_of(units + first, n), n)]

    def to_far_layer(j):
        n = shared_hbm[j].shape[0] // (eighths * layers)
        first = pl.multiple_of((eighth * layers + layer) * n, n)
        return remote(
            shared_hbm[j].at[pl.ds(first, n)],
            held_layer(j, layer),
            eighth_send.at[j],
            layer_recv.at[3 * layer + j],
            ep,
            far,
        )

    def layer_device(d):
        return 2 * ((z - layer + lax.rem(layer + d, layers)) * rings + y) + core

    def to_layer(j, d):
        return remote(
            held_layer(j, layer),
            held_layer(j, layer),
            layer_send.at[3 * d + j],
            layer_recv.at[3 * layer + j],
            layer_device(d),
            x,
        )

    def from_layer(j, d):
        source = lax.rem(layer + d, layers)
        return remote(
            held_layer(j, source),
            held_layer(j, source),
            layer_send.at[3 * d + j],
            layer_recv.at[3 * source + j],
            layer_device(d),
            x,
        )

    tiles = width // tile // 2

    def round_ring(j, d):
        return remote(
            held_eighth(j, eighth),
            held_eighth(j, eighth),
            ring_send.at[3 * d + j],
            eighth_recv.at[3 * eighth + j],
            2 * (chip - y + lax.rem(y + d, rings)) + core,
            x,
        )

    def opposite(j):
        d = 1 if j == 1 else rings - 1
        i = 2 * lax.rem(y + d, rings) + core
        return remote(
            held_eighth(j, i),
            held_eighth(j, i),
            ring_send.at[j],
            eighth_recv.at[3 * i + j],
            2 * (chip - y + lax.rem(y + rings - d, rings)) + core,
            x,
        )

    def from_ring(j, d):
        i = 2 * lax.rem(y + d, rings) + core
        return remote(
            held_eighth(j, i),
            held_eighth(j, i),
            pass_send.at[3 * d + j],
            eighth_recv.at[3 * i + j],
            twin,
            x,
        )

    def from_twin(j, d):
        i = 2 * lax.rem(y + d, rings) + 1 - core
        return remote(
            held_eighth(j, i),
            held_eighth(j, i),
            pass_send.at[3 * d + j],
            eighth_recv.at[3 * i + j],
            twin,
            x,
        )

    pl.semaphore_wait(barrier, 3 + len(ring) + below(1) + above(1))
    for j in range(3):
        to_far_layer(j).start()

    @pl.when(owner == 1)
    def _():
        for j in range(PIECES):
            to_near(j).start()
        for j in range(PIECES):
            to_twin(0, j).start()

    @pl.when(owner == 0)
    def _():
        to_far(0).start()

    stages = [None, ring]
    stages += [d for d in (1, 2, 4) if d < deep]

    def announce(n):
        def tell(device, tp):
            pl.semaphore_signal(
                met.at[n], inc=1, device_id={"ep": device, "tp": tp}, device_id_type=MESH
            )

        if n == 0:
            tell(twin, x)
        elif isinstance(stages[n], list):
            for d in stages[n]:
                tell(along_y(d), x)
        else:
            tell_z(stages[n], tell)

    def meet(n):
        if n == 0:
            count = 1
        elif isinstance(stages[n], list):
            count = len(stages[n])
        else:
            count = below(stages[n]) + above(stages[n])
        pl.semaphore_wait(met.at[n], count)

    announce(0)

    small[0].wait()
    at = pl.ds(pl.multiple_of(x * block, block), block)
    chosen = [routes[k : k + 1, at].astype(f32) for k in range(2)]
    expert_ids = lax.broadcasted_iota(jnp.int32, (experts, block), 0).astype(f32)
    hits = [(expert_ids == chosen[k]).astype(f32) for k in range(2)]
    earlier = (
        lax.broadcasted_iota(jnp.int32, (block, block), 0)
        < lax.broadcasted_iota(jnp.int32, (block, block), 1)
    ).astype(f32)
    rank = dot((hits[0] + hits[1]).astype(bf16), earlier.astype(bf16))
    place = [
        chosen[k] * capacity + jnp.sum(rank * hits[k], axis=0, keepdims=True) for k in range(2)
    ]
    slot_ids = lax.broadcasted_iota(jnp.int32, (slots, block), 0).astype(f32)
    pick[...] = ((slot_ids == place[0]).astype(f32) + (slot_ids == place[1]).astype(f32)).astype(
        bf16
    )

    meet(0)
    announce(1)

    loads[0].wait()
    small[1].wait()
    scale = gain[...].reshape(1, width).astype(f32)
    step = min(16, block)

    @pl.loop(0, block // step)
    def _(i):
        r = pl.ds(pl.multiple_of(i * step, step), step)
        v = moe[r, :].astype(f32)
        square = jnp.mean(v * v, axis=-1, keepdims=True)
        group[r, :] = (v * lax.rsqrt(square + epsilon) * scale).astype(bf16)

    meet(1)
    if len(stages) > 2:
        announce(2)

    @pl.loop(0, width // tile)
    def _(i):
        cols = pl.ds(pl.multiple_of(i * tile, tile), tile)
        taken = dot(pick[...], group[own_rows, cols])
        outgoing[:, :, cols] = taken.reshape(experts, capacity, tile).astype(bf16)

    def spread_order(i):
        per = min(8, experts)
        deep = experts // per
        dz, dw = lax.rem(3 * lax.rem(i, deep), deep), lax.div(i, deep)
        return lax.rem(lax.div(ep, per) + dz, deep) * per + lax.rem(ep + dw, per)

    def source_order(i):
        per = min(8, experts)
        deep = experts // per
        dz, dw = lax.rem(3 * lax.rem(i, deep), deep), lax.div(i, deep)
        return lax.rem(lax.div(mine, per) + deep - dz, deep) * per + lax.rem(
            lax.rem(mine, per) + per - dw, per
        )

    half = slots // 2
    half_experts = experts // 2

    def send_out(i):
        e = spread_order(i)
        cross = lax.rem(lax.rem(e, 2) + side, 2)
        return remote(
            outgoing.at[e],
            landed.at[i],
            out_send.at[0],
            out_recv.at[lax.div(i, half_experts)],
            2 * lax.div(e, 2) + side,
            x + (far - x) * cross,
        )

    for n in range(2, len(stages)):
        meet(n)
        if n + 1 < len(stages):
            announce(n + 1)
    for j in range(3):
        to_far_layer(j).wait_recv()
        for d in range(1, layers):
            to_layer(j, d).start()
    for h in halos:
        h.start()

    @pl.loop(0, experts, unroll=8)
    def _(i):
        @pl.when(i + 1 - owner > 0)
        def _():
            send_out(i).start()

    @pl.when(owner == 0)
    def _():
        for j in range(1, PIECES):
            to_far(j).start()

    def relay(j):
        @pl.when(owner == 1)
        def _():
            to_far(j).wait_recv()
            onward(j).start()
            to_twin(2, j).start()

    def pass_near(j):
        @pl.when(owner == 1)
        def _():
            to_near(j).wait_recv()
            to_twin(1, j).start()

    @pl.when(owner == 1)
    def _():
        landed[0] = outgoing[ep]

    small[2].wait()
    share = [weights[k : k + 1, at] for k in range(2)]
    spread = jnp.where(slot_ids == place[0], share[0], 0.0) + jnp.where(
        slot_ids == place[1], share[1], 0.0
    )
    spread = spread.T
    high = spread.astype(bf16)
    spread_hi[...] = high
    spread_lo[...] = (spread - high.astype(f32)).astype(bf16)

    for c in loads[1:4] + small[3:]:
        c.wait()
    for h in halos:
        h.wait_recv()
    first = (ep > 0).astype(f32)
    product[0:HALO, :] = halo_inner[...].astype(f32) * halo_values[...].astype(f32) * first
    piece = min(64, length)

    @pl.loop(0, length // piece)
    def _(i):
        r = pl.ds(pl.multiple_of(i * piece, piece), piece)
        product[pl.ds(pl.multiple_of(HALO + i * piece, HALO), piece), :] = inner[r, :].astype(
            f32
        ) * values[r, :].astype(f32)

    tap = taps[...].astype(f32)
    for i in range(length // piece):
        lo = i * piece
        conv = tap[0:1] * product[HALO - 2 + lo : HALO - 2 + lo + piece, :]
        conv = conv + tap[1:2] * product[HALO - 1 + lo : HALO - 1 + lo + piece, :]
        conv = conv + tap[2:3] * product[HALO + lo : HALO + lo + piece, :]
        gated[lo : lo + piece, :] = (outer[lo : lo + piece, :].astype(f32) * conv).astype(bf16)
    loads[4].wait()

    @pl.loop(0, width // tile)
    def _(i):
        cols = pl.ds(pl.multiple_of(i * tile, tile), tile)
        some = pl.ds(pl.multiple_of(lax.rem(i, tiles) * tile, tile), tile)
        part = dot(gated[...], outw[:, cols]).astype(bf16)
        mixer_part[lax.div(i, tiles), :, :, some] = part.reshape(4, block, tile)

    pass_near(0)
    pass_near(1)
    relay(0)
    for j in range(2, PIECES):
        pass_near(j)

    relay(1)
    relay(2)
    relay(3)

    for j in range(3):
        for d in range(1, layers):
            from_layer(j, d).wait_recv()
        for d in sides:
            round_ring(j, d).start()
        from_ring(j, 0).start()
    for j in range(4, PIECES):
        relay(j)

    def passed(j):
        @pl.when(owner == 1)
        def _():
            onward(j).wait_recv()
            to_twin(3, j).start()

    passed(0)


    @pl.when(owner == 1)
    def _():
        some = landed.at[pl.ds(0, half_experts - 1)]
        remote(some, some, out_send.at[0], out_recv.at[0], twin, x).wait_recv()
        for j in range(PIECES):
            keep_own(j).wait()

    @pl.when(owner == 0)
    def _():
        some = landed.at[pl.ds(0, half_experts)]
        remote(some, some, out_send.at[0], out_recv.at[0], twin, x).wait_recv()

    def take_rows(m):
        @pl.loop(0, width // tile)
        def _(i):
            cols = pl.ds(pl.multiple_of(i * tile, tile), tile)
            rows[m * half : (m + 1) * half, cols] = landed[
                m * half_experts : (m + 1) * half_experts, :, cols
            ].reshape(half, tile)

    def gate_up(k, m):
        r = pl.ds(m * half, half)
        g = dot(rows[r, :], wgate[k])
        u = dot(rows[r, :], wup[k])
        act[r, k * units : (k + 1) * units] = (g / (1.0 + jnp.exp(-g)) * u).astype(bf16)

    take_rows(0)
    for k in range(3):

        @pl.when(owner == 0)
        def _():
            for j in range(PIECES):
                to_twin(k, j).wait_recv()

        gate_up(k, 0)
    passed(1)

    for i in range(width // tile):
        cols = pl.ds(i * tile, tile)
        total = dot(act[0:half, 0:units], wdown[0, :, cols])
        for k in range(1, 3):
            total = total + dot(act[0:half, k * units : (k + 1) * units], wdown[k, :, cols])
        total_down[:, cols] = total

    some = landed.at[pl.ds(half_experts, half_experts)]
    remote(some, some, out_send.at[0], out_recv.at[1], twin, x).wait_recv()
    take_rows(1)
    for k in range(3):
        gate_up(k, 1)

    for j in range(3):
        for d in sides:
            from_ring(j, d).wait_recv()
        if rings > 2:
            opposite(j).start()
        for d in sides:
            from_ring(j, d).start()

    for j in range(2):

        @pl.when(owner == 0)
        def _():
            to_twin(3, j).wait_recv()

    gate_up(3, 0)
    gate_up(3, 1)

    group_copy = remote(
        group.at[own_rows], group.at[near_rows], group_send.at[0], group_recv.at[0], ep, near
    )

    partners = [near, far]

    def first_copy(h, b):
        src = partners[h] if b == 0 else 3 - near
        return remote(
            mixer_part.at[h, src],
            first_in.at[h, b],
            first_send.at[2 * h + b],
            first_recv.at[2 * h + b],
            ep,
            partners[h],
        )

    def second_copy(h):
        return remote(
            second_out.at[h],
            second_in.at[h],
            second_send.at[h],
            second_recv.at[h],
            ep,
            partners[1 - h],
        )

    shared_copy = remote(
        shared_near, shared_in, shared_send.at[0], shared_recv.at[0], ep, near
    )

    for j in range(2, PIECES):
        passed(j)

    @pl.when(owner == 0)
    def _():
        for j in range(2, PIECES):
            to_twin(3, j).wait_recv()

    group_copy.start()
    for b in (1, 0):
        first_copy(0, b).start()

    def send_back(i):
        return remote(
            results.at[i],
            returned.at[mine],
            back_send.at[0],
            back_recv.at[0],
            source_order(i),
            plane,
        )

    def down(m):
        r = pl.ds(m * half, half)
        for i in range(width // tile):
            cols = pl.ds(i * tile, tile)
            total = dot(act[r, 3 * units : 4 * units], wdown[3, :, cols])
            if m == 0:
                total = total + total_down[:, cols]
            else:
                for k in range(3):
                    total = total + dot(act[r, k * units : (k + 1) * units], wdown[k, :, cols])
            results[m * half_experts : (m + 1) * half_experts, :, cols] = total.reshape(
                half_experts, capacity, tile
            ).astype(bf16)

        @pl.loop(m * half_experts, (m + 1) * half_experts, unroll=8)
        def _(i):
            @pl.when(i + 1 - owner > 0)
            def _():
                send_back(i).start()

    down(0)
    down(1)

    for b in (1, 0):
        first_copy(1, b).start()

    @pl.when(owner == 1)
    def _():
        returned[ep] = results[0]

    for d in range(2, rings - 1):
        for j in range(3):
            from_ring(j, d).wait_recv()
            from_ring(j, d).start()

    group_copy.wait_recv()
    for c in loads[5:8]:
        c.wait()

    def shared_gate_up(k):
        g = dot(group[...], sgate[k])
        u = dot(group[...], sup[k])
        sact[:, k * units : (k + 1) * units] = (g / (1.0 + jnp.exp(-g)) * u).astype(bf16)

    shared_gate_up(0)

    pieces = 4 if block % 64 == 0 else 1
    some_rows = block // pieces

    def pass_sum(h):
        first_copy(h, 1).wait_recv()

        @pl.loop(0, pieces)
        def _(i):
            r = pl.ds(pl.multiple_of(i * some_rows, some_rows), some_rows)
            second_out[h, r, :] = (
                mixer_part[h, partners[1 - h], r, :].astype(f32)
                + first_in[h, 1, r, :].astype(f32)
            ).astype(bf16)

        second_copy(h).start()

    for d in range(rings):
        for j in range(3):
            from_twin(j, d).wait_recv()
    shared_gate_up(1)

    for i in range(width // tile):
        cols = pl.ds(i * tile, tile)
        shared_near[:, cols] = dot(sact[near_rows, :], sdown[:, cols]).astype(bf16)

    shared_copy.start()

    for i in range(width // tile):
        cols = pl.ds(i * tile, tile)
        shared_own[:, cols] = dot(sact[own_rows, :], sdown[:, cols])

    pass_sum(0)
    pass_sum(1)

    for h in range(2):
        first_copy(h, 0).wait_recv()
        second_copy(h).wait_recv()

        @pl.loop(0, pieces)
        def _(i):
            r = pl.ds(pl.multiple_of(i * some_rows, some_rows), some_rows)
            mixer_out[r, h * (width // 2) : (h + 1) * (width // 2)] = (
                mixer_part[h, x, r, :].astype(f32)
                + first_in[h, 0, r, :].astype(f32)
                + second_in[h, r, :].astype(f32)
            ).astype(bf16)

    shared_copy.wait_recv()

    @pl.when(owner == 1)
    def _():
        some = returned.at[pl.ds(0, experts - 1)]
        remote(some, some, back_send.at[0], back_recv.at[0], twin, x).wait_recv()

    @pl.when(owner == 0)
    def _():
        remote(returned, returned, back_send.at[0], back_recv.at[0], twin, x).wait_recv()

    for i in range(width // tile):
        cols = pl.ds(i * tile, tile)
        back = returned[:, :, cols].reshape(slots, tile)
        total = shared_own[:, cols] + shared_in[:, cols].astype(f32)
        total = total + dot(spread_hi[...], back) + dot(spread_lo[...], back)
        expert_out[:, cols] = total.astype(bf16)

    for h in halos:
        h.wait_send()
    group_copy.wait_send()
    for h in range(2):
        for b in range(2):
            first_copy(h, b).wait_send()
        second_copy(h).wait_send()
    shared_copy.wait_send()
    for j in range(3):
        to_far_layer(j).wait_send()
        for d in range(1, layers):
            to_layer(j, d).wait_send()
        for d in range(rings):
            from_ring(j, d).wait_send()
        for d in sides:
            round_ring(j, d).wait_send()
        if rings > 2:
            opposite(j).wait_send()

    @pl.when(owner == 1)
    def _():
        for j in range(PIECES):
            to_near(j).wait_send()
            onward(j).wait_send()
            for k in range(4):
                to_twin(k, j).wait_send()
        some = outgoing.at[pl.ds(0, experts - 1)]
        remote(some, some, out_send.at[0], out_recv.at[0], twin, x).wait_send()
        some = results.at[pl.ds(0, experts - 1)]
        remote(some, some, back_send.at[0], back_recv.at[0], twin, x).wait_send()

    @pl.when(owner == 0)
    def _():
        for j in range(PIECES):
            to_far(j).wait_send()
        remote(outgoing, outgoing, out_send.at[0], out_recv.at[0], twin, x).wait_send()
        remote(results, results, back_send.at[0], back_recv.at[0], twin, x).wait_send()


def leave(mixer, expert, mixer_out, expert_out, sem):
    copies = [
        pltpu.make_async_copy(mixer, mixer_out, sem.at[0]),
        pltpu.make_async_copy(expert, expert_out, sem.at[1]),
    ]
    for c in copies:
        c.start()
    for c in copies:
        c.wait()


def per_device(
    outer_gate,
    inner_gate,
    conv_values,
    conv_taps,
    out_weight,
    moe_input,
    norm_gain,
    gate_proj,
    up_proj,
    down_proj,
    shared_gate,
    shared_up,
    shared_down,
    routes,
    route_weight,
):
    experts = lax.axis_size("ep")
    length, channels = inner_gate.shape
    block, width = moe_input.shape
    units = gate_proj.shape[2]
    capacity = 2 * block * routes.shape[1] // experts
    slots = experts * capacity
    rings = 4 if experts % 32 == 0 else 2
    layers = min(2, experts // (2 * rings))
    tile = min(256, width)
    vmem = pl.BlockSpec(memory_space=pltpu.VMEM)
    hbm = pl.BlockSpec(memory_space=pl.ANY)
    dma = pltpu.SemaphoreType.DMA

    def space(*shape):
        return pltpu.VMEM(shape, bf16)

    out = jax.ShapeDtypeStruct((block, width), bf16)
    outs = pl.pallas_call(
        functools.partial(kernel, experts, capacity, rings, layers, tile),
        name="whole",
        out_shape=(pltpu.VMEM(out.shape, bf16), pltpu.VMEM(out.shape, bf16)),
        in_specs=[hbm] * 15,
        out_specs=(vmem, vmem),
        scratch_shapes=[
            space(block, width),
            space(length, channels),
            space(length, channels),
            space(length, channels),
            space(HALO, channels),
            space(HALO, channels),
            pltpu.VMEM((HALO + length, channels), f32),
            space(length, channels),
            space(channels, width),
            space(2 * block, width),
            space(experts, capacity, width),
            space(experts, capacity, width),
            space(experts, capacity, width),
            space(experts, capacity, width),
            space(slots, width),
            space(4, width, units),
            space(4, width, units),
            space(4, units, width),
            space(2, width, units),
            space(2, width, units),
            space(2 * units, width),
            space(slots, 4 * units),
            space(2 * block, 2 * units),
            space(slots, block),
            space(block, slots),
            space(block, slots),
            pltpu.VMEM((slots // 2, width), f32),
            space(2, 4, block, width // 2),
            pltpu.VMEM((block, width), f32),
            space(block, width),
            space(block, width),
            space(2, 2, block, width // 2),
            space(2, block, width // 2),
            space(2, block, width // 2),
            dma((8,)),
            dma((2,)),
            dma((2,)),
            dma((1,)),
            dma((1,)),
            dma((1,)),
            dma((2,)),
            dma((PIECES,)),
            dma((PIECES,)),
            dma((2 * PIECES,)),
            dma((4 * PIECES,)),
            dma((4 * PIECES,)),
            dma((4,)),
            dma((4,)),
            dma((2,)),
            dma((2,)),
            dma((1,)),
            dma((1,)),
            dma((3,)),
            dma((3 * layers,)),
            dma((3 * layers,)),
            dma((3 * rings,)),
            dma((3 * rings,)),
            dma((6 * rings,)),
            dma((1,)),
            dma((1,)),
            pltpu.SemaphoreType.REGULAR((8,)),
            space(*conv_taps.shape),
            space(width),
            pltpu.VMEM(routes.shape[::-1], jnp.int32),
            pltpu.VMEM(route_weight.shape[::-1], f32),
            dma((4,)),
        ],
        compiler_params=pltpu.CompilerParams(
            collective_id=0, has_side_effects=True, vmem_limit_bytes=60 * 1024 * 1024
        ),
    )(
        outer_gate,
        inner_gate,
        conv_values,
        conv_taps,
        out_weight,
        moe_input,
        norm_gain,
        gate_proj,
        up_proj,
        down_proj,
        shared_gate,
        shared_up,
        shared_down,
        routes.T,
        route_weight.T,
    )
    return pl.pallas_call(
        leave,
        name="leave",
        out_shape=(out, out),
        in_specs=[vmem, vmem],
        out_specs=(hbm, hbm),
        scratch_shapes=[dma((2,))],
    )(*[pltpu.with_memory_space_constraint(o, pltpu.VMEM) for o in outs])


def solution(mesh):
    return jax.shard_map(
        per_device,
        mesh=mesh,
        in_specs=(
            P("ep", "tp"),
            P("ep", "tp"),
            P("ep", "tp"),
            P(None, "tp"),
            P("tp", None),
            P(("ep", "tp"), None),
            P(),
            P("ep", None, "tp"),
            P("ep", None, "tp"),
            P("ep", "tp", None),
            P(None, "tp"),
            P(None, "tp"),
            P("tp", None),
            P("ep", None),
            P("ep", None),
        ),
        out_specs=(P(("ep", "tp"), None), P(("ep", "tp"), None)),
        check_vma=False,
    )
```
